512 devices in a mesh: ep: 32 (over z, core), tp: 16 (over y, x).
Axes of the slice: x: 4, y: 4, z: 16, core: 2. Of those that a mesh axis runs over, the one named last changes fastest.
Arguments:
- mixer_input: bfloat16 [8192, 2048], P('ep'), may hold values from -6 to 6
- mixer_gain: float32 [2048], replicated, may hold values from 0.1 to 1.9
- query_weight: bfloat16 [2048, 2048], P(None, 'tp'), may hold values from -0.13258252 to 0.13258252
- key_weight: bfloat16 [2048, 1024], P(None, 'tp'), may hold values from -2.78423295 to 2.78423295
- value_weight: bfloat16 [2048, 1024], P(None, 'tp'), may hold values from -0.125 to 0.125
- output_weight: bfloat16 [2048, 2048], P(None, 'tp'), may hold values from -1 to 1
- sink_logit: float32 [32], P('tp'), may hold values from 2 to 7
- expert_input: bfloat16 [4096, 2048], P('ep'), may hold values from -6 to 6
- expert_gain: float32 [2048], replicated, may hold values from 0.1 to 1.9
- routes: int32 [4096, 4], P('ep'), may hold values from 0 to 31, all different within a row; in each aligned block of 128 rows (0 to 127, 128 to 255, ...) at most 32 rows name the same one
- route_logits: float32 [4096, 4], P('ep'), may hold values from -6 to 6
- gate_weight: bfloat16 [32, 2048, 2048], P('ep', None, 'tp'), may hold values from -0.375 to 0.375
- up_weight: bfloat16 [32, 2048, 2048], P('ep', None, 'tp'), may hold values from -0.375 to 0.375
- down_weight: bfloat16 [32, 2048, 2048], P('ep', None, 'tp'), may hold values from -0.03125 to 0.03125
Outputs:
- mixer_output: bfloat16 [8192, 2048], P('ep', 'tp')
- expert_output: bfloat16 [4096, 2048], P('ep', 'tp')
The draws below stay inside these ranges and needn't reach their ends.
Inputs may be any that keep to these rules, and one draw needn't show every extreme that they name: `routes`: each token names 4 different experts. Among the 128 tokens of one index of ep (aligned blocks) no expert is named more than 32 times, and in some blocks one expert is named exactly 32 times.
All inputs are finite; a program needn't handle non-finite values.
Results may differ from the reference program's by a relative error of at most 0.0055.
The reference program's roundings to bfloat16 on the way count: a program that leaves them out, or rounds other values in their place, can miss the bound.
Values may be sent and summed in bfloat16 or wider, within the bound.
No kernel may reach another device: no remote copies, remote signals or barrier semaphores. Data moves between devices by JAX's collectives and lax.ppermute only.
A program may use at most 64 MiB of HBM per device.

```python
import math
import jax
import jax.numpy as jnp
import numpy as np
from jax import lax

D = 2048
HEADS = 32
KV_HEADS = 16
HEAD_DIM = 64
FF = 2048
TOP_K = 4
WINDOW = 128
GRID_W = 64
EXP_DEV = 128
EXPERTS = 32
CAP = 32
MIX_TOKENS = 8192
EXP_TOKENS = 4096
N_EP = 32


def paired_weights(key):
    base = jax.random.fold_in(key, 11)
    first, second = jax.random.split(base)
    query = jnp.clip(jax.random.normal(first, (D, HEADS * HEAD_DIM), jnp.float32), -6.0, 6.0) / math.sqrt(D)
    noise = jnp.clip(jax.random.normal(second, (D, KV_HEADS * HEAD_DIM), jnp.float32), -6.0, 6.0) / math.sqrt(D)
    keys = noise
    return (query, keys)


def draw_query_weight(key, part):
    return paired_weights(key)[0].astype(jnp.bfloat16)


def draw_key_weight(key, part):
    return paired_weights(key)[1].astype(jnp.bfloat16)


def levels(rng, shape, pieces, least, largest):
    level = 1.0
    for position, blocks in pieces:
        draws = jax.random.uniform(jax.random.fold_in(jax.random.fold_in(rng, 6), position), (blocks,), jnp.float32, least / len(pieces), largest / len(pieces))
        level = level * jnp.repeat(jnp.exp(draws), shape[position] // blocks).reshape((-1,) + (1,) * (len(shape) - 1 - position))
    return level


def routed_block(own_key, own, number, rows, amount, top, reach, slope):
    sequence = jax.random.permutation(own_key, amount)
    packed, common = portions_of(amount, rows * top, reach, slope, True), portions_of(amount, rows * top, reach, slope, False)
    places = jnp.arange(amount)

    def named(sizes, rotation):
        used = int((sizes > 0).sum())
        fixed = max(1, used // 4)
        moved = fixed + (places - fixed + rotation * (used - fixed)) % max(1, amount - fixed)
        return jnp.zeros((amount,), jnp.int32).at[sequence[jnp.where(places < fixed, places, moved)]].set(jnp.asarray(sizes, jnp.int32))

    sizes = jnp.where(number % 4 == 0, named(packed, number // 4), named(common, number - number // 4 - 1))
    mixed = jax.random.permutation(jax.random.fold_in(own, 3), amount)
    giver, sink = mixed[0:amount // 2 * 2:2], mixed[1:amount // 2 * 2:2]
    margin = jnp.minimum(sizes[giver] - 1, reach - sizes[sink]) // 2
    margin = jnp.where((giver == sequence[0]) | (sink == sequence[0]) | (sizes[sink] == 0), 0, jnp.maximum(margin, 0))
    moved = jax.random.randint(jax.random.fold_in(own, 4), (amount // 2,), 0, 1 << 20) % (margin + 1)
    sizes = sizes.at[giver].add(-moved).at[sink].add(moved)
    labels = jnp.searchsorted(jnp.cumsum(sizes), jnp.arange(rows * top), side="right").astype(jnp.int32)
    grid = labels.reshape(top, rows).T
    grid = grid[jax.random.permutation(jax.random.fold_in(own, 1), rows)]
    rotation = jax.random.randint(jax.random.fold_in(own, 2), (rows, 1), 0, top)
    return jnp.take_along_axis(grid, (jnp.arange(top)[None, :] + rotation) % top, axis=1)


def portions_of(amount, total, reach, slope, full):
    portions = [(1 << 20) // math.isqrt(standing ** slope) + 1 for standing in range(1, amount + 1)]
    largest = reach if full else min(reach, max(-(-total // amount), total * portions[0] // sum(portions)))
    least = 1 if total - largest >= amount - 1 else 0
    given, rest = [largest] + [least] * (amount - 1), total - largest - least * (amount - 1)
    while rest > 0:
        free = [i for i in range(1, amount) if given[i] < largest] or [i for i in range(1, amount) if given[i] < reach]
        whole, remaining = sum([portions[i] for i in free]), rest
        for i in free:
            addition = min(reach - given[i], max(1, remaining * portions[i] // whole), rest)
            given[i] = given[i] + addition
            rest = rest - addition
    return np.array(given)


def gaussian(rng, extent, width, reach, cuts=(), kind=jnp.bfloat16):
    entries = jax.random.normal(rng, extent, jnp.float32) * width
    if len(cuts) > 0:
        entries = levels(rng, extent, cuts, -0.22, 0.18) * entries
    return jnp.clip(entries, min=-reach, max=reach).astype(kind)


def setup_inputs(seed: int = 0) -> dict:
    splits = jax.random.split(jax.random.key(seed), 15)
    mixer_input = gaussian(splits[0], (MIX_TOKENS, D), 1.0, 6.0, ((0, 32),))
    mixer_gain = jnp.clip(1.0 + 0.18 * jax.random.normal(splits[1], (D,), jnp.float32), 0.1, 1.9)
    query_weight = draw_query_weight(jax.random.fold_in(splits[14], 71), 0)
    key_weight = draw_key_weight(jax.random.fold_in(splits[14], 71), 0)
    value_weight = gaussian(splits[4], (D, KV_HEADS * HEAD_DIM), D ** -0.5, 0.125, ((1, 16),))
    output_weight = gaussian(splits[5], (HEADS * HEAD_DIM, D), (HEADS * HEAD_DIM // 64) ** -0.5, 1.0, ((1, 16),))
    sink_logit = jnp.clip(2.0 + 5.0 * jax.random.uniform(splits[6], (HEADS,), jnp.float32) ** levels(splits[6], (HEADS,), ((0, 16),), -0.2, 0.2), 2.0, 7.0)
    expert_input = gaussian(splits[7], (EXP_TOKENS, D), 1.0, 6.0, ((0, 32),))
    expert_gain = jnp.clip(1.0 + 0.18 * jax.random.normal(splits[8], (D,), jnp.float32), 0.1, 1.9)
    routes_keys = jax.random.split(jax.random.fold_in(splits[9], 1), EXP_TOKENS // EXP_DEV)
    routes_turns = jax.random.permutation(jax.random.fold_in(splits[9], 3), EXP_TOKENS // EXP_DEV)
    routes = jax.vmap(lambda own, number: routed_block(jax.random.fold_in(splits[9], 2), own, number, EXP_DEV, EXPERTS, TOP_K, CAP, 2))(routes_keys, routes_turns).reshape((EXP_TOKENS, TOP_K))
    route_logits = gaussian(splits[10], (EXP_TOKENS, TOP_K), 1.5, 6.0, ((0, 32),), jnp.float32)
    gate_weight = gaussian(splits[11], (EXPERTS, D, FF), (D // 9) ** -0.5, 0.375, ((0, 32), (2, 16)))
    up_weight = gaussian(splits[12], (EXPERTS, D, FF), (D // 9) ** -0.5, 0.375, ((0, 32), (2, 16)))
    down_weight = gaussian(splits[13], (EXPERTS, FF, D), (16 * FF) ** -0.5, 0.03125, ((0, 32), (2, 16)))
    return {"mixer_input": mixer_input, "mixer_gain": mixer_gain, "query_weight": query_weight, "key_weight": key_weight, "value_weight": value_weight, "output_weight": output_weight, "sink_logit": sink_logit, "expert_input": expert_input, "expert_gain": expert_gain, "routes": routes, "route_logits": route_logits, "gate_weight": gate_weight, "up_weight": up_weight, "down_weight": down_weight}


EPSILON = 1e-06
LIMIT = 7.0
SLOPE = 1.702
BASE = 10000.0

def normalize(rows, gain):
    values = rows.astype(jnp.float32)
    scaled = values * lax.rsqrt(lax.optimization_barrier(jnp.mean(values * values, axis=-1, keepdims=True)) + EPSILON)
    return (scaled * gain).astype(jnp.bfloat16)

def turn(values, cosine, sine):
    first, second = jnp.split(values, 2, axis=-1)
    cosine = cosine[:, None, :]
    sine = sine[:, None, :]
    return jnp.concatenate([first * cosine - second * sine, second * cosine + first * sine], axis=-1)

def axial_rope(values, places):
    quarter = values.shape[-1] // 4
    frequency = BASE ** (-jnp.arange(quarter, dtype=jnp.float32) / quarter)
    row_angle = (places // GRID_W).astype(jnp.float32)[:, None] * frequency[None, :]
    column_angle = (places % GRID_W).astype(jnp.float32)[:, None] * frequency[None, :]
    row_part, column_part = jnp.split(values, 2, axis=-1)
    return jnp.concatenate([turn(row_part, jnp.cos(row_angle), jnp.sin(row_angle)), turn(column_part, jnp.cos(column_angle), jnp.sin(column_angle))], axis=-1)

def activate(gate, up):
    capped = jnp.minimum(gate, LIMIT)
    bounded = jnp.clip(up, -LIMIT, LIMIT)
    return (capped * jax.nn.sigmoid(SLOPE * capped) * (bounded + 1.0)).astype(jnp.bfloat16)

def band_attention(parts):
    query, keys, values, sinks = parts
    total = query.shape[0]
    group = query.shape[1]
    blocks = total // WINDOW
    padded_keys = jnp.pad(keys, ((WINDOW, WINDOW), (0, 0))).reshape(blocks + 2, WINDOW, HEAD_DIM)
    padded_values = jnp.pad(values, ((WINDOW, WINDOW), (0, 0))).reshape(blocks + 2, WINDOW, HEAD_DIM)
    near_keys = jnp.concatenate([padded_keys[:-2], padded_keys[1:-1], padded_keys[2:]], axis=1)
    near_values = jnp.concatenate([padded_values[:-2], padded_values[1:-1], padded_values[2:]], axis=1)
    blocked = query.reshape(blocks, WINDOW, group, HEAD_DIM)
    scores = jnp.einsum('nqrd,nkd->nrqk', blocked.astype(jnp.float32), near_keys.astype(jnp.float32)) * HEAD_DIM ** (-0.5)
    query_place = jnp.arange(total, dtype=jnp.int32).reshape(blocks, WINDOW)
    key_place = (jnp.arange(blocks, dtype=jnp.int32)[:, None] - 1) * WINDOW + jnp.arange(3 * WINDOW, dtype=jnp.int32)[None, :]
    allowed = (jnp.abs(query_place[:, :, None] - key_place[:, None, :]) <= WINDOW) & (key_place[:, None, :] >= 0) & (key_place[:, None, :] < total)
    scores = jnp.where(allowed[:, None], scores, -1e+30)
    sink_column = sinks[None, :, None]
    top = jnp.maximum(lax.optimization_barrier(jnp.max(scores, axis=-1)), sink_column)
    weights = jnp.exp(scores - top[..., None])
    denominator = lax.optimization_barrier(jnp.sum(weights, axis=-1)) + jnp.exp(sink_column - top)
    shares = (weights / denominator[..., None]).astype(jnp.bfloat16)
    mixed = jnp.einsum('nrqk,nkd->nqrd', shares.astype(jnp.float32), near_values.astype(jnp.float32))
    return mixed.astype(jnp.bfloat16).reshape(total, group * HEAD_DIM)

def mixer_half(mixer_input, mixer_gain, query_weight, key_weight, value_weight, output_weight, sink_logit):
    total = mixer_input.shape[0]
    group = HEADS // KV_HEADS
    normed = normalize(mixer_input, mixer_gain)
    places = jnp.arange(total, dtype=jnp.int32)
    query = jnp.dot(normed, query_weight, preferred_element_type=jnp.float32).reshape(total, HEADS, HEAD_DIM)
    query = axial_rope(query, places).astype(jnp.bfloat16).reshape(total, KV_HEADS, group, HEAD_DIM)
    keys = jnp.dot(normed, key_weight, preferred_element_type=jnp.float32).reshape(total, KV_HEADS, HEAD_DIM)
    keys = axial_rope(keys, places).astype(jnp.bfloat16)
    values = jnp.dot(normed, value_weight, preferred_element_type=jnp.float32).astype(jnp.bfloat16).reshape(total, KV_HEADS, HEAD_DIM)
    mixed = lax.map(band_attention, (query.transpose(1, 0, 2, 3), keys.transpose(1, 0, 2), values.transpose(1, 0, 2), sink_logit.reshape(KV_HEADS, group)))
    mixed = mixed.transpose(1, 0, 2).reshape(total, HEADS * HEAD_DIM)
    return jnp.dot(mixed, output_weight, preferred_element_type=jnp.float32).astype(jnp.bfloat16)

def expert_half(expert_input, expert_gain, routes, route_logits, gate_weight, up_weight, down_weight):
    normed = normalize(expert_input, expert_gain)
    chances = jax.nn.softmax(route_logits, axis=-1)
    chosen = routes.reshape(-1)
    count = chosen.shape[0]
    marks = (chosen[:, None] == jnp.arange(EXPERTS, dtype=jnp.int32)[None, :]).astype(jnp.int32)
    earlier = lax.optimization_barrier(jnp.sum((jnp.cumsum(marks, axis=0) - marks) * marks, axis=1))
    room = N_EP * CAP
    target = chosen * room + earlier
    holder = jnp.full((EXPERTS * room,), count, jnp.int32).at[target].set(jnp.arange(count, dtype=jnp.int32))
    holder = (holder // TOP_K).reshape(EXPERTS, room)
    padded = jnp.concatenate([normed, jnp.zeros((1, normed.shape[1]), jnp.bfloat16)], axis=0)

    def serve(parts):
        token_index, gate_part, up_part, down_part = parts
        rows = padded[token_index]
        gate = jnp.dot(rows, gate_part, preferred_element_type=jnp.float32)
        up = jnp.dot(rows, up_part, preferred_element_type=jnp.float32)
        hidden = activate(gate, up)
        return jnp.dot(hidden, down_part, preferred_element_type=jnp.float32).astype(jnp.bfloat16)
    served = lax.map(serve, (holder, gate_weight, up_weight, down_weight))
    flat = served.reshape(EXPERTS * room, served.shape[2])
    picked = flat[target].astype(jnp.float32).reshape(-1, TOP_K, served.shape[2])
    return lax.optimization_barrier(jnp.sum(picked * chances[:, :, None], axis=1)).astype(jnp.bfloat16)

def reference(mixer_input, mixer_gain, query_weight, key_weight, value_weight, output_weight, sink_logit, expert_input, expert_gain, routes, route_logits, gate_weight, up_weight, down_weight):
    mixer_output = mixer_half(mixer_input, mixer_gain, query_weight, key_weight, value_weight, output_weight, sink_logit)
    expert_output = expert_half(expert_input, expert_gain, routes, route_logits, gate_weight, up_weight, down_weight)
    return (mixer_output, expert_output)
```

```python
import jax
import jax.numpy as jnp
from jax import lax
from jax.experimental import pallas as pl
from jax.experimental.pallas import tpu as pltpu
from jax.sharding import Mesh
from jax.sharding import PartitionSpec as P

HEAD_DIM = 64
TOP_K = 4
WINDOW = 128
GRID_W = 64
EP = ("ep_0", "ep_1")
TP = ("y", "x")

EPSILON = 1e-06
LIMIT = 7.0
SLOPE = 1.702
BASE = 10000.0


def extended(shard, axis, width):
    devices, length = lax.axis_size(axis), shard.shape[0]
    up = [(i, (i + 1) % devices) for i in range(devices - 1)]
    down = [(j, i) for i, j in up]
    before = lax.ppermute(shard[length - width :], axis, up)
    after = lax.ppermute(shard[:width], axis, down)
    return jnp.concatenate([before, shard, after], axis=0)


def swap(pieces, axis):
    return lax.all_to_all(pieces, axis, 0, 0, tiled=True)


def spread(shard, axis):
    return swap(jnp.broadcast_to(shard[None], (lax.axis_size(axis), *shard.shape)), axis)


def normalize(rows, gain):
    values = rows.astype(jnp.float32)
    scaled = values * lax.rsqrt(jnp.mean(values * values, axis=-1, keepdims=True) + EPSILON)
    return (scaled * gain).astype(jnp.bfloat16)


def turn(values, cosine, sine):
    first, second = jnp.split(values, 2, axis=-1)
    cosine = cosine[:, None, :]
    sine = sine[:, None, :]
    return jnp.concatenate(
        [first * cosine - second * sine, second * cosine + first * sine], axis=-1
    )


def axial_rope(values, places):
    quarter = values.shape[-1] // 4
    frequency = BASE ** (-jnp.arange(quarter, dtype=jnp.float32) / quarter)
    row_angle = (places // GRID_W).astype(jnp.float32)[:, None] * frequency[None, :]
    column_angle = (places % GRID_W).astype(jnp.float32)[:, None] * frequency[None, :]
    row_part, column_part = jnp.split(values, 2, axis=-1)
    return jnp.concatenate(
        [
            turn(row_part, jnp.cos(row_angle), jnp.sin(row_angle)),
            turn(column_part, jnp.cos(column_angle), jnp.sin(column_angle)),
        ],
        axis=-1,
    )


def activate(gate, up):
    capped = jnp.minimum(gate, LIMIT)
    bounded = jnp.clip(up, -LIMIT, LIMIT)
    return (capped * jax.nn.sigmoid(SLOPE * capped) * (bounded + 1.0)).astype(jnp.bfloat16)


def dot(a, b):
    return jnp.dot(a, b, preferred_element_type=jnp.float32)


def dispatch(rows, gain, routes, place, experts, slots, width):
    tokens = rows.shape[0]
    capacity = slots * lax.axis_size("x")

    def kernel(place_ref, rows_ref, gain_ref, routes_ref, routes_t_ref, out_ref, target_ref):
        values = rows_ref[...].astype(jnp.float32)
        scale = lax.rsqrt(jnp.mean(values * values, axis=-1, keepdims=True) + EPSILON)
        start = pl.multiple_of(place_ref[0] * width, width)
        own = rows_ref[:, pl.ds(start, width)].astype(jnp.float32)
        normed = (own * scale * gain_ref[:, pl.ds(start, width)]).astype(jnp.bfloat16)
        first = lax.broadcasted_iota(jnp.int32, (tokens, tokens), 0)
        second = lax.broadcasted_iota(jnp.int32, (tokens, tokens), 1)
        expert = lax.broadcasted_iota(jnp.int32, (experts, tokens), 0)
        named = jnp.zeros((experts, tokens), jnp.float32)
        for k in range(TOP_K):
            named = named + (routes_t_ref[k : k + 1, :] == expert).astype(jnp.float32)
        earlier = dot(named.astype(jnp.bfloat16), (first < second).astype(jnp.bfloat16))
        rank = jnp.where(named > 0.0, earlier.astype(jnp.int32), -1) - place_ref[1] * slots
        slot = lax.broadcasted_iota(jnp.int32, (experts, slots, tokens), 1)
        chosen = (rank[:, None, :] == slot).astype(jnp.float32).reshape(experts * slots, tokens)
        out_ref[...] = dot(chosen.astype(jnp.bfloat16), normed).astype(jnp.bfloat16)
        column = lax.broadcasted_iota(jnp.int32, (tokens, experts), 1)
        marks = [(routes_ref[:, k : k + 1] == column).astype(jnp.float32) for k in range(TOP_K)]
        before = dot((second < first).astype(jnp.bfloat16), sum(marks).astype(jnp.bfloat16))
        position = before + column.astype(jnp.float32) * float(capacity)
        target_ref[...] = jnp.concatenate(
            [jnp.sum(mark * position, axis=1, keepdims=True) for mark in marks], axis=1
        ).astype(jnp.int32)

    vmem = pl.BlockSpec(memory_space=pltpu.VMEM)
    return pl.pallas_call(
        kernel,
        out_shape=(
            jax.ShapeDtypeStruct((experts * slots, width), jnp.bfloat16),
            jax.ShapeDtypeStruct((tokens, TOP_K), jnp.int32),
        ),
        in_specs=[pl.BlockSpec(memory_space=pltpu.SMEM)] + [vmem] * 4,
        out_specs=(vmem, vmem),
        name="dispatch",
    )(place, rows, gain[None, :], routes, routes.T)


def gated(rows, weights):
    parts, n, k = rows.shape
    pieces, _, both = weights.shape
    u = both // 2

    def kernel(rows_ref, weights_ref, out_ref):
        total = dot(rows_ref[0], weights_ref[0, :k, :])
        for part in range(1, parts):
            total = total + dot(rows_ref[part], weights_ref[0, part * k : (part + 1) * k, :])
        hidden = activate(total[:, :u], total[:, u:])
        for copy in range(parts):
            out_ref[copy] = hidden

    return pl.pallas_call(
        kernel,
        grid=(pieces,),
        out_shape=jax.ShapeDtypeStruct((parts, n, pieces * u), jnp.bfloat16),
        in_specs=[
            pl.BlockSpec((parts, n, k), lambda i: (0, 0, 0)),
            pl.BlockSpec((1, parts * k, both), lambda i: (i, 0, 0)),
        ],
        out_specs=pl.BlockSpec((parts, n, u), lambda i: (0, 0, i)),
        name="gated",
    )(rows, weights)


def lowered(hidden, weights):
    parts, n, k = hidden.shape
    pieces, _, f = weights.shape

    def kernel(hidden_ref, weights_ref, out_ref):
        total = dot(hidden_ref[0], weights_ref[0, :k, :])
        for part in range(1, parts):
            total = total + dot(hidden_ref[part], weights_ref[0, part * k : (part + 1) * k, :])
        out_ref[0] = total.astype(jnp.bfloat16)

    return pl.pallas_call(
        kernel,
        grid=(pieces,),
        out_shape=jax.ShapeDtypeStruct((pieces, n, f), jnp.bfloat16),
        in_specs=[
            pl.BlockSpec((parts, n, k), lambda i: (0, 0, 0)),
            pl.BlockSpec((1, parts * k, f), lambda i: (i, 0, 0)),
        ],
        out_specs=pl.BlockSpec((1, n, f), lambda i: (i, 0, 0)),
        name="lowered",
    )(hidden, weights)


def combine(results, target, logits):
    slots, f = results.shape
    tokens = target.shape[0]

    def kernel(results_ref, target_ref, logits_ref, out_ref):
        chances = jax.nn.softmax(logits_ref[...], axis=-1)
        lane = lax.broadcasted_iota(jnp.int32, (tokens, slots), 1)
        total = jnp.zeros((tokens, f), jnp.float32)
        for k in range(TOP_K):
            chosen = (target_ref[:, k : k + 1] == lane).astype(jnp.float32).astype(jnp.bfloat16)
            total = total + dot(chosen, results_ref[...]) * chances[:, k : k + 1]
        out_ref[...] = total.astype(jnp.bfloat16)

    vmem = pl.BlockSpec(memory_space=pltpu.VMEM)
    return pl.pallas_call(
        kernel,
        out_shape=jax.ShapeDtypeStruct((tokens, f), jnp.bfloat16),
        in_specs=[vmem] * 3,
        out_specs=vmem,
        name="combine",
    )(results, target, logits)


def attention(mixer_input, mixer_gain, query_weight, key_weight, value_weight, sink_logit):
    tokens = mixer_input.shape[0]
    query_heads = query_weight.shape[1] // HEAD_DIM
    key_heads = key_weight.shape[1] // HEAD_DIM
    group = query_heads // key_heads
    blocks = tokens // WINDOW
    offset = lax.axis_index(EP) * tokens
    length = lax.axis_size(EP) * tokens
    places = offset + jnp.arange(tokens, dtype=jnp.int32)
    normed = normalize(mixer_input, mixer_gain)
    query = dot(normed, query_weight).reshape(tokens, query_heads, HEAD_DIM)
    query = (
        axial_rope(query, places)
        .astype(jnp.bfloat16)
        .reshape(blocks, WINDOW, key_heads, group, HEAD_DIM)
    )
    keys = dot(normed, key_weight).reshape(tokens, key_heads, HEAD_DIM)
    keys = axial_rope(keys, places).astype(jnp.bfloat16).reshape(tokens, key_heads * HEAD_DIM)
    values = dot(normed, value_weight).astype(jnp.bfloat16)
    stacked = jnp.concatenate([keys, values], axis=1)
    widened = extended(stacked, EP, WINDOW)
    framed = widened.reshape(blocks + 2, WINDOW, 2, key_heads, HEAD_DIM)
    nearby = jnp.concatenate([framed[:-2], framed[1:-1], framed[2:]], axis=1)
    scores = jnp.einsum(
        "nqgrd,nkgd->ngrqk", query, nearby[:, :, 0], preferred_element_type=jnp.float32
    ) * HEAD_DIM ** (-0.5)
    query_place = places.reshape(blocks, WINDOW)
    key_place = (
        offset
        + (jnp.arange(blocks, dtype=jnp.int32)[:, None] - 1) * WINDOW
        + jnp.arange(3 * WINDOW, dtype=jnp.int32)[None, :]
    )
    allowed = (
        (jnp.abs(query_place[:, :, None] - key_place[:, None, :]) <= WINDOW)
        & (key_place[:, None, :] >= 0)
        & (key_place[:, None, :] < length)
    )
    scores = jnp.where(allowed[:, None, None], scores, -1e30)
    sinks = sink_logit.reshape(key_heads, group)[None, :, :, None]
    top = jnp.maximum(jnp.max(scores, axis=-1), sinks)
    weights = jnp.exp(scores - top[..., None])
    denominator = jnp.sum(weights, axis=-1) + jnp.exp(sinks - top)
    shares = (weights / denominator[..., None]).astype(jnp.bfloat16)
    mixed = jnp.einsum(
        "ngrqk,nkgd->nqgrd", shares, nearby[:, :, 1], preferred_element_type=jnp.float32
    )
    return mixed.astype(jnp.bfloat16).reshape(tokens, query_heads * HEAD_DIM)


def shards(
    mixer_input,
    mixer_gain,
    query_weight,
    key_weight,
    value_weight,
    output_weight,
    sink_logit,
    expert_input,
    expert_gain,
    routes,
    route_logits,
    gate_weight,
    up_weight,
    down_weight,
):
    experts = lax.axis_size(EP)
    rows_here, features = expert_input.shape
    across, along = lax.axis_size("x"), lax.axis_size("y")
    slots = 2 * rows_here * TOP_K // experts // across
    width = features // along
    place = jnp.stack([lax.axis_index("y"), lax.axis_index("x")]).astype(jnp.int32)

    outgoing, target = dispatch(
        expert_input, expert_gain, routes, place, experts, slots, width
    )
    received = swap(outgoing.reshape(experts, slots, width), EP)
    both = spread(jnp.concatenate([gate_weight[0], up_weight[0]], axis=1), "x")
    down = spread(down_weight[0], "x")

    mixed = attention(
        mixer_input, mixer_gain, query_weight, key_weight, value_weight, sink_logit
    )
    heads = spread(mixed, TP)

    rows = spread(received.reshape(experts * slots, width), "y")
    hidden = swap(gated(rows, both), "y")
    result = swap(lowered(hidden, down), "x")
    result = result.reshape(across, experts, slots, -1).transpose(1, 0, 2, 3)
    returned = swap(result, EP)
    expert_output = combine(
        returned.reshape(experts * across * slots, -1), target, route_logits
    )
    pieces = output_weight.reshape(heads.shape[0], heads.shape[2], -1)
    mixer_output = jnp.einsum(
        "trj,tjn->rn", heads, pieces, preferred_element_type=jnp.float32
    ).astype(jnp.bfloat16)
    return (mixer_output, expert_output)


def solution(mesh):
    finer = Mesh(mesh.devices.reshape(16, 2, 4, 4), ("ep_0", "ep_1", "y", "x"))
    in_specs = (
        P(EP, None),
        P(),
        P(None, TP),
        P(None, TP),
        P(None, TP),
        P(None, TP),
        P(TP),
        P(EP, None),
        P(),
        P(EP, None),
        P(EP, None),
        P(EP, None, TP),
        P(EP, None, TP),
        P(EP, None, TP),
    )
    out_specs = (P(EP, TP), P(EP, TP))
    return jax.shard_map(
        shards, mesh=finer, in_specs=in_specs, out_specs=out_specs, check_vma=False
    )
```

```python
import itertools

import jax
import jax.numpy as jnp
from jax import lax
from jax.experimental import pallas as pl
from jax.experimental.pallas import tpu as pltpu
from jax.sharding import Mesh
from jax.sharding import PartitionSpec as P

HEAD_DIM = 64
TOP_K = 4
WINDOW = 128
GRID_W = 64
EP = ("ep_0", "ep_1")
TP = ("Y", "h", "X", "p")

EPSILON = 1e-06
LIMIT = 7.0
SLOPE = 1.702
BASE = 10000.0


def extended(shard, axis, width):
    devices, length = lax.axis_size(axis), shard.shape[0]
    up = [(i, (i + 1) % devices) for i in range(devices - 1)]
    down = [(j, i) for i, j in up]
    before = lax.ppermute(shard[length - width :], axis, up)
    after = lax.ppermute(shard[:width], axis, down)
    return jnp.concatenate([before, shard, after], axis=0)


def swap(pieces, axis):
    return lax.all_to_all(pieces, axis, 0, 0, tiled=True)


def spread(shard, axis):
    return swap(jnp.broadcast_to(shard[None], (lax.axis_size(axis), *shard.shape)), axis)


def normalize(rows, gain):
    values = rows.astype(jnp.float32)
    scaled = values * lax.rsqrt(jnp.mean(values * values, axis=-1, keepdims=True) + EPSILON)
    return (scaled * gain).astype(jnp.bfloat16)


def turn(values, cosine, sine):
    first, second = jnp.split(values, 2, axis=-1)
    cosine = cosine[:, None, :]
    sine = sine[:, None, :]
    return jnp.concatenate(
        [first * cosine - second * sine, second * cosine + first * sine], axis=-1
    )


def axial_rope(values, places):
    quarter = values.shape[-1] // 4
    frequency = BASE ** (-jnp.arange(quarter, dtype=jnp.float32) / quarter)
    row_angle = (places // GRID_W).astype(jnp.float32)[:, None] * frequency[None, :]
    column_angle = (places % GRID_W).astype(jnp.float32)[:, None] * frequency[None, :]
    row_part, column_part = jnp.split(values, 2, axis=-1)
    return jnp.concatenate(
        [
            turn(row_part, jnp.cos(row_angle), jnp.sin(row_angle)),
            turn(column_part, jnp.cos(column_angle), jnp.sin(column_angle)),
        ],
        axis=-1,
    )


def activate(gate, up):
    capped = jnp.minimum(gate, LIMIT)
    bounded = jnp.clip(up, -LIMIT, LIMIT)
    return (capped * jax.nn.sigmoid(SLOPE * capped) * (bounded + 1.0)).astype(jnp.bfloat16)


def dot(a, b):
    return jnp.dot(a, b, preferred_element_type=jnp.float32)


def dispatch(rows, gain, routes, place, experts, slots, width):
    tokens = rows.shape[0]
    pairs = experts // 2

    def kernel(place_ref, rows_ref, gain_ref, routes_ref, routes_t_ref, out_ref, target_ref):
        values = rows_ref[...].astype(jnp.float32)
        scale = lax.rsqrt(jnp.mean(values * values, axis=-1, keepdims=True) + EPSILON)
        start = pl.multiple_of(place_ref[0] * width, width)
        own = rows_ref[:, pl.ds(start, width)].astype(jnp.float32)
        normed = (own * scale * gain_ref[:, pl.ds(start, width)]).astype(jnp.bfloat16)
        first = lax.broadcasted_iota(jnp.int32, (tokens, tokens), 0)
        second = lax.broadcasted_iota(jnp.int32, (tokens, tokens), 1)
        expert = lax.broadcasted_iota(jnp.int32, (pairs, tokens), 0) * 2 + place_ref[2]
        named = jnp.zeros((pairs, tokens), jnp.float32)
        for k in range(TOP_K):
            named = named + (routes_t_ref[k : k + 1, :] == expert).astype(jnp.float32)
        earlier = dot(named.astype(jnp.bfloat16), (first < second).astype(jnp.bfloat16))
        rank = jnp.where(named > 0.0, earlier.astype(jnp.int32), -1) - place_ref[1] * (2 * slots)
        slot = lax.broadcasted_iota(jnp.int32, (pairs, 2 * slots, tokens), 1)
        chosen = (rank[:, None, :] == slot).astype(jnp.float32)
        chosen = chosen.reshape(experts * slots, tokens).astype(jnp.bfloat16)
        out_ref[...] = dot(chosen, normed).astype(jnp.bfloat16)
        column = lax.broadcasted_iota(jnp.int32, (tokens, experts), 1)
        marks = [(routes_ref[:, k : k + 1] == column).astype(jnp.float32) for k in range(TOP_K)]
        before = dot((second < first).astype(jnp.bfloat16), sum(marks).astype(jnp.bfloat16))
        before = before.astype(jnp.int32)
        core, half, spot = (before // slots) % 2, before // (2 * slots), before % slots
        position = (((column // 2) * 2 + core) * 2 + half) * 2 + column % 2
        position = (position * slots + spot).astype(jnp.float32)
        target_ref[...] = jnp.concatenate(
            [jnp.sum(mark * position, axis=1, keepdims=True) for mark in marks], axis=1
        ).astype(jnp.int32)

    vmem = pl.BlockSpec(memory_space=pltpu.VMEM)
    return pl.pallas_call(
        kernel,
        out_shape=(
            jax.ShapeDtypeStruct((experts * slots, width), jnp.bfloat16),
            jax.ShapeDtypeStruct((tokens, TOP_K), jnp.int32),
        ),
        in_specs=[pl.BlockSpec(memory_space=pltpu.SMEM)] + [vmem] * 4,
        out_specs=(vmem, vmem),
        name="dispatch",
    )(place, rows, gain[None, :], routes, routes.T)


def device_pairs(where):
    names = list(itertools.product(range(2), repeat=5))
    number = {name: i for i, name in enumerate(names)}
    return [(number[n], number[where(*n)]) for n in names if where(*n) is not None]


def gather_shares(own):
    axes = ("ep_1", "Y", "h", "X", "p")

    def outer(c, Y, h, X, p):
        return (c, Y, 1 - h, X, p) if c == p else (1 - c, Y, h, X, 1 - p)

    def cross(c, Y, h, X, p):
        return (1 - c, Y, h, X, p) if c == p else (c, Y, 1 - h, X, 1 - p)

    def trade(c, Y, h, X, p):
        return (1 - c, Y, h, X, p)

    def give(c, Y, h, X, p):
        return (1 - c, Y, h, X, p) if c == p else None

    first = lax.ppermute(own, axes, device_pairs(outer))
    second = lax.ppermute(own, axes, device_pairs(cross))
    third = lax.ppermute(first, axes, device_pairs(trade))
    fourth = lax.ppermute(second, axes, device_pairs(give))
    return own, first, second, third, fourth


def share_order(native, h, p):
    own, up = 2 * h + p, 2 * (1 - h) + p
    side, across = 2 * h + (1 - p), 2 * (1 - h) + (1 - p)
    return [own, jnp.where(native, up, side), across, jnp.where(native, side, up)]


def share_copies(order_ref, shares, index, start, size, target, sem):
    own, first, second, third, fourth = shares
    rows = pl.ds(start, size)
    native = order_ref[4] == 1
    if index in (1, 3):
        source = first if index == 1 else third
        pltpu.make_async_copy(source.at[rows], target, sem).start()
        return
    here, there = (own, second) if index == 0 else (second, fourth)

    @pl.when(native)
    def _():
        pltpu.make_async_copy(here.at[rows], target, sem).start()

    @pl.when(jnp.logical_not(native))
    def _():
        pltpu.make_async_copy(there.at[rows], target, sem).start()


def gated(order, rows, shares):
    parts, n, k = rows.shape
    u = shares[0].shape[1]
    whole = parts * k

    def kernel(order_ref, rows_ref, *refs):
        shares, (out_ref, weights_ref, sems) = refs[:5], refs[5:]
        targets = [
            (weights_ref.at[i, :, pl.ds(side * u, u)], sems.at[i, side])
            for i in range(4)
            for side in range(2)
        ]
        for i in range(4):
            for side in range(2):
                target, sem = targets[2 * i + side]
                share_copies(order_ref, shares, i, side * whole, whole, target, sem)
        for i in range(4):
            for side in range(2):
                target, sem = targets[2 * i + side]
                pltpu.make_async_copy(shares[1].at[pl.ds(0, whole)], target, sem).wait()
            total = dot(rows_ref[0], weights_ref[i, :k, :])
            for part in range(1, parts):
                total = total + dot(rows_ref[part], weights_ref[i, part * k : (part + 1) * k, :])
            hidden = activate(total[:, :u], total[:, u:])
            lane = pl.multiple_of(order_ref[i] * u, u)
            for copy in range(parts):
                out_ref[copy, :, pl.ds(lane, u)] = hidden

    vmem = pl.BlockSpec(memory_space=pltpu.VMEM)
    anywhere = pl.BlockSpec(memory_space=pl.ANY)
    return pl.pallas_call(
        kernel,
        out_shape=jax.ShapeDtypeStruct((parts, n, 4 * u), jnp.bfloat16),
        in_specs=[pl.BlockSpec(memory_space=pltpu.SMEM), vmem] + [anywhere] * 5,
        out_specs=vmem,
        scratch_shapes=[
            pltpu.VMEM((4, whole, 2 * u), jnp.bfloat16),
            pltpu.SemaphoreType.DMA((4, 2)),
        ],
        name="gated",
    )(order, rows, *shares)


def lowered(order, hidden, shares):
    parts, n, k = hidden.shape
    f = shares[0].shape[1]
    whole = parts * k
    half = k // 2

    def kernel(order_ref, hidden_ref, *refs):
        shares, (out_ref, weights_ref, sems) = refs[:5], refs[5:]
        targets = [
            (weights_ref.at[i // 2, :, pl.ds((i % 2) * f, f)], sems.at[i]) for i in range(4)
        ]
        for i in range(4):
            share_copies(order_ref, shares, i, 2 * whole, whole, *targets[i])
        for pair in range(2):
            for i in (2 * pair, 2 * pair + 1):
                pltpu.make_async_copy(shares[1].at[pl.ds(0, whole)], *targets[i]).wait()
            total = jnp.zeros((n, 2 * f), jnp.float32)
            for Y, X, h in itertools.product(range(2), repeat=3):
                unit = (8 * Y + 4 * h + 2 * X) * f
                piece = hidden_ref[2 * Y + X, :, h * half : (h + 1) * half]
                total = total + dot(piece, weights_ref[pair, unit : unit + half, :])
            rounded = total.astype(jnp.bfloat16)
            out_ref[order_ref[2 * pair]] = rounded[:, :f]
            out_ref[order_ref[2 * pair + 1]] = rounded[:, f:]

    vmem = pl.BlockSpec(memory_space=pltpu.VMEM)
    anywhere = pl.BlockSpec(memory_space=pl.ANY)
    return pl.pallas_call(
        kernel,
        out_shape=jax.ShapeDtypeStruct((4, n, f), jnp.bfloat16),
        in_specs=[pl.BlockSpec(memory_space=pltpu.SMEM), vmem] + [anywhere] * 5,
        out_specs=vmem,
        scratch_shapes=[
            pltpu.VMEM((2, whole, 2 * f), jnp.bfloat16),
            pltpu.SemaphoreType.DMA((4,)),
        ],
        name="lowered",
    )(order, hidden, *shares)


def combine(results, target, logits):
    slots, f = results.shape
    tokens = target.shape[0]

    def kernel(results_ref, target_ref, logits_ref, out_ref):
        chances = jax.nn.softmax(logits_ref[...], axis=-1)
        lane = lax.broadcasted_iota(jnp.int32, (tokens, slots), 1)
        total = jnp.zeros((tokens, f), jnp.float32)
        for k in range(TOP_K):
            chosen = (target_ref[:, k : k + 1] == lane).astype(jnp.float32).astype(jnp.bfloat16)
            total = total + dot(chosen, results_ref[...]) * chances[:, k : k + 1]
        out_ref[...] = total.astype(jnp.bfloat16)

    vmem = pl.BlockSpec(memory_space=pltpu.VMEM)
    return pl.pallas_call(
        kernel,
        out_shape=jax.ShapeDtypeStruct((tokens, f), jnp.bfloat16),
        in_specs=[vmem] * 3,
        out_specs=vmem,
        name="combine",
    )(results, target, logits)


def ring(shard, axes):
    size = lax.axis_size(axes)
    others = [
        lax.ppermute(shard, axes, [(i, (i + k) % size) for i in range(size)]) for k in range(1, size)
    ]
    return jnp.stack([shard] + others)


def projected(heads, weight, place):
    down, across, n, j = heads.shape
    f = weight.shape[1]

    def kernel(place_ref, heads_ref, weight_ref, out_ref):
        total = jnp.zeros((n, f), jnp.float32)
        for a in range(down):
            for b in range(across):
                y = (place_ref[0] + down - a) % down
                x = (place_ref[1] + across - b) % across
                unit = pl.multiple_of((y * across + x) * j, j)
                total = total + dot(heads_ref[a, b], weight_ref[pl.ds(unit, j), :])
        out_ref[...] = total.astype(jnp.bfloat16)

    vmem = pl.BlockSpec(memory_space=pltpu.VMEM)
    return pl.pallas_call(
        kernel,
        out_shape=jax.ShapeDtypeStruct((n, f), jnp.bfloat16),
        in_specs=[pl.BlockSpec(memory_space=pltpu.SMEM), vmem, vmem],
        out_specs=vmem,
        name="projected",
    )(place, heads, weight)


def attention(mixer_input, mixer_gain, query_weight, key_weight, value_weight, sink_logit):
    tokens = mixer_input.shape[0]
    query_heads = query_weight.shape[1] // HEAD_DIM
    key_heads = key_weight.shape[1] // HEAD_DIM
    group = query_heads // key_heads
    blocks = tokens // WINDOW
    offset = lax.axis_index(EP) * tokens
    length = lax.axis_size(EP) * tokens
    places = offset + jnp.arange(tokens, dtype=jnp.int32)
    normed = normalize(mixer_input, mixer_gain)
    query = dot(normed, query_weight).reshape(tokens, query_heads, HEAD_DIM)
    query = (
        axial_rope(query, places)
        .astype(jnp.bfloat16)
        .reshape(blocks, WINDOW, key_heads, group, HEAD_DIM)
    )
    keys = dot(normed, key_weight).reshape(tokens, key_heads, HEAD_DIM)
    keys = axial_rope(keys, places).astype(jnp.bfloat16).reshape(tokens, key_heads * HEAD_DIM)
    values = dot(normed, value_weight).astype(jnp.bfloat16)
    stacked = jnp.concatenate([keys, values], axis=1)
    widened = extended(stacked, EP, WINDOW)
    framed = widened.reshape(blocks + 2, WINDOW, 2, key_heads, HEAD_DIM)
    nearby = jnp.concatenate([framed[:-2], framed[1:-1], framed[2:]], axis=1)
    scores = jnp.einsum(
        "nqgrd,nkgd->ngrqk", query, nearby[:, :, 0], preferred_element_type=jnp.float32
    ) * HEAD_DIM ** (-0.5)
    query_place = places.reshape(blocks, WINDOW)
    key_place = (
        offset
        + (jnp.arange(blocks, dtype=jnp.int32)[:, None] - 1) * WINDOW
        + jnp.arange(3 * WINDOW, dtype=jnp.int32)[None, :]
    )
    allowed = (
        (jnp.abs(query_place[:, :, None] - key_place[:, None, :]) <= WINDOW)
        & (key_place[:, None, :] >= 0)
        & (key_place[:, None, :] < length)
    )
    scores = jnp.where(allowed[:, None, None], scores, -1e30)
    sinks = sink_logit.reshape(key_heads, group)[None, :, :, None]
    top = jnp.maximum(jnp.max(scores, axis=-1), sinks)
    weights = jnp.exp(scores - top[..., None])
    denominator = jnp.sum(weights, axis=-1) + jnp.exp(sinks - top)
    shares = (weights / denominator[..., None]).astype(jnp.bfloat16)
    mixed = jnp.einsum(
        "ngrqk,nkgd->nqgrd", shares, nearby[:, :, 1], preferred_element_type=jnp.float32
    )
    return mixed.astype(jnp.bfloat16).reshape(tokens, query_heads * HEAD_DIM)


def shards(
    mixer_input,
    mixer_gain,
    query_weight,
    key_weight,
    value_weight,
    output_weight,
    sink_logit,
    expert_input,
    expert_gain,
    routes,
    route_logits,
    gate_weight,
    up_weight,
    down_weight,
):
    experts = lax.axis_size(EP)
    rows_here, features = expert_input.shape
    slots = 2 * rows_here * TOP_K // experts // 4
    width = features // 4
    c, p, h = (lax.axis_index(a) for a in ("ep_1", "p", "h"))
    native = c == p
    block = 2 * lax.axis_index("Y") + lax.axis_index("X")
    place = jnp.stack([block, h, p]).astype(jnp.int32)
    order = jnp.stack([*share_order(native, h, p), native]).astype(jnp.int32)
    spot = jnp.stack([lax.axis_index(("Y", "h")), lax.axis_index(("X", "p"))]).astype(jnp.int32)

    shares = gather_shares(jnp.concatenate([gate_weight[0], up_weight[0], down_weight[0]], axis=0))
    outgoing, target = dispatch(
        expert_input, expert_gain, routes, place, experts, slots, width
    )
    received = swap(outgoing.reshape(experts, slots, width), EP)

    mixed = attention(
        mixer_input, mixer_gain, query_weight, key_weight, value_weight, sink_logit
    )
    heads = ring(ring(mixed, ("X", "p")), ("Y", "h"))
    mixer_output = projected(heads, output_weight, spot)

    rows = spread(received.reshape(experts * slots, width), ("Y", "X"))
    hidden = swap(gated(order, rows, shares), ("Y", "X"))
    result = swap(lowered(order, hidden, shares), ("h", "p"))
    result = result.reshape(4, experts, slots, -1).transpose(1, 0, 2, 3)
    returned = swap(result, EP)
    expert_output = combine(
        returned.reshape(experts * 4 * slots, -1), target, route_logits
    )
    return (mixer_output, expert_output)


def solution(mesh):
    names = ("ep_0", "ep_1", "Y", "h", "X", "p")
    finer = Mesh(mesh.devices.reshape(16, 2, 2, 2, 2, 2), names)
    in_specs = (
        P(EP, None),
        P(),
        P(None, TP),
        P(None, TP),
        P(None, TP),
        P(None, TP),
        P(TP),
        P(EP, None),
        P(),
        P(EP, None),
        P(EP, None),
        P(EP, None, TP),
        P(EP, None, TP),
        P(EP, None, TP),
    )
    out_specs = (P(EP, TP), P(EP, TP))
    return jax.shard_map(
        shards, mesh=finer, in_specs=in_specs, out_specs=out_specs, check_vma=False
    )
```

```python
import itertools

import jax
import jax.numpy as jnp
from jax import lax
from jax.experimental import pallas as pl
from jax.experimental.pallas import tpu as pltpu
from jax.sharding import Mesh
from jax.sharding import PartitionSpec as P

HEAD_DIM = 64
TOP_K = 4
WINDOW = 128
GRID_W = 64
EP = ("ep_0", "ep_1")
TP = ("Y", "h", "X", "p")

EPSILON = 1e-06
LIMIT = 7.0
SLOPE = 1.702
BASE = 10000.0


def swap(pieces, axis):
    return lax.all_to_all(pieces, axis, 0, 0, tiled=True)


def spread(shard, axis):
    return swap(jnp.broadcast_to(shard[None], (lax.axis_size(axis), *shard.shape)), axis)


def activate(gate, up):
    capped = jnp.minimum(gate, LIMIT)
    bounded = jnp.clip(up, -LIMIT, LIMIT)
    return (capped * jax.nn.sigmoid(SLOPE * capped) * (bounded + 1.0)).astype(jnp.bfloat16)


def dot(a, b):
    return jnp.dot(a, b, preferred_element_type=jnp.float32)


def tall(wide):
    k, n = wide.shape
    square = jnp.concatenate([wide, jnp.zeros((n - k, n), wide.dtype)], axis=0)
    return square.T


def dispatch(rows, gain, routes, experts, slots, width):
    tokens = rows.shape[0]
    pairs = experts // 2

    def kernel(rows_ref, gain_ref, routes_ref, out_ref, target_ref):
        block = 2 * lax.axis_index("Y") + lax.axis_index("X")
        values = rows_ref[...].astype(jnp.float32)
        scale = lax.rsqrt(jnp.mean(values * values, axis=-1, keepdims=True) + EPSILON)
        start = pl.multiple_of(block * width, width)
        own = rows_ref[:, pl.ds(start, width)].astype(jnp.float32)
        normed = (own * scale * gain_ref[:, pl.ds(start, width)]).astype(jnp.bfloat16)
        first = lax.broadcasted_iota(jnp.int32, (tokens, tokens), 0)
        second = lax.broadcasted_iota(jnp.int32, (tokens, tokens), 1)
        parity = lax.axis_index("p")
        expert = lax.broadcasted_iota(jnp.int32, (pairs, tokens), 0) * 2 + parity
        named = jnp.zeros((pairs, tokens), jnp.float32)
        for k in range(TOP_K):
            named = named + (routes_ref[k : k + 1, :] == expert).astype(jnp.float32)
        earlier = dot(named.astype(jnp.bfloat16), (first < second).astype(jnp.bfloat16))
        rank = jnp.where(named > 0.0, earlier.astype(jnp.int32), -1)
        rank = rank - lax.axis_index("h") * (2 * slots)
        slot = lax.broadcasted_iota(jnp.int32, (pairs, 2 * slots, tokens), 1)
        chosen = (rank[:, None, :] == slot).astype(jnp.float32)
        chosen = chosen.reshape(experts * slots, tokens).astype(jnp.bfloat16)
        out_ref[...] = dot(chosen, normed).astype(jnp.bfloat16)
        routed = tall(routes_ref[...].astype(jnp.float32))
        column = lax.broadcasted_iota(jnp.int32, (tokens, experts), 1)
        wanted = column.astype(jnp.float32)
        marks = [(routed[:, k : k + 1] == wanted).astype(jnp.float32) for k in range(TOP_K)]
        before = dot((second < first).astype(jnp.bfloat16), sum(marks).astype(jnp.bfloat16))
        before = before.astype(jnp.int32)
        core, half, spot = (before // slots) % 2, before // (2 * slots), before % slots
        position = (((column // 2) * 2 + core) * 2 + half) * 2 + column % 2
        position = (position * slots + spot).astype(jnp.float32)
        target_ref[...] = jnp.concatenate(
            [jnp.sum(mark * position, axis=1, keepdims=True) for mark in marks], axis=1
        ).astype(jnp.int32)

    vmem = pl.BlockSpec(memory_space=pltpu.VMEM)
    return pl.pallas_call(
        kernel,
        out_shape=(
            jax.ShapeDtypeStruct((experts * slots, width), jnp.bfloat16),
            jax.ShapeDtypeStruct((tokens, TOP_K), jnp.int32),
        ),
        in_specs=[vmem] * 3,
        out_specs=(vmem, vmem),
        name="dispatch",
    )(rows, gain[None, :], routes.T)


def device_pairs(where):
    names = list(itertools.product(range(2), repeat=5))
    number = {name: i for i, name in enumerate(names)}
    return [(number[n], number[where(*n)]) for n in names if where(*n) is not None]


def gather_shares(own):
    axes = ("ep_1", "Y", "h", "X", "p")

    def outer(c, Y, h, X, p):
        return (c, Y, 1 - h, X, p) if c == p else (1 - c, Y, h, X, 1 - p)

    def cross(c, Y, h, X, p):
        return (1 - c, Y, h, X, p) if c == p else (c, Y, 1 - h, X, 1 - p)

    def trade(c, Y, h, X, p):
        return (1 - c, Y, h, X, p)

    def give(c, Y, h, X, p):
        return (1 - c, Y, h, X, p) if c == p else None

    first = lax.ppermute(own, axes, device_pairs(outer))
    second = lax.ppermute(own, axes, device_pairs(cross))
    third = lax.ppermute(first, axes, device_pairs(trade))
    fourth = lax.ppermute(second, axes, device_pairs(give))
    return own, first, second, third, fourth


def share_order():
    c, h, p = (lax.axis_index(a) for a in ("ep_1", "h", "p"))
    native = c == p
    own, up = 2 * h + p, 2 * (1 - h) + p
    side, across = 2 * h + (1 - p), 2 * (1 - h) + (1 - p)
    return native, [own, jnp.where(native, up, side), across, jnp.where(native, side, up)]


def copy_share(native, shares, index, start, size, target, sem):
    own, first, second, third, fourth = shares
    rows = pl.ds(start, size)
    if index in (1, 3):
        source = first if index == 1 else third
        pltpu.make_async_copy(source.at[rows], target, sem).start()
        return
    here, there = (own, second) if index == 0 else (second, fourth)

    @pl.when(native)
    def _():
        pltpu.make_async_copy(here.at[rows], target, sem).start()

    @pl.when(jnp.logical_not(native))
    def _():
        pltpu.make_async_copy(there.at[rows], target, sem).start()


def gated(rows, mixed, shares):
    parts, n, k = rows.shape
    u = shares[0].shape[1]
    j = mixed.shape[1]
    whole = parts * k

    def kernel(rows_ref, mixed_ref, *refs):
        shares, (out_ref, weights_ref, sems) = refs[:5], refs[5:]
        native, order = share_order()
        targets = [
            (weights_ref.at[i, :, pl.ds(side * u, u)], sems.at[i, side])
            for i in range(4)
            for side in range(2)
        ]
        for i in range(4):
            for side in range(2):
                target, sem = targets[2 * i + side]
                copy_share(native, shares, i, side * whole, whole, target, sem)
        for copy in range(parts):
            out_ref[copy, :, 4 * u :] = mixed_ref[...]
        for i in range(4):
            for side in range(2):
                target, sem = targets[2 * i + side]
                pltpu.make_async_copy(shares[1].at[pl.ds(0, whole)], target, sem).wait()
            total = dot(rows_ref[0], weights_ref[i, :k, :])
            for part in range(1, parts):
                total = total + dot(rows_ref[part], weights_ref[i, part * k : (part + 1) * k, :])
            hidden = activate(total[:, :u], total[:, u:])
            lane = pl.multiple_of(order[i] * u, u)
            for copy in range(parts):
                out_ref[copy, :, pl.ds(lane, u)] = hidden

    vmem = pl.BlockSpec(memory_space=pltpu.VMEM)
    anywhere = pl.BlockSpec(memory_space=pl.ANY)
    return pl.pallas_call(
        kernel,
        out_shape=jax.ShapeDtypeStruct((parts, n, 4 * u + j), jnp.bfloat16),
        in_specs=[vmem, vmem] + [anywhere] * 5,
        out_specs=vmem,
        scratch_shapes=[
            pltpu.VMEM((4, whole, 2 * u), jnp.bfloat16),
            pltpu.SemaphoreType.DMA((4, 2)),
        ],
        name="gated",
    )(rows, mixed, *shares)


def lowered(hidden, shares, slots):
    parts, n, _ = hidden.shape
    f = shares[0].shape[1]
    k = 4 * f
    whole = parts * k
    half = k // 2

    def kernel(hidden_ref, *refs):
        shares, (out_ref, weights_ref, sems) = refs[:5], refs[5:]
        native, order = share_order()
        targets = [
            (weights_ref.at[i // 2, :, pl.ds((i % 2) * f, f)], sems.at[i]) for i in range(4)
        ]
        for i in range(4):
            copy_share(native, shares, i, 2 * whole, whole, *targets[i])
        for pair in range(2):
            for i in (2 * pair, 2 * pair + 1):
                pltpu.make_async_copy(shares[1].at[pl.ds(0, whole)], *targets[i]).wait()
            total = jnp.zeros((n, 2 * f), jnp.float32)
            for Y, X, h in itertools.product(range(2), repeat=3):
                unit = (8 * Y + 4 * h + 2 * X) * f
                piece = hidden_ref[2 * Y + X, :, h * half : (h + 1) * half]
                total = total + dot(piece, weights_ref[pair, unit : unit + half, :])
            rounded = total.astype(jnp.bfloat16).reshape(n // slots, slots, 2 * f)
            out_ref[:, order[2 * pair]] = rounded[:, :, :f]
            out_ref[:, order[2 * pair + 1]] = rounded[:, :, f:]

    vmem = pl.BlockSpec(memory_space=pltpu.VMEM)
    anywhere = pl.BlockSpec(memory_space=pl.ANY)
    return pl.pallas_call(
        kernel,
        out_shape=jax.ShapeDtypeStruct((n // slots, 4, slots, f), jnp.bfloat16),
        in_specs=[vmem] + [anywhere] * 5,
        out_specs=vmem,
        scratch_shapes=[
            pltpu.VMEM((2, whole, 2 * f), jnp.bfloat16),
            pltpu.SemaphoreType.DMA((4,)),
        ],
        name="lowered",
    )(hidden, *shares)


def combine(results, target, chances):
    slots, f = results.shape
    tokens = target.shape[0]

    def kernel(results_ref, target_ref, chances_ref, out_ref):
        chances = tall(chances_ref[...])
        lane = lax.broadcasted_iota(jnp.int32, (tokens, slots), 1)
        total = jnp.zeros((tokens, f), jnp.float32)
        for k in range(TOP_K):
            chosen = (target_ref[:, k : k + 1] == lane).astype(jnp.float32).astype(jnp.bfloat16)
            total = total + dot(chosen, results_ref[...]) * chances[:, k : k + 1]
        out_ref[...] = total.astype(jnp.bfloat16)

    vmem = pl.BlockSpec(memory_space=pltpu.VMEM)
    return pl.pallas_call(
        kernel,
        out_shape=jax.ShapeDtypeStruct((tokens, f), jnp.bfloat16),
        in_specs=[vmem] * 3,
        out_specs=vmem,
        name="combine",
    )(results, target, chances)


def rotary_tables(places, width):
    quarter = HEAD_DIM // 4
    lane = jnp.arange(width, dtype=jnp.int32)
    frequency = BASE ** (-(lane % quarter).astype(jnp.float32) / quarter)
    row = (places // GRID_W).astype(jnp.float32)[:, None]
    column = (places % GRID_W).astype(jnp.float32)[:, None]
    angle = jnp.where(lane % HEAD_DIM < HEAD_DIM // 2, row, column) * frequency
    sign = jnp.where(lane % (2 * quarter) < quarter, -1.0, 1.0)
    return jnp.cos(angle), jnp.sin(angle) * sign


def projections(rows, gain, query_weight, key_weight, value_weight, places):
    tokens, _ = rows.shape
    width = query_weight.shape[1]
    half = width // 2
    quarter = HEAD_DIM // 4
    cosine, sine = rotary_tables(places, width)

    def kernel(
        rows_ref, gain_ref, query_ref, key_ref, value_ref, cos_ref, sin_ref, out_ref, *pair_refs
    ):
        values = rows_ref[...].astype(jnp.float32)
        scale = lax.rsqrt(jnp.mean(values * values, axis=-1, keepdims=True) + EPSILON)
        normed = (values * scale * gain_ref[...]).astype(jnp.bfloat16)
        lane = lax.broadcasted_iota(jnp.int32, (tokens, width), 1) % (2 * quarter)

        def turned(a):
            partner = jnp.where(
                lane < quarter,
                pltpu.roll(a, width - quarter, 1),
                pltpu.roll(a, quarter, 1),
            )
            return (a * cos_ref[...] + partner * sin_ref[...]).astype(jnp.bfloat16)

        def flipped(weight_ref):
            return lax.dot_general(
                normed, weight_ref[...], (((1,), (1,)), ((), ())), preferred_element_type=jnp.float32
            )

        out_ref[...] = turned(dot(normed, query_ref[...]))
        keys, mine = flipped(key_ref), flipped(value_ref)
        both = jnp.concatenate([keys, mine], axis=1)
        rounded = jnp.where(
            lax.broadcasted_iota(jnp.int32, (tokens, width), 1) < half,
            turned(both),
            both.astype(jnp.bfloat16),
        )
        for i, ref in enumerate(pair_refs):
            ref[...] = rounded[i * WINDOW : (i + 1) * WINDOW]

    vmem = pl.BlockSpec(memory_space=pltpu.VMEM)
    return pl.pallas_call(
        kernel,
        out_shape=[jax.ShapeDtypeStruct((tokens, width), jnp.bfloat16)]
        + [jax.ShapeDtypeStruct((WINDOW, width), jnp.bfloat16)] * (tokens // WINDOW),
        in_specs=[vmem] * 7,
        out_specs=[vmem] * (1 + tokens // WINDOW),
        name="projections",
    )(rows, gain[None, :], query_weight, key_weight.T, value_weight.T, cosine, sine)


def banded(query, pieces, sinks):
    tokens, width = query.shape
    blocks = tokens // WINDOW
    heads = width // HEAD_DIM

    def kernel(sink_ref, query_ref, *refs):
        piece_refs, out_ref = refs[:-1], refs[-1]
        place, last = lax.axis_index(EP), lax.axis_size(EP) - 1
        row = lax.broadcasted_iota(jnp.int32, (WINDOW, 3 * WINDOW), 0)
        column = lax.broadcasted_iota(jnp.int32, (WINDOW, 3 * WINDOW), 1)
        band = (column >= row) & (column <= row + 2 * WINDOW)
        for n in range(blocks):
            near = jnp.concatenate([piece_refs[n + i][...] for i in range(3)], axis=0)
            keys, values = near[:, :HEAD_DIM], near[:, HEAD_DIM:]
            least = jnp.where(place == 0, WINDOW, 0) if n == 0 else 0
            most = jnp.where(place == last, 2 * WINDOW, 3 * WINDOW) if n == blocks - 1 else 3 * WINDOW
            allowed = band & (column >= least) & (column < most)
            outs = []
            for r in range(heads):
                here = query_ref[n * WINDOW : (n + 1) * WINDOW, r * HEAD_DIM : (r + 1) * HEAD_DIM]
                scores = lax.dot_general(
                    here, keys, (((1,), (1,)), ((), ())), preferred_element_type=jnp.float32
                )
                scores = jnp.where(allowed, scores * HEAD_DIM ** (-0.5), -1e30)
                sink = sink_ref[r]
                top = jnp.maximum(jnp.max(scores, axis=-1, keepdims=True), sink)
                weights = jnp.exp(scores - top)
                total = jnp.sum(weights, axis=-1, keepdims=True) + jnp.exp(sink - top)
                outs.append(dot((weights / total).astype(jnp.bfloat16), values))
            mixed = jnp.concatenate(outs, axis=1).astype(jnp.bfloat16)
            out_ref[n * WINDOW : (n + 1) * WINDOW, :] = mixed

    vmem = pl.BlockSpec(memory_space=pltpu.VMEM)
    return pl.pallas_call(
        kernel,
        out_shape=jax.ShapeDtypeStruct((tokens, width), jnp.bfloat16),
        in_specs=[pl.BlockSpec(memory_space=pltpu.SMEM)] + [vmem] * (blocks + 3),
        out_specs=vmem,
        name="banded",
    )(sinks, query, *pieces)


def attention(mixer_input, mixer_gain, query_weight, key_weight, value_weight, sink_logit):
    tokens = mixer_input.shape[0]
    places = lax.axis_index(EP) * tokens + jnp.arange(tokens, dtype=jnp.int32)
    query, *pieces = projections(
        mixer_input, mixer_gain, query_weight, key_weight, value_weight, places
    )
    up = [(i, i + 1) for i in range(lax.axis_size(EP) - 1)]
    before = lax.ppermute(pieces[-1], EP, up)
    after = lax.ppermute(pieces[0], EP, [(j, i) for i, j in up])
    return banded(query, [before, *pieces, after], sink_logit)


def projected(heads, weight):
    _, n, j = heads[0].shape
    f = weight.shape[1]

    def kernel(*refs):
        heads_refs, weight_ref, out_ref = refs[:4], refs[4], refs[5]
        total = jnp.zeros((n, f), jnp.float32)
        for k in range(4):
            h, p = lax.axis_index("h") ^ (k // 2), lax.axis_index("p") ^ (k % 2)
            for Y, X in itertools.product(range(2), repeat=2):
                unit = pl.multiple_of((8 * Y + 4 * h + 2 * X + p) * j, j)
                total = total + dot(heads_refs[k][2 * Y + X], weight_ref[pl.ds(unit, j), :])
        out_ref[...] = total.astype(jnp.bfloat16)

    vmem = pl.BlockSpec(memory_space=pltpu.VMEM)
    return pl.pallas_call(
        kernel,
        out_shape=jax.ShapeDtypeStruct((n, f), jnp.bfloat16),
        in_specs=[vmem] * 5,
        out_specs=vmem,
        name="projected",
    )(*heads, weight)


def shards(
    mixer_input,
    mixer_gain,
    query_weight,
    key_weight,
    value_weight,
    output_weight,
    sink_logit,
    expert_input,
    expert_gain,
    routes,
    route_logits,
    gate_weight,
    up_weight,
    down_weight,
):
    experts = lax.axis_size(EP)
    rows_here, features = expert_input.shape
    slots = 2 * rows_here * TOP_K // experts // 4
    width = features // 4
    own = jnp.concatenate([gate_weight[0], up_weight[0], down_weight[0]], axis=0)
    shares = gather_shares(own)
    outgoing, target = dispatch(expert_input, expert_gain, routes, experts, slots, width)
    received = swap(outgoing.reshape(experts, slots, width), EP)
    mixed = attention(mixer_input, mixer_gain, query_weight, key_weight, value_weight, sink_logit)
    rows = spread(received.reshape(experts * slots, width), ("Y", "X"))
    inner = gated(rows, mixed, shares)
    beside = swap(inner, ("Y", "X"))
    chances = jax.nn.softmax(route_logits.T, axis=0)
    result = lowered(beside, shares, slots)
    returned = swap(result.reshape(4 * experts, slots, -1), (*EP, "h", "p"))
    heads = beside[:, :, width:]
    heads = [heads] + [
        lax.ppermute(heads, ("h", "p"), [(i, i ^ k) for i in range(4)])
        for k in range(1, 4)
    ]
    mixer_output = projected(heads, output_weight)
    expert_output = combine(
        returned.reshape(experts * 4 * slots, -1), target, chances
    )
    return (mixer_output, expert_output)


def solution(mesh):
    names = ("ep_0", "ep_1", "Y", "h", "X", "p")
    finer = Mesh(mesh.devices.reshape(16, 2, 2, 2, 2, 2), names)
    in_specs = (
        P(EP, None),
        P(),
        P(None, TP),
        P(None, TP),
        P(None, TP),
        P(None, TP),
        P(TP),
        P(EP, None),
        P(),
        P(EP, None),
        P(EP, None),
        P(EP, None, TP),
        P(EP, None, TP),
        P(EP, None, TP),
    )
    out_specs = (P(EP, TP), P(EP, TP))
    return jax.shard_map(
        shards, mesh=finer, in_specs=in_specs, out_specs=out_specs, check_vma=False
    )
```

```python
import itertools

import jax
import jax.numpy as jnp
from jax import lax
from jax.experimental import pallas as pl
from jax.experimental.pallas import tpu as pltpu
from jax.sharding import Mesh
from jax.sharding import PartitionSpec as P

HEAD_DIM = 64
TOP_K = 4
WINDOW = 128
GRID_W = 64
EP = ("ep_0", "ep_1")
TP = ("Y", "h", "X", "p")

EPSILON = 1e-06
LIMIT = 7.0
SLOPE = 1.702
BASE = 10000.0


def swap(pieces, axis):
    return lax.all_to_all(pieces, axis, 0, 0, tiled=True)


def spread(shard, axis):
    return swap(jnp.broadcast_to(shard[None], (lax.axis_size(axis), *shard.shape)), axis)


def activate(gate, up):
    capped = jnp.minimum(gate, LIMIT)
    bounded = jnp.clip(up, -LIMIT, LIMIT)
    return (capped * jax.nn.sigmoid(SLOPE * capped) * (bounded + 1.0)).astype(jnp.bfloat16)


def dot(a, b):
    return jnp.dot(a, b, preferred_element_type=jnp.float32)


def tall(wide):
    k, n = wide.shape
    square = jnp.concatenate([wide, jnp.zeros((n - k, n), wide.dtype)], axis=0)
    return square.T


def dispatch(rows, gain, routes, weights, experts, slots, width):
    tokens = rows.shape[0]
    pairs = experts // 2
    tall_rows, columns = weights[0].shape

    def kernel(rows_ref, gain_ref, routes_ref, *refs):
        weight_refs, (out_ref, target_ref, stacked_ref, sems) = refs[:3], refs[3:]
        copies = [
            pltpu.make_async_copy(
                ref, stacked_ref.at[pl.ds(i * tall_rows, tall_rows)], sems.at[i]
            )
            for i, ref in enumerate(weight_refs)
        ]
        for copy in copies:
            copy.start()
        block = 2 * lax.axis_index("Y") + lax.axis_index("X")
        values = rows_ref[...].astype(jnp.float32)
        scale = lax.rsqrt(jnp.mean(values * values, axis=-1, keepdims=True) + EPSILON)
        start = pl.multiple_of(block * width, width)
        own = rows_ref[:, pl.ds(start, width)].astype(jnp.float32)
        normed = (own * scale * gain_ref[:, pl.ds(start, width)]).astype(jnp.bfloat16)
        first = lax.broadcasted_iota(jnp.int32, (tokens, tokens), 0)
        second = lax.broadcasted_iota(jnp.int32, (tokens, tokens), 1)
        parity = lax.axis_index("p")
        expert = lax.broadcasted_iota(jnp.int32, (pairs, tokens), 0) * 2 + parity
        named = jnp.zeros((pairs, tokens), jnp.float32)
        for k in range(TOP_K):
            named = named + (routes_ref[k : k + 1, :] == expert).astype(jnp.float32)
        earlier = dot(named.astype(jnp.bfloat16), (first < second).astype(jnp.bfloat16))
        rank = jnp.where(named > 0.0, earlier.astype(jnp.int32), -1)
        rank = rank - lax.axis_index("h") * (2 * slots)
        slot = lax.broadcasted_iota(jnp.int32, (pairs, 2 * slots, tokens), 1)
        chosen = (rank[:, None, :] == slot).astype(jnp.float32)
        chosen = chosen.reshape(experts * slots, tokens).astype(jnp.bfloat16)
        out_ref[...] = dot(chosen, normed).astype(jnp.bfloat16)
        routed = tall(routes_ref[...].astype(jnp.float32))
        column = lax.broadcasted_iota(jnp.int32, (tokens, experts), 1)
        wanted = column.astype(jnp.float32)
        marks = [(routed[:, k : k + 1] == wanted).astype(jnp.float32) for k in range(TOP_K)]
        before = dot((second < first).astype(jnp.bfloat16), sum(marks).astype(jnp.bfloat16))
        before = before.astype(jnp.int32)
        core, half, spot = (before // slots) % 2, before // (2 * slots), before % slots
        position = (((column // 2) * 2 + core) * 2 + half) * 2 + column % 2
        position = (position * slots + spot).astype(jnp.float32)
        target_ref[...] = jnp.concatenate(
            [jnp.sum(mark * position, axis=1, keepdims=True) for mark in marks], axis=1
        ).astype(jnp.int32)
        for copy in copies:
            copy.wait()

    vmem = pl.BlockSpec(memory_space=pltpu.VMEM)
    anywhere = pl.BlockSpec(memory_space=pl.ANY)
    return pl.pallas_call(
        kernel,
        out_shape=(
            jax.ShapeDtypeStruct((experts * slots, width), jnp.bfloat16),
            jax.ShapeDtypeStruct((tokens, TOP_K), jnp.int32),
            jax.ShapeDtypeStruct((3 * tall_rows, columns), jnp.bfloat16),
        ),
        in_specs=[vmem] * 3 + [anywhere] * 3,
        out_specs=(vmem, vmem, anywhere),
        scratch_shapes=[pltpu.SemaphoreType.DMA((3,))],
        name="dispatch",
    )(rows, gain[None, :], routes.T, *weights)


def device_pairs(where):
    names = list(itertools.product(range(2), repeat=5))
    number = {name: i for i, name in enumerate(names)}
    return [(number[n], number[where(*n)]) for n in names if where(*n) is not None]


def gather_shares(own):
    axes = ("ep_1", "Y", "h", "X", "p")

    def outer(c, Y, h, X, p):
        return (c, Y, 1 - h, X, p) if c == p else (1 - c, Y, h, X, 1 - p)

    def cross(c, Y, h, X, p):
        return (1 - c, Y, h, X, p) if c == p else (c, Y, 1 - h, X, 1 - p)

    def trade(c, Y, h, X, p):
        return (1 - c, Y, h, X, p)

    def give(c, Y, h, X, p):
        return (1 - c, Y, h, X, p) if c == p else None

    first = lax.ppermute(own, axes, device_pairs(outer))
    second = lax.ppermute(own, axes, device_pairs(cross))
    third = lax.ppermute(first, axes, device_pairs(trade))
    fourth = lax.ppermute(second, axes, device_pairs(give))
    return own, first, second, third, fourth


def share_order():
    c, h, p = (lax.axis_index(a) for a in ("ep_1", "h", "p"))
    native = c == p
    own, up = 2 * h + p, 2 * (1 - h) + p
    side, across = 2 * h + (1 - p), 2 * (1 - h) + (1 - p)
    return native, [own, jnp.where(native, up, side), across, jnp.where(native, side, up)]


def copy_share(native, shares, index, start, size, target, sem):
    own, first, second, third, fourth = shares
    rows = pl.ds(start, size)
    if index in (1, 3):
        source = first if index == 1 else third
        pltpu.make_async_copy(source.at[rows], target, sem).start()
        return
    here, there = (own, second) if index == 0 else (second, fourth)

    @pl.when(native)
    def _():
        pltpu.make_async_copy(here.at[rows], target, sem).start()

    @pl.when(jnp.logical_not(native))
    def _():
        pltpu.make_async_copy(there.at[rows], target, sem).start()


def gated(rows, shares, arrived):
    parts, n, wide = rows.shape
    u = shares[0].shape[1]
    k = 4 * u
    j = wide - k
    whole = parts * k

    def kernel(rows_ref, _, *refs):
        shares, refs = refs[:5], refs[5:]
        out_ref, heads_ref, here_ref, weights_ref, hidden_ref, sems, row_sems, out_sems = refs
        native, order = share_order()
        arrivals = [
            pltpu.make_async_copy(
                rows_ref.at[part, :, pl.ds(0, k)], here_ref.at[part], row_sems.at[part]
            )
            for part in range(parts)
        ]
        heads = pltpu.make_async_copy(
            rows_ref.at[:, :, pl.ds(k, j)], heads_ref, row_sems.at[parts]
        )
        targets = [
            (weights_ref.at[i, :, pl.ds(side * u, u)], sems.at[i, side])
            for i in range(4)
            for side in range(2)
        ]

        def fetch(i):
            for side in range(2):
                target, sem = targets[2 * i + side]
                copy_share(native, shares, i, side * whole, whole, target, sem)

        for part in range(parts):
            arrivals[part].start()
        for i in range(4):
            fetch(i)
        heads.start()
        for part in range(parts):
            arrivals[part].wait()
        leaving = []
        for i in range(4):
            for side in range(2):
                target, sem = targets[2 * i + side]
                pltpu.make_async_copy(shares[1].at[pl.ds(0, whole)], target, sem).wait()
            total = dot(here_ref[0], weights_ref[i, :k, :])
            for part in range(1, parts):
                total = total + dot(here_ref[part], weights_ref[i, part * k : (part + 1) * k, :])
            hidden_ref[i] = activate(total[:, :u], total[:, u:])
            lane = pl.multiple_of(order[i] * u, u)
            for copy in range(parts):
                out = out_ref.at[copy, :, pl.ds(lane, u)]
                leaving.append(
                    pltpu.make_async_copy(hidden_ref.at[i], out, out_sems.at[i, copy])
                )
                leaving[-1].start()
        for copy in leaving:
            copy.wait()
        heads.wait()

    anywhere = pl.BlockSpec(memory_space=pl.ANY)
    return pl.pallas_call(
        kernel,
        out_shape=(
            jax.ShapeDtypeStruct((parts, n, 4 * u), jnp.bfloat16),
            jax.ShapeDtypeStruct((parts, n, j), jnp.bfloat16),
        ),
        in_specs=[anywhere] * 7,
        out_specs=(anywhere, anywhere),
        scratch_shapes=[
            pltpu.VMEM((parts, n, k), jnp.bfloat16),
            pltpu.VMEM((4, whole, 2 * u), jnp.bfloat16),
            pltpu.VMEM((4, n, u), jnp.bfloat16),
            pltpu.SemaphoreType.DMA((4, 2)),
            pltpu.SemaphoreType.DMA((parts + 1,)),
            pltpu.SemaphoreType.DMA((4, parts)),
        ],
        name="gated",
    )(rows, arrived, *shares)


def lowered(hidden, shares, slots):
    parts, n, k = hidden.shape
    f = shares[0].shape[1]
    whole = parts * k
    half = k // 2

    def kernel(hidden_ref, *refs):
        shares, (out_ref, here_ref, weights_ref, sems, row_sems) = refs[:5], refs[5:]
        native, order = share_order()
        targets = [
            (weights_ref.at[i // 2, :, pl.ds((i % 2) * f, f)], sems.at[i]) for i in range(4)
        ]
        arrivals = [
            pltpu.make_async_copy(hidden_ref.at[part], here_ref.at[part], row_sems.at[part])
            for part in range(parts)
        ]
        for i in range(2):
            copy_share(native, shares, i, 2 * whole, whole, *targets[i])
        for part in range(parts):
            arrivals[part].start()
        for i in range(2, 4):
            copy_share(native, shares, i, 2 * whole, whole, *targets[i])
        for pair in range(2):
            for i in (2 * pair, 2 * pair + 1):
                pltpu.make_async_copy(shares[1].at[pl.ds(0, whole)], *targets[i]).wait()
            total = jnp.zeros((n, 2 * f), jnp.float32)
            for Y, X in itertools.product(range(2), repeat=2):
                if pair == 0:
                    arrivals[2 * Y + X].wait()
                for h in range(2):
                    unit = (8 * Y + 4 * h + 2 * X) * f
                    piece = here_ref[2 * Y + X, :, h * half : (h + 1) * half]
                    total = total + dot(piece, weights_ref[pair, unit : unit + half, :])
            rounded = total.astype(jnp.bfloat16).reshape(n // slots, slots, 2 * f)
            out_ref[:, order[2 * pair]] = rounded[:, :, :f]
            out_ref[:, order[2 * pair + 1]] = rounded[:, :, f:]

    vmem = pl.BlockSpec(memory_space=pltpu.VMEM)
    anywhere = pl.BlockSpec(memory_space=pl.ANY)
    return pl.pallas_call(
        kernel,
        out_shape=jax.ShapeDtypeStruct((n // slots, 4, slots, f), jnp.bfloat16),
        in_specs=[anywhere] * 6,
        out_specs=vmem,
        scratch_shapes=[
            pltpu.VMEM((parts, n, k), jnp.bfloat16),
            pltpu.VMEM((2, whole, 2 * f), jnp.bfloat16),
            pltpu.SemaphoreType.DMA((4,)),
            pltpu.SemaphoreType.DMA((parts,)),
        ],
        name="lowered",
    )(hidden, *shares)


def combine(results, target, chances):
    slots, f = results.shape
    tokens = target.shape[0]

    def kernel(results_ref, target_ref, chances_ref, out_ref):
        chances = tall(chances_ref[...])
        lane = lax.broadcasted_iota(jnp.int32, (tokens, slots), 1)
        chosen = [
            (target_ref[:, k : k + 1] == lane).astype(jnp.float32).astype(jnp.bfloat16)
            for k in range(TOP_K)
        ]
        picked = dot(jnp.concatenate(chosen, axis=0), results_ref[...])
        total = jnp.zeros((tokens, f), jnp.float32)
        for k in range(TOP_K):
            total = total + picked[k * tokens : (k + 1) * tokens] * chances[:, k : k + 1]
        out_ref[...] = total.astype(jnp.bfloat16)

    vmem = pl.BlockSpec(memory_space=pltpu.VMEM)
    return pl.pallas_call(
        kernel,
        out_shape=jax.ShapeDtypeStruct((tokens, f), jnp.bfloat16),
        in_specs=[vmem] * 3,
        out_specs=vmem,
        name="combine",
    )(results, target, chances)


def rotary_tables(places, width):
    quarter = HEAD_DIM // 4
    lane = jnp.arange(width, dtype=jnp.int32)
    frequency = BASE ** (-(lane % quarter).astype(jnp.float32) / quarter)
    row = (places // GRID_W).astype(jnp.float32)[:, None]
    column = (places % GRID_W).astype(jnp.float32)[:, None]
    angle = jnp.where(lane % HEAD_DIM < HEAD_DIM // 2, row, column) * frequency
    sign = jnp.where(lane % (2 * quarter) < quarter, -1.0, 1.0)
    return jnp.cos(angle), jnp.sin(angle) * sign


def projections(rows, gain, query_weight, key_weight, value_weight, places):
    tokens, _ = rows.shape
    width = query_weight.shape[1]
    half = width // 2
    quarter = HEAD_DIM // 4
    cosine, sine = rotary_tables(places, width)

    def kernel(
        rows_ref, gain_ref, query_ref, key_ref, value_ref, cos_ref, sin_ref, out_ref, *pair_refs
    ):
        values = rows_ref[...].astype(jnp.float32)
        scale = lax.rsqrt(jnp.mean(values * values, axis=-1, keepdims=True) + EPSILON)
        normed = (values * scale * gain_ref[...]).astype(jnp.bfloat16)
        lane = lax.broadcasted_iota(jnp.int32, (tokens, width), 1) % (2 * quarter)

        def turned(a):
            partner = jnp.where(
                lane < quarter,
                pltpu.roll(a, width - quarter, 1),
                pltpu.roll(a, quarter, 1),
            )
            return (a * cos_ref[...] + partner * sin_ref[...]).astype(jnp.bfloat16)

        def flipped(weight_ref):
            return lax.dot_general(
                normed, weight_ref[...], (((1,), (1,)), ((), ())), preferred_element_type=jnp.float32
            )

        out_ref[...] = turned(dot(normed, query_ref[...]))
        keys, mine = flipped(key_ref), flipped(value_ref)
        both = jnp.concatenate([keys, mine], axis=1)
        rounded = jnp.where(
            lax.broadcasted_iota(jnp.int32, (tokens, width), 1) < half,
            turned(both),
            both.astype(jnp.bfloat16),
        )
        for i, ref in enumerate(pair_refs):
            ref[...] = rounded[i * WINDOW : (i + 1) * WINDOW]

    vmem = pl.BlockSpec(memory_space=pltpu.VMEM)
    return pl.pallas_call(
        kernel,
        out_shape=[jax.ShapeDtypeStruct((tokens, width), jnp.bfloat16)]
        + [jax.ShapeDtypeStruct((WINDOW, width), jnp.bfloat16)] * (tokens // WINDOW),
        in_specs=[vmem] * 7,
        out_specs=[vmem] * (1 + tokens // WINDOW),
        name="projections",
    )(rows, gain[None, :], query_weight, key_weight.T, value_weight.T, cosine, sine)


def banded(query, pieces, sinks):
    tokens, width = query.shape
    blocks = tokens // WINDOW
    heads = width // HEAD_DIM

    def kernel(sink_ref, query_ref, *refs):
        piece_refs, out_ref = refs[:-1], refs[-1]
        place, last = lax.axis_index(EP), lax.axis_size(EP) - 1
        row = lax.broadcasted_iota(jnp.int32, (WINDOW, 3 * WINDOW), 0)
        column = lax.broadcasted_iota(jnp.int32, (WINDOW, 3 * WINDOW), 1)
        band = (column >= row) & (column <= row + 2 * WINDOW)
        for n in range(blocks):
            near = jnp.concatenate([piece_refs[n + i][...] for i in range(3)], axis=0)
            keys, values = near[:, :HEAD_DIM], near[:, HEAD_DIM:]
            least = jnp.where(place == 0, WINDOW, 0) if n == 0 else 0
            most = jnp.where(place == last, 2 * WINDOW, 3 * WINDOW) if n == blocks - 1 else 3 * WINDOW
            allowed = band & (column >= least) & (column < most)
            outs = []
            for r in range(heads):
                here = query_ref[n * WINDOW : (n + 1) * WINDOW, r * HEAD_DIM : (r + 1) * HEAD_DIM]
                scores = lax.dot_general(
                    here, keys, (((1,), (1,)), ((), ())), preferred_element_type=jnp.float32
                )
                scores = jnp.where(allowed, scores * HEAD_DIM ** (-0.5), -1e30)
                sink = sink_ref[r]
                top = jnp.maximum(jnp.max(scores, axis=-1, keepdims=True), sink)
                weights = jnp.exp(scores - top)
                total = jnp.sum(weights, axis=-1, keepdims=True) + jnp.exp(sink - top)
                outs.append(dot((weights / total).astype(jnp.bfloat16), values))
            mixed = jnp.concatenate(outs, axis=1).astype(jnp.bfloat16)
            out_ref[n * WINDOW : (n + 1) * WINDOW, :] = mixed

    vmem = pl.BlockSpec(memory_space=pltpu.VMEM)
    return pl.pallas_call(
        kernel,
        out_shape=jax.ShapeDtypeStruct((tokens, width), jnp.bfloat16),
        in_specs=[pl.BlockSpec(memory_space=pltpu.SMEM)] + [vmem] * (blocks + 3),
        out_specs=vmem,
        name="banded",
    )(sinks, query, *pieces)


def attention(mixer_input, mixer_gain, query_weight, key_weight, value_weight, sink_logit):
    tokens = mixer_input.shape[0]
    places = lax.axis_index(EP) * tokens + jnp.arange(tokens, dtype=jnp.int32)
    query, *pieces = projections(
        mixer_input, mixer_gain, query_weight, key_weight, value_weight, places
    )
    up = [(i, i + 1) for i in range(lax.axis_size(EP) - 1)]
    before = lax.ppermute(pieces[-1], EP, up)
    after = lax.ppermute(pieces[0], EP, [(j, i) for i, j in up])
    return banded(query, [before, *pieces, after], sink_logit)


def projected(heads, weight):
    _, n, j = heads[0].shape
    f = weight.shape[1]

    def kernel(*refs):
        heads_refs, weight_ref, out_ref = refs[:4], refs[4], refs[5]
        total = jnp.zeros((n, f), jnp.float32)
        for k in range(4):
            h, p = lax.axis_index("h") ^ (k // 2), lax.axis_index("p") ^ (k % 2)
            for Y, X in itertools.product(range(2), repeat=2):
                unit = pl.multiple_of((8 * Y + 4 * h + 2 * X + p) * j, j)
                total = total + dot(heads_refs[k][2 * Y + X], weight_ref[pl.ds(unit, j), :])
        out_ref[...] = total.astype(jnp.bfloat16)

    vmem = pl.BlockSpec(memory_space=pltpu.VMEM)
    return pl.pallas_call(
        kernel,
        out_shape=jax.ShapeDtypeStruct((n, f), jnp.bfloat16),
        in_specs=[vmem] * 5,
        out_specs=vmem,
        name="projected",
    )(*heads, weight)


def shards(
    mixer_input,
    mixer_gain,
    query_weight,
    key_weight,
    value_weight,
    output_weight,
    sink_logit,
    expert_input,
    expert_gain,
    routes,
    route_logits,
    gate_weight,
    up_weight,
    down_weight,
):
    experts = lax.axis_size(EP)
    rows_here, features = expert_input.shape
    slots = 2 * rows_here * TOP_K // experts // 4
    width = features // 4
    weights = (gate_weight[0], up_weight[0], down_weight[0])
    outgoing, target, own = dispatch(
        expert_input, expert_gain, routes, weights, experts, slots, width
    )
    shares = gather_shares(own)
    received = swap(outgoing.reshape(experts, slots, width), EP)
    mixed = attention(mixer_input, mixer_gain, query_weight, key_weight, value_weight, sink_logit)
    beside = jnp.concatenate([received.reshape(experts * slots, width), mixed], axis=1)
    rows = spread(beside, ("Y", "X"))
    arrived = shares[3][:8] + shares[4][:8]
    inner, heads = gated(rows, shares, arrived)
    hidden = swap(inner, ("Y", "X"))
    heads = [heads] + [
        lax.ppermute(heads, ("h", "p"), [(i, i ^ k) for i in range(4)])
        for k in range(1, 4)
    ]
    result = lowered(hidden, shares, slots)
    returned = swap(result.reshape(4 * experts, slots, -1), (*EP, "h", "p"))
    mixer_output = projected(heads, output_weight)
    chances = jax.nn.softmax(route_logits.T, axis=0)
    expert_output = combine(
        returned.reshape(experts * 4 * slots, -1), target, chances
    )
    return (mixer_output, expert_output)


def solution(mesh):
    names = ("ep_0", "ep_1", "Y", "h", "X", "p")
    finer = Mesh(mesh.devices.reshape(16, 2, 2, 2, 2, 2), names)
    in_specs = (
        P(EP, None),
        P(),
        P(None, TP),
        P(None, TP),
        P(None, TP),
        P(None, TP),
        P(TP),
        P(EP, None),
        P(),
        P(EP, None),
        P(EP, None),
        P(EP, None, TP),
        P(EP, None, TP),
        P(EP, None, TP),
    )
    out_specs = (P(EP, TP), P(EP, TP))
    return jax.shard_map(
        shards, mesh=finer, in_specs=in_specs, out_specs=out_specs, check_vma=False
    )
```

```python
import itertools

import jax
import jax.numpy as jnp
from jax import lax
from jax.experimental import pallas as pl
from jax.experimental.pallas import tpu as pltpu
from jax.sharding import Mesh
from jax.sharding import PartitionSpec as P

HEAD_DIM = 64
TOP_K = 4
WINDOW = 128
GRID_W = 64
EP = ("ep_0", "ep_1")
TP = ("Y", "h", "X", "p")

EPSILON = 1e-06
LIMIT = 7.0
SLOPE = 1.702
BASE = 10000.0


def swap(pieces, axis):
    return lax.all_to_all(pieces, axis, 0, 0, tiled=True)


def spread(shard, axis):
    return swap(jnp.broadcast_to(shard[None], (lax.axis_size(axis), *shard.shape)), axis)


def activate(gate, up):
    capped = jnp.minimum(gate, LIMIT)
    bounded = jnp.clip(up, -LIMIT, LIMIT)
    return (capped * jax.nn.sigmoid(SLOPE * capped) * (bounded + 1.0)).astype(jnp.bfloat16)


def dot(a, b):
    return jnp.dot(a, b, preferred_element_type=jnp.float32)


def tall(wide):
    k, n = wide.shape
    square = jnp.concatenate([wide, jnp.zeros((n - k, n), wide.dtype)], axis=0)
    return square.T


def dispatch(rows, gain, routes, weights, experts, slots, width):
    tokens = rows.shape[0]
    pairs = experts // 2
    tall_rows, columns = weights[0].shape

    def kernel(rows_ref, gain_ref, routes_ref, *refs):
        weight_refs, (out_ref, target_ref, stacked_ref, held_ref, sems) = refs[:3], refs[3:]
        arriving = [
            pltpu.make_async_copy(ref, held_ref.at[i], sems.at[i])
            for i, ref in enumerate(weight_refs)
        ]
        leaving = [
            pltpu.make_async_copy(
                held_ref.at[i], stacked_ref.at[pl.ds(i * tall_rows, tall_rows)], sems.at[3 + i]
            )
            for i in range(3)
        ]
        for copy in arriving:
            copy.start()
        block = 2 * lax.axis_index("Y") + lax.axis_index("X")
        values = rows_ref[...].astype(jnp.float32)
        scale = lax.rsqrt(jnp.mean(values * values, axis=-1, keepdims=True) + EPSILON)
        for come, go in zip(arriving, leaving):
            come.wait()
            go.start()
        start = pl.multiple_of(block * width, width)
        own = rows_ref[:, pl.ds(start, width)].astype(jnp.float32)
        normed = (own * scale * gain_ref[:, pl.ds(start, width)]).astype(jnp.bfloat16)
        first = lax.broadcasted_iota(jnp.int32, (tokens, tokens), 0)
        second = lax.broadcasted_iota(jnp.int32, (tokens, tokens), 1)
        parity = lax.axis_index("p")
        expert = lax.broadcasted_iota(jnp.int32, (pairs, tokens), 0) * 2 + parity
        named = jnp.zeros((pairs, tokens), jnp.float32)
        for k in range(TOP_K):
            named = named + (routes_ref[k : k + 1, :] == expert).astype(jnp.float32)
        earlier = dot(named.astype(jnp.bfloat16), (first < second).astype(jnp.bfloat16))
        rank = jnp.where(named > 0.0, earlier.astype(jnp.int32), -1)
        rank = rank - lax.axis_index("h") * (2 * slots)
        slot = lax.broadcasted_iota(jnp.int32, (pairs, 2 * slots, tokens), 1)
        chosen = (rank[:, None, :] == slot).astype(jnp.float32)
        chosen = chosen.reshape(experts * slots, tokens).astype(jnp.bfloat16)
        out_ref[...] = dot(chosen, normed).astype(jnp.bfloat16)
        routed = tall(routes_ref[...].astype(jnp.float32))
        column = lax.broadcasted_iota(jnp.int32, (tokens, experts), 1)
        wanted = column.astype(jnp.float32)
        marks = [(routed[:, k : k + 1] == wanted).astype(jnp.float32) for k in range(TOP_K)]
        before = dot((second < first).astype(jnp.bfloat16), sum(marks).astype(jnp.bfloat16))
        before = before.astype(jnp.int32)
        core, half, spot = (before // slots) % 2, before // (2 * slots), before % slots
        position = (((column // 2) * 2 + core) * 2 + half) * 2 + column % 2
        position = (position * slots + spot).astype(jnp.float32)
        target_ref[...] = jnp.concatenate(
            [jnp.sum(mark * position, axis=1, keepdims=True) for mark in marks], axis=1
        ).astype(jnp.int32)
        for copy in leaving:
            copy.wait()

    vmem = pl.BlockSpec(memory_space=pltpu.VMEM)
    anywhere = pl.BlockSpec(memory_space=pl.ANY)
    return pl.pallas_call(
        kernel,
        out_shape=(
            jax.ShapeDtypeStruct((experts * slots, width), jnp.bfloat16),
            jax.ShapeDtypeStruct((tokens, TOP_K), jnp.int32),
            jax.ShapeDtypeStruct((3 * tall_rows, columns), jnp.bfloat16),
        ),
        in_specs=[vmem] * 3 + [anywhere] * 3,
        out_specs=(vmem, vmem, anywhere),
        scratch_shapes=[
            pltpu.VMEM((3, tall_rows, columns), jnp.bfloat16),
            pltpu.SemaphoreType.DMA((6,)),
        ],
        name="dispatch",
    )(rows, gain[None, :], routes.T, *weights)


def device_pairs(where):
    names = list(itertools.product(range(2), repeat=5))
    number = {name: i for i, name in enumerate(names)}
    return [(number[n], number[where(*n)]) for n in names if where(*n) is not None]


def gather_shares(own):
    axes = ("ep_1", "Y", "h", "X", "p")

    def outer(c, Y, h, X, p):
        return (c, Y, 1 - h, X, p) if c == p else (1 - c, Y, h, X, 1 - p)

    def cross(c, Y, h, X, p):
        return (1 - c, Y, h, X, p) if c == p else (c, Y, 1 - h, X, 1 - p)

    def trade(c, Y, h, X, p):
        return (1 - c, Y, h, X, p)

    def give(c, Y, h, X, p):
        return (1 - c, Y, h, X, p) if c == p else None

    first = lax.ppermute(own, axes, device_pairs(outer))
    second = lax.ppermute(own, axes, device_pairs(cross))
    third = lax.ppermute(first, axes, device_pairs(trade))
    fourth = lax.ppermute(second, axes, device_pairs(give))
    return own, first, second, third, fourth


def share_order():
    c, h, p = (lax.axis_index(a) for a in ("ep_1", "h", "p"))
    native = c == p
    own, up = 2 * h + p, 2 * (1 - h) + p
    side, across = 2 * h + (1 - p), 2 * (1 - h) + (1 - p)
    return native, [own, jnp.where(native, up, side), across, jnp.where(native, side, up)]


def copy_share(native, shares, index, start, size, target, sem):
    own, first, second, third, fourth = shares
    rows = pl.ds(start, size)
    if index in (1, 3):
        source = first if index == 1 else third
        pltpu.make_async_copy(source.at[rows], target, sem).start()
        return
    here, there = (own, second) if index == 0 else (second, fourth)

    @pl.when(native)
    def _():
        pltpu.make_async_copy(here.at[rows], target, sem).start()

    @pl.when(jnp.logical_not(native))
    def _():
        pltpu.make_async_copy(there.at[rows], target, sem).start()


def gated(rows, shares, arrived):
    parts, n, wide = rows.shape
    u = shares[0].shape[1]
    k = 4 * u
    j = wide - k
    whole = parts * k

    def kernel(rows_ref, _, *refs):
        shares, refs = refs[:5], refs[5:]
        out_ref, heads_ref, here_ref, weights_ref, hidden_ref, sems, row_sems, out_sems = refs
        native, order = share_order()
        arrivals = [
            pltpu.make_async_copy(rows_ref.at[part], here_ref.at[part], row_sems.at[part])
            for part in range(parts)
        ]
        heads = pltpu.make_async_copy(
            here_ref.at[:, :, pl.ds(k, j)], heads_ref, row_sems.at[parts]
        )
        targets = [
            (weights_ref.at[i, :, pl.ds(side * u, u)], sems.at[i, side])
            for i in range(4)
            for side in range(2)
        ]

        def fetch(i):
            for side in range(2):
                target, sem = targets[2 * i + side]
                copy_share(native, shares, i, side * whole, whole, target, sem)

        for part in range(parts):
            arrivals[part].start()
        for i in range(4):
            fetch(i)
        for part in range(parts):
            arrivals[part].wait()
        heads.start()
        leaving = []
        for i in range(4):
            for side in range(2):
                target, sem = targets[2 * i + side]
                pltpu.make_async_copy(shares[1].at[pl.ds(0, whole)], target, sem).wait()
            total = dot(here_ref[0, :, :k], weights_ref[i, :k, :])
            for part in range(1, parts):
                piece = here_ref[part, :, :k]
                total = total + dot(piece, weights_ref[i, part * k : (part + 1) * k, :])
            hidden_ref[i] = activate(total[:, :u], total[:, u:])
            lane = pl.multiple_of(order[i] * u, u)
            for copy in range(parts):
                out = out_ref.at[copy, :, pl.ds(lane, u)]
                leaving.append(
                    pltpu.make_async_copy(hidden_ref.at[i], out, out_sems.at[i, copy])
                )
                leaving[-1].start()
        for copy in leaving:
            copy.wait()
        heads.wait()

    anywhere = pl.BlockSpec(memory_space=pl.ANY)
    return pl.pallas_call(
        kernel,
        out_shape=(
            jax.ShapeDtypeStruct((parts, n, 4 * u), jnp.bfloat16),
            jax.ShapeDtypeStruct((parts, n, j), jnp.bfloat16),
        ),
        in_specs=[anywhere] * 7,
        out_specs=(anywhere, anywhere),
        scratch_shapes=[
            pltpu.VMEM((parts, n, wide), jnp.bfloat16),
            pltpu.VMEM((4, whole, 2 * u), jnp.bfloat16),
            pltpu.VMEM((4, n, u), jnp.bfloat16),
            pltpu.SemaphoreType.DMA((4, 2)),
            pltpu.SemaphoreType.DMA((parts + 1,)),
            pltpu.SemaphoreType.DMA((4, parts)),
        ],
        name="gated",
    )(rows, arrived, *shares)


def lowered(hidden, shares, slots):
    parts, n, k = hidden.shape
    f = shares[0].shape[1]
    whole = parts * k
    half = k // 2

    def kernel(hidden_ref, *refs):
        shares, (out_ref, here_ref, weights_ref, sems, row_sems) = refs[:5], refs[5:]
        native, order = share_order()
        targets = [
            (weights_ref.at[i // 2, :, pl.ds((i % 2) * f, f)], sems.at[i]) for i in range(4)
        ]
        arrivals = [
            pltpu.make_async_copy(hidden_ref.at[part], here_ref.at[part], row_sems.at[part])
            for part in range(parts)
        ]
        for i in range(2):
            copy_share(native, shares, i, 2 * whole, whole, *targets[i])
        for part in range(parts):
            arrivals[part].start()
        for i in range(2, 4):
            copy_share(native, shares, i, 2 * whole, whole, *targets[i])
        for pair in range(2):
            for i in (2 * pair, 2 * pair + 1):
                pltpu.make_async_copy(shares[1].at[pl.ds(0, whole)], *targets[i]).wait()
            total = jnp.zeros((n, 2 * f), jnp.float32)
            for Y, X in itertools.product(range(2), repeat=2):
                if pair == 0:
                    arrivals[2 * Y + X].wait()
                for h in range(2):
                    unit = (8 * Y + 4 * h + 2 * X) * f
                    piece = here_ref[2 * Y + X, :, h * half : (h + 1) * half]
                    total = total + dot(piece, weights_ref[pair, unit : unit + half, :])
            rounded = total.astype(jnp.bfloat16).reshape(n // slots, slots, 2 * f)
            out_ref[:, order[2 * pair]] = rounded[:, :, :f]
            out_ref[:, order[2 * pair + 1]] = rounded[:, :, f:]

    vmem = pl.BlockSpec(memory_space=pltpu.VMEM)
    anywhere = pl.BlockSpec(memory_space=pl.ANY)
    return pl.pallas_call(
        kernel,
        out_shape=jax.ShapeDtypeStruct((n // slots, 4, slots, f), jnp.bfloat16),
        in_specs=[anywhere] * 6,
        out_specs=vmem,
        scratch_shapes=[
            pltpu.VMEM((parts, n, k), jnp.bfloat16),
            pltpu.VMEM((2, whole, 2 * f), jnp.bfloat16),
            pltpu.SemaphoreType.DMA((4,)),
            pltpu.SemaphoreType.DMA((parts,)),
        ],
        name="lowered",
    )(hidden, *shares)


def combine(results, target, chances):
    slots, f = results.shape
    tokens = target.shape[0]

    def kernel(results_ref, target_ref, chances_ref, out_ref):
        chances = tall(chances_ref[...])
        lane = lax.broadcasted_iota(jnp.int32, (tokens, slots), 1)
        chosen = [
            (target_ref[:, k : k + 1] == lane).astype(jnp.float32).astype(jnp.bfloat16)
            for k in range(TOP_K)
        ]
        picked = dot(jnp.concatenate(chosen, axis=0), results_ref[...])
        total = jnp.zeros((tokens, f), jnp.float32)
        for k in range(TOP_K):
            total = total + picked[k * tokens : (k + 1) * tokens] * chances[:, k : k + 1]
        out_ref[...] = total.astype(jnp.bfloat16)

    vmem = pl.BlockSpec(memory_space=pltpu.VMEM)
    return pl.pallas_call(
        kernel,
        out_shape=jax.ShapeDtypeStruct((tokens, f), jnp.bfloat16),
        in_specs=[vmem] * 3,
        out_specs=vmem,
        name="combine",
    )(results, target, chances)


def rotary_tables(places, width):
    quarter = HEAD_DIM // 4
    lane = jnp.arange(width, dtype=jnp.int32)
    frequency = BASE ** (-(lane % quarter).astype(jnp.float32) / quarter)
    row = (places // GRID_W).astype(jnp.float32)[:, None]
    column = (places % GRID_W).astype(jnp.float32)[:, None]
    angle = jnp.where(lane % HEAD_DIM < HEAD_DIM // 2, row, column) * frequency
    sign = jnp.where(lane % (2 * quarter) < quarter, -1.0, 1.0)
    return jnp.cos(angle), jnp.sin(angle) * sign


def projections(rows, gain, query_weight, key_weight, value_weight, places):
    tokens, _ = rows.shape
    width = query_weight.shape[1]
    half = width // 2
    quarter = HEAD_DIM // 4
    cosine, sine = rotary_tables(places, width)

    def kernel(
        rows_ref, gain_ref, query_ref, key_ref, value_ref, cos_ref, sin_ref, out_ref, *pair_refs
    ):
        values = rows_ref[...].astype(jnp.float32)
        scale = lax.rsqrt(jnp.mean(values * values, axis=-1, keepdims=True) + EPSILON)
        normed = (values * scale * gain_ref[...]).astype(jnp.bfloat16)
        lane = lax.broadcasted_iota(jnp.int32, (tokens, width), 1) % (2 * quarter)

        def turned(a):
            partner = jnp.where(
                lane < quarter,
                pltpu.roll(a, width - quarter, 1),
                pltpu.roll(a, quarter, 1),
            )
            return (a * cos_ref[...] + partner * sin_ref[...]).astype(jnp.bfloat16)

        def flipped(weight_ref):
            return lax.dot_general(
                normed, weight_ref[...], (((1,), (1,)), ((), ())), preferred_element_type=jnp.float32
            )

        out_ref[...] = turned(dot(normed, query_ref[...]))
        keys, mine = flipped(key_ref), flipped(value_ref)
        both = jnp.concatenate([keys, mine], axis=1)
        rounded = jnp.where(
            lax.broadcasted_iota(jnp.int32, (tokens, width), 1) < half,
            turned(both),
            both.astype(jnp.bfloat16),
        )
        for i, ref in enumerate(pair_refs):
            ref[...] = rounded[i * WINDOW : (i + 1) * WINDOW]

    vmem = pl.BlockSpec(memory_space=pltpu.VMEM)
    return pl.pallas_call(
        kernel,
        out_shape=[jax.ShapeDtypeStruct((tokens, width), jnp.bfloat16)]
        + [jax.ShapeDtypeStruct((WINDOW, width), jnp.bfloat16)] * (tokens // WINDOW),
        in_specs=[vmem] * 7,
        out_specs=[vmem] * (1 + tokens // WINDOW),
        name="projections",
    )(rows, gain[None, :], query_weight, key_weight.T, value_weight.T, cosine, sine)


def banded(query, pieces, sinks):
    tokens, width = query.shape
    blocks = tokens // WINDOW
    heads = width // HEAD_DIM

    def kernel(sink_ref, query_ref, *refs):
        piece_refs, out_ref = refs[:-1], refs[-1]
        place, last = lax.axis_index(EP), lax.axis_size(EP) - 1
        row = lax.broadcasted_iota(jnp.int32, (WINDOW, 3 * WINDOW), 0)
        column = lax.broadcasted_iota(jnp.int32, (WINDOW, 3 * WINDOW), 1)
        band = (column >= row) & (column <= row + 2 * WINDOW)
        for n in range(blocks):
            near = jnp.concatenate([piece_refs[n + i][...] for i in range(3)], axis=0)
            keys, values = near[:, :HEAD_DIM], near[:, HEAD_DIM:]
            least = jnp.where(place == 0, WINDOW, 0) if n == 0 else 0
            most = jnp.where(place == last, 2 * WINDOW, 3 * WINDOW) if n == blocks - 1 else 3 * WINDOW
            allowed = band & (column >= least) & (column < most)
            outs = []
            for r in range(heads):
                here = query_ref[n * WINDOW : (n + 1) * WINDOW, r * HEAD_DIM : (r + 1) * HEAD_DIM]
                scores = lax.dot_general(
                    here, keys, (((1,), (1,)), ((), ())), preferred_element_type=jnp.float32
                )
                scores = jnp.where(allowed, scores * HEAD_DIM ** (-0.5), -1e30)
                sink = sink_ref[r]
                top = jnp.maximum(jnp.max(scores, axis=-1, keepdims=True), sink)
                weights = jnp.exp(scores - top)
                total = jnp.sum(weights, axis=-1, keepdims=True) + jnp.exp(sink - top)
                outs.append(dot((weights / total).astype(jnp.bfloat16), values))
            mixed = jnp.concatenate(outs, axis=1).astype(jnp.bfloat16)
            out_ref[n * WINDOW : (n + 1) * WINDOW, :] = mixed

    vmem = pl.BlockSpec(memory_space=pltpu.VMEM)
    return pl.pallas_call(
        kernel,
        out_shape=jax.ShapeDtypeStruct((tokens, width), jnp.bfloat16),
        in_specs=[pl.BlockSpec(memory_space=pltpu.SMEM)] + [vmem] * (blocks + 3),
        out_specs=vmem,
        name="banded",
    )(sinks, query, *pieces)


def attention(mixer_input, mixer_gain, query_weight, key_weight, value_weight, sink_logit):
    tokens = mixer_input.shape[0]
    places = lax.axis_index(EP) * tokens + jnp.arange(tokens, dtype=jnp.int32)
    query, *pieces = projections(
        mixer_input, mixer_gain, query_weight, key_weight, value_weight, places
    )
    up = [(i, i + 1) for i in range(lax.axis_size(EP) - 1)]
    before = lax.ppermute(pieces[-1], EP, up)
    after = lax.ppermute(pieces[0], EP, [(j, i) for i, j in up])
    return banded(query, [before, *pieces, after], sink_logit)


def projected(heads, weight):
    _, n, j = heads[0].shape
    f = weight.shape[1]

    def kernel(*refs):
        heads_refs, weight_ref, out_ref = refs[:4], refs[4], refs[5]
        total = jnp.zeros((n, f), jnp.float32)
        for k in range(4):
            h, p = lax.axis_index("h") ^ (k // 2), lax.axis_index("p") ^ (k % 2)
            for Y, X in itertools.product(range(2), repeat=2):
                unit = pl.multiple_of((8 * Y + 4 * h + 2 * X + p) * j, j)
                total = total + dot(heads_refs[k][2 * Y + X], weight_ref[pl.ds(unit, j), :])
        out_ref[...] = total.astype(jnp.bfloat16)

    vmem = pl.BlockSpec(memory_space=pltpu.VMEM)
    return pl.pallas_call(
        kernel,
        out_shape=jax.ShapeDtypeStruct((n, f), jnp.bfloat16),
        in_specs=[vmem] * 5,
        out_specs=vmem,
        name="projected",
    )(*heads, weight)


def shards(
    mixer_input,
    mixer_gain,
    query_weight,
    key_weight,
    value_weight,
    output_weight,
    sink_logit,
    expert_input,
    expert_gain,
    routes,
    route_logits,
    gate_weight,
    up_weight,
    down_weight,
):
    experts = lax.axis_size(EP)
    rows_here, features = expert_input.shape
    slots = 2 * rows_here * TOP_K // experts // 4
    width = features // 4
    weights = (gate_weight[0], up_weight[0], down_weight[0])
    outgoing, target, own = dispatch(
        expert_input, expert_gain, routes, weights, experts, slots, width
    )
    shares = gather_shares(own)
    received = swap(outgoing.reshape(experts, slots, width), EP)
    mixed = attention(mixer_input, mixer_gain, query_weight, key_weight, value_weight, sink_logit)
    beside = jnp.concatenate([received.reshape(experts * slots, width), mixed], axis=1)
    rows = spread(beside, ("Y", "X"))
    arrived = shares[3][:8] + shares[4][:8]
    inner, heads = gated(rows, shares, arrived)
    hidden = swap(inner, ("Y", "X"))
    heads = [heads] + [
        lax.ppermute(heads, ("h", "p"), [(i, i ^ k) for i in range(4)])
        for k in range(1, 4)
    ]
    result = lowered(hidden, shares, slots)
    returned = swap(result.reshape(4 * experts, slots, -1), (*EP, "h", "p"))
    mixer_output = projected(heads, output_weight)
    chances = jax.nn.softmax(route_logits.T, axis=0)
    expert_output = combine(
        returned.reshape(experts * 4 * slots, -1), target, chances
    )
    return (mixer_output, expert_output)


def solution(mesh):
    names = ("ep_0", "ep_1", "Y", "h", "X", "p")
    finer = Mesh(mesh.devices.reshape(16, 2, 2, 2, 2, 2), names)
    in_specs = (
        P(EP, None),
        P(),
        P(None, TP),
        P(None, TP),
        P(None, TP),
        P(None, TP),
        P(TP),
        P(EP, None),
        P(),
        P(EP, None),
        P(EP, None),
        P(EP, None, TP),
        P(EP, None, TP),
        P(EP, None, TP),
    )
    out_specs = (P(EP, TP), P(EP, TP))
    return jax.shard_map(
        shards, mesh=finer, in_specs=in_specs, out_specs=out_specs, check_vma=False
    )
```

```python
import itertools

import jax
import jax.numpy as jnp
from jax import lax
from jax.experimental import pallas as pl
from jax.experimental.pallas import tpu as pltpu
from jax.sharding import Mesh
from jax.sharding import PartitionSpec as P

HEAD_DIM = 64
TOP_K = 4
WINDOW = 128
GRID_W = 64
EP = ("ep_0", "ep_1")
TP = ("Y", "h", "X", "p")

EPSILON = 1e-06
LIMIT = 7.0
SLOPE = 1.702
BASE = 10000.0


def swap(pieces, axis):
    return lax.all_to_all(pieces, axis, 0, 0, tiled=True)


def spread(shard, axis):
    return swap(jnp.broadcast_to(shard[None], (lax.axis_size(axis), *shard.shape)), axis)


def activate(gate, up):
    capped = jnp.minimum(gate, LIMIT)
    bounded = jnp.clip(up, -LIMIT, LIMIT)
    return (capped * jax.nn.sigmoid(SLOPE * capped) * (bounded + 1.0)).astype(jnp.bfloat16)


def dot(a, b):
    return jnp.dot(a, b, preferred_element_type=jnp.float32)


def tall(wide):
    k, n = wide.shape
    square = jnp.concatenate([wide, jnp.zeros((n - k, n), wide.dtype)], axis=0)
    return square.T


def dispatch(rows, gain, routes, weights, experts, slots, width):
    tokens = rows.shape[0]
    pairs = experts // 2
    tall_rows, columns = weights[0].shape

    def kernel(rows_ref, gain_ref, routes_ref, *refs):
        weight_refs, refs = refs[:3], refs[3:]
        out_ref, target_ref, stacked_ref, held_ref, here_ref, sems = refs
        rows_copy = pltpu.make_async_copy(rows_ref, here_ref, sems.at[6])
        rows_copy.start()
        arriving = [
            pltpu.make_async_copy(ref, held_ref.at[i], sems.at[i])
            for i, ref in enumerate(weight_refs)
        ]
        leaving = [
            pltpu.make_async_copy(
                held_ref.at[i], stacked_ref.at[pl.ds(i * tall_rows, tall_rows)], sems.at[3 + i]
            )
            for i in range(3)
        ]
        for copy in arriving:
            copy.start()
        block = 2 * lax.axis_index("Y") + lax.axis_index("X")
        rows_copy.wait()
        for come, go in zip(arriving, leaving):
            come.wait()
            go.start()
        values = here_ref[...].astype(jnp.float32)
        scale = lax.rsqrt(jnp.mean(values * values, axis=-1, keepdims=True) + EPSILON)
        start = pl.multiple_of(block * width, width)
        own = here_ref[:, pl.ds(start, width)].astype(jnp.float32)
        normed = (own * scale * gain_ref[:, pl.ds(start, width)]).astype(jnp.bfloat16)
        first = lax.broadcasted_iota(jnp.int32, (tokens, tokens), 0)
        second = lax.broadcasted_iota(jnp.int32, (tokens, tokens), 1)
        parity = lax.axis_index("p")
        expert = lax.broadcasted_iota(jnp.int32, (pairs, tokens), 0) * 2 + parity
        named = jnp.zeros((pairs, tokens), jnp.float32)
        for k in range(TOP_K):
            named = named + (routes_ref[k : k + 1, :] == expert).astype(jnp.float32)
        earlier = dot(named.astype(jnp.bfloat16), (first < second).astype(jnp.bfloat16))
        rank = jnp.where(named > 0.0, earlier.astype(jnp.int32), -1)
        rank = rank - lax.axis_index("h") * (2 * slots)
        slot = lax.broadcasted_iota(jnp.int32, (pairs, 2 * slots, tokens), 1)
        chosen = (rank[:, None, :] == slot).astype(jnp.float32)
        chosen = chosen.reshape(experts * slots, tokens).astype(jnp.bfloat16)
        out_ref[...] = dot(chosen, normed).astype(jnp.bfloat16)
        routed = tall(routes_ref[...].astype(jnp.float32))
        column = lax.broadcasted_iota(jnp.int32, (tokens, experts), 1)
        wanted = column.astype(jnp.float32)
        marks = [(routed[:, k : k + 1] == wanted).astype(jnp.float32) for k in range(TOP_K)]
        before = dot((second < first).astype(jnp.bfloat16), sum(marks).astype(jnp.bfloat16))
        before = before.astype(jnp.int32)
        core, half, spot = (before // slots) % 2, before // (2 * slots), before % slots
        position = (((column // 2) * 2 + core) * 2 + half) * 2 + column % 2
        position = (position * slots + spot).astype(jnp.float32)
        target_ref[...] = jnp.concatenate(
            [jnp.sum(mark * position, axis=1, keepdims=True) for mark in marks], axis=1
        ).astype(jnp.int32)
        for copy in leaving:
            copy.wait()

    vmem = pl.BlockSpec(memory_space=pltpu.VMEM)
    anywhere = pl.BlockSpec(memory_space=pl.ANY)
    return pl.pallas_call(
        kernel,
        out_shape=(
            jax.ShapeDtypeStruct((experts * slots, width), jnp.bfloat16),
            jax.ShapeDtypeStruct((tokens, TOP_K), jnp.int32),
            jax.ShapeDtypeStruct((3 * tall_rows, columns), jnp.bfloat16),
        ),
        in_specs=[anywhere] + [vmem] * 2 + [anywhere] * 3,
        out_specs=(vmem, vmem, anywhere),
        scratch_shapes=[
            pltpu.VMEM((3, tall_rows, columns), jnp.bfloat16),
            pltpu.VMEM(rows.shape, rows.dtype),
            pltpu.SemaphoreType.DMA((7,)),
        ],
        name="dispatch",
    )(rows, gain[None, :], routes.T, *weights)


def device_pairs(where):
    names = list(itertools.product(range(2), repeat=5))
    number = {name: i for i, name in enumerate(names)}
    return [(number[n], number[where(*n)]) for n in names if where(*n) is not None]


def gather_shares(own):
    axes = ("ep_1", "Y", "h", "X", "p")

    def outer(c, Y, h, X, p):
        return (c, Y, 1 - h, X, p) if c == p else (1 - c, Y, h, X, 1 - p)

    def cross(c, Y, h, X, p):
        return (1 - c, Y, h, X, p) if c == p else (c, Y, 1 - h, X, 1 - p)

    def trade(c, Y, h, X, p):
        return (1 - c, Y, h, X, p)

    def give(c, Y, h, X, p):
        return (1 - c, Y, h, X, p) if c == p else None

    first = lax.ppermute(own, axes, device_pairs(outer))
    second = lax.ppermute(own, axes, device_pairs(cross))
    third = lax.ppermute(first, axes, device_pairs(trade))
    fourth = lax.ppermute(second, axes, device_pairs(give))
    return own, first, second, third, fourth


def share_order():
    c, h, p = (lax.axis_index(a) for a in ("ep_1", "h", "p"))
    native = c == p
    own, up = 2 * h + p, 2 * (1 - h) + p
    side, across = 2 * h + (1 - p), 2 * (1 - h) + (1 - p)
    return native, [own, jnp.where(native, up, side), across, jnp.where(native, side, up)]


def copy_share(native, shares, index, start, size, target, sem):
    own, first, second, third, fourth = shares
    rows = pl.ds(start, size)
    if index in (1, 3):
        source = first if index == 1 else third
        pltpu.make_async_copy(source.at[rows], target, sem).start()
        return
    here, there = (own, second) if index == 0 else (second, fourth)

    @pl.when(native)
    def _():
        pltpu.make_async_copy(here.at[rows], target, sem).start()

    @pl.when(jnp.logical_not(native))
    def _():
        pltpu.make_async_copy(there.at[rows], target, sem).start()


def gated(rows, mixed, shares, arrived):
    parts, n, k = rows.shape
    u = shares[0].shape[1]
    j = mixed.shape[1]
    whole = parts * k

    def kernel(rows_ref, mixed_ref, _, *refs):
        shares, refs = refs[:5], refs[5:]
        out_ref, here_ref, weights_ref, hidden_ref, sems, row_sems, out_sems = refs
        native, order = share_order()
        arrivals = [
            pltpu.make_async_copy(rows_ref.at[part], here_ref.at[part], row_sems.at[part])
            for part in range(parts)
        ]
        arrivals.append(
            pltpu.make_async_copy(
                mixed_ref, hidden_ref.at[:, pl.ds(4 * u, j)], row_sems.at[parts]
            )
        )
        targets = [
            (weights_ref.at[i, :, pl.ds(side * u, u)], sems.at[i, side])
            for i in range(4)
            for side in range(2)
        ]
        for copy in arrivals:
            copy.start()
        for i in range(4):
            for side in range(2):
                copy_share(native, shares, i, side * whole, whole, *targets[2 * i + side])
        for copy in arrivals:
            copy.wait()
        for target in targets:
            pltpu.make_async_copy(shares[1].at[pl.ds(0, whole)], *target).wait()
        for i in range(4):
            total = dot(here_ref[0], weights_ref[i, :k, :])
            for part in range(1, parts):
                total = total + dot(here_ref[part], weights_ref[i, part * k : (part + 1) * k, :])
            lane = pl.multiple_of(order[i] * u, u)
            hidden_ref[:, pl.ds(lane, u)] = activate(total[:, :u], total[:, u:])
        leaving = [
            pltpu.make_async_copy(hidden_ref, out_ref.at[copy], out_sems.at[copy])
            for copy in range(parts)
        ]
        for copy in leaving:
            copy.start()
        for copy in leaving:
            copy.wait()

    anywhere = pl.BlockSpec(memory_space=pl.ANY)
    return pl.pallas_call(
        kernel,
        out_shape=jax.ShapeDtypeStruct((parts, n, 4 * u + j), jnp.bfloat16),
        in_specs=[anywhere] * 8,
        out_specs=anywhere,
        scratch_shapes=[
            pltpu.VMEM((parts, n, k), jnp.bfloat16),
            pltpu.VMEM((4, whole, 2 * u), jnp.bfloat16),
            pltpu.VMEM((n, 4 * u + j), jnp.bfloat16),
            pltpu.SemaphoreType.DMA((4, 2)),
            pltpu.SemaphoreType.DMA((parts + 1,)),
            pltpu.SemaphoreType.DMA((parts,)),
        ],
        name="gated",
    )(rows, mixed, arrived, *shares)


def lowered(hidden, shares, slots):
    parts, n, wide = hidden.shape
    f = shares[0].shape[1]
    k = 4 * f
    j = wide - k
    whole = parts * k
    half = k // 2

    def kernel(hidden_ref, *refs):
        shares, refs = refs[:5], refs[5:]
        out_ref, heads_ref, here_ref, weights_ref, sems, row_sems = refs
        native, order = share_order()
        targets = [
            (weights_ref.at[i // 2, :, pl.ds((i % 2) * f, f)], sems.at[i]) for i in range(4)
        ]
        arrivals = [
            pltpu.make_async_copy(hidden_ref.at[part], here_ref.at[part], row_sems.at[part])
            for part in range(parts)
        ]
        heads = pltpu.make_async_copy(
            here_ref.at[:, :, pl.ds(k, j)], heads_ref, row_sems.at[parts]
        )
        for copy in arrivals:
            copy.start()
        for i in range(4):
            copy_share(native, shares, i, 2 * whole, whole, *targets[i])
        for copy in arrivals:
            copy.wait()
        heads.start()
        for target in targets:
            pltpu.make_async_copy(shares[1].at[pl.ds(0, whole)], *target).wait()
        for pair in range(2):
            total = jnp.zeros((n, 2 * f), jnp.float32)
            for Y, X, h in itertools.product(range(2), repeat=3):
                unit = (8 * Y + 4 * h + 2 * X) * f
                piece = here_ref[2 * Y + X, :, h * half : (h + 1) * half]
                total = total + dot(piece, weights_ref[pair, unit : unit + half, :])
            rounded = total.astype(jnp.bfloat16).reshape(n // slots, slots, 2 * f)
            out_ref[:, order[2 * pair]] = rounded[:, :, :f]
            out_ref[:, order[2 * pair + 1]] = rounded[:, :, f:]
        heads.wait()

    vmem = pl.BlockSpec(memory_space=pltpu.VMEM)
    anywhere = pl.BlockSpec(memory_space=pl.ANY)
    return pl.pallas_call(
        kernel,
        out_shape=(
            jax.ShapeDtypeStruct((n // slots, 4, slots, f), jnp.bfloat16),
            jax.ShapeDtypeStruct((parts, n, j), jnp.bfloat16),
        ),
        in_specs=[anywhere] * 6,
        out_specs=(vmem, anywhere),
        scratch_shapes=[
            pltpu.VMEM((parts, n, wide), jnp.bfloat16),
            pltpu.VMEM((2, whole, 2 * f), jnp.bfloat16),
            pltpu.SemaphoreType.DMA((4,)),
            pltpu.SemaphoreType.DMA((parts + 1,)),
        ],
        name="lowered",
    )(hidden, *shares)


def combine(results, target, chances):
    slots, f = results.shape
    tokens = target.shape[0]

    def kernel(results_ref, target_ref, chances_ref, out_ref):
        chances = tall(chances_ref[...])
        lane = lax.broadcasted_iota(jnp.int32, (tokens, slots), 1)
        chosen = [
            (target_ref[:, k : k + 1] == lane).astype(jnp.float32).astype(jnp.bfloat16)
            for k in range(TOP_K)
        ]
        picked = dot(jnp.concatenate(chosen, axis=0), results_ref[...])
        total = jnp.zeros((tokens, f), jnp.float32)
        for k in range(TOP_K):
            total = total + picked[k * tokens : (k + 1) * tokens] * chances[:, k : k + 1]
        out_ref[...] = total.astype(jnp.bfloat16)

    vmem = pl.BlockSpec(memory_space=pltpu.VMEM)
    return pl.pallas_call(
        kernel,
        out_shape=jax.ShapeDtypeStruct((tokens, f), jnp.bfloat16),
        in_specs=[vmem] * 3,
        out_specs=vmem,
        name="combine",
    )(results, target, chances)


def rotary_tables(first, rows, width):
    quarter = HEAD_DIM // 4
    lane = jnp.arange(width, dtype=jnp.int32)
    frequency = BASE ** (-(lane % quarter).astype(jnp.float32) / quarter)
    at = jnp.arange(GRID_W + rows, dtype=jnp.int32)
    place = jnp.where(at < GRID_W, at, at - GRID_W + first)
    angle = place.astype(jnp.float32)[:, None] * frequency
    sign = jnp.where(lane % (2 * quarter) < quarter, -1.0, 1.0)
    return jnp.cos(angle), jnp.sin(angle) * sign


def projections(rows, gain, query_weight, key_weight, value_weight):
    tokens, _ = rows.shape
    width = query_weight.shape[1]
    half = width // 2
    quarter = HEAD_DIM // 4
    spans = tokens // GRID_W
    cosine, sine = rotary_tables(lax.axis_index(EP) * spans, spans, width)

    def kernel(
        rows_ref, gain_ref, query_ref, key_ref, value_ref, cos_ref, sin_ref, out_ref, *pair_refs
    ):
        values = rows_ref[...].astype(jnp.float32)
        scale = lax.rsqrt(jnp.mean(values * values, axis=-1, keepdims=True) + EPSILON)
        normed = (values * scale * gain_ref[...]).astype(jnp.bfloat16)
        lane = lax.broadcasted_iota(jnp.int32, (tokens, width), 1)
        near = lane % (2 * quarter) < quarter
        by_row = lax.broadcasted_iota(jnp.int32, (GRID_W, width), 1) % HEAD_DIM < HEAD_DIM // 2

        def table(ref):
            columns = ref[:GRID_W, :]
            parts = [
                jnp.where(by_row, ref[GRID_W + i : GRID_W + i + 1, :], columns)
                for i in range(spans)
            ]
            return jnp.concatenate(parts, axis=0)

        cos, sin = table(cos_ref), table(sin_ref)

        def turned(a):
            partner = jnp.where(
                near, pltpu.roll(a, width - quarter, 1), pltpu.roll(a, quarter, 1)
            )
            return (a * cos + partner * sin).astype(jnp.bfloat16)

        def flipped(weight_ref):
            return lax.dot_general(
                normed, weight_ref[...], (((1,), (1,)), ((), ())), preferred_element_type=jnp.float32
            )

        out_ref[...] = turned(dot(normed, query_ref[...]))
        keys, mine = flipped(key_ref), flipped(value_ref)
        both = jnp.concatenate([keys, mine], axis=1)
        rounded = jnp.where(lane < half, turned(both), both.astype(jnp.bfloat16))
        for i, ref in enumerate(pair_refs):
            ref[...] = rounded[i * WINDOW : (i + 1) * WINDOW]

    vmem = pl.BlockSpec(memory_space=pltpu.VMEM)
    return pl.pallas_call(
        kernel,
        out_shape=[jax.ShapeDtypeStruct((tokens, width), jnp.bfloat16)]
        + [jax.ShapeDtypeStruct((WINDOW, width), jnp.bfloat16)] * (tokens // WINDOW),
        in_specs=[vmem] * 7,
        out_specs=[vmem] * (1 + tokens // WINDOW),
        name="projections",
    )(rows, gain[None, :], query_weight, key_weight.T, value_weight.T, cosine, sine)


def banded(query, pieces, sinks):
    tokens, width = query.shape
    blocks = tokens // WINDOW
    heads = width // HEAD_DIM

    def kernel(sink_ref, query_ref, *refs):
        piece_refs, out_ref = refs[:-1], refs[-1]
        place, last = lax.axis_index(EP), lax.axis_size(EP) - 1
        row = lax.broadcasted_iota(jnp.int32, (WINDOW, 3 * WINDOW), 0)
        column = lax.broadcasted_iota(jnp.int32, (WINDOW, 3 * WINDOW), 1)
        band = (column >= row) & (column <= row + 2 * WINDOW)
        for n in range(blocks):
            near = jnp.concatenate([piece_refs[n + i][...] for i in range(3)], axis=0)
            keys, values = near[:, :HEAD_DIM], near[:, HEAD_DIM:]
            least = jnp.where(place == 0, WINDOW, 0) if n == 0 else 0
            most = jnp.where(place == last, 2 * WINDOW, 3 * WINDOW) if n == blocks - 1 else 3 * WINDOW
            allowed = band & (column >= least) & (column < most)
            outs = []
            for r in range(heads):
                here = query_ref[n * WINDOW : (n + 1) * WINDOW, r * HEAD_DIM : (r + 1) * HEAD_DIM]
                scores = lax.dot_general(
                    here, keys, (((1,), (1,)), ((), ())), preferred_element_type=jnp.float32
                )
                scores = jnp.where(allowed, scores * HEAD_DIM ** (-0.5), -1e30)
                sink = sink_ref[r]
                top = jnp.maximum(jnp.max(scores, axis=-1, keepdims=True), sink)
                weights = jnp.exp(scores - top)
                total = jnp.sum(weights, axis=-1, keepdims=True) + jnp.exp(sink - top)
                outs.append(dot((weights / total).astype(jnp.bfloat16), values))
            mixed = jnp.concatenate(outs, axis=1).astype(jnp.bfloat16)
            out_ref[n * WINDOW : (n + 1) * WINDOW, :] = mixed

    vmem = pl.BlockSpec(memory_space=pltpu.VMEM)
    return pl.pallas_call(
        kernel,
        out_shape=jax.ShapeDtypeStruct((tokens, width), jnp.bfloat16),
        in_specs=[pl.BlockSpec(memory_space=pltpu.SMEM)] + [vmem] * (blocks + 3),
        out_specs=vmem,
        name="banded",
    )(sinks, query, *pieces)


def attention(mixer_input, mixer_gain, query_weight, key_weight, value_weight, sink_logit):
    query, *pieces = projections(mixer_input, mixer_gain, query_weight, key_weight, value_weight)
    up = [(i, i + 1) for i in range(lax.axis_size(EP) - 1)]
    before = lax.ppermute(pieces[-1], EP, up)
    after = lax.ppermute(pieces[0], EP, [(j, i) for i, j in up])
    return banded(query, [before, *pieces, after], sink_logit)


def projected(heads, weight):
    _, n, j = heads[0].shape
    f = weight.shape[1]

    def kernel(*refs):
        heads_refs, weight_ref, out_ref = refs[:4], refs[4], refs[5]
        total = jnp.zeros((n, f), jnp.float32)
        for k in range(4):
            h, p = lax.axis_index("h") ^ (k // 2), lax.axis_index("p") ^ (k % 2)
            for Y, X in itertools.product(range(2), repeat=2):
                unit = pl.multiple_of((8 * Y + 4 * h + 2 * X + p) * j, j)
                total = total + dot(heads_refs[k][2 * Y + X], weight_ref[pl.ds(unit, j), :])
        out_ref[...] = total.astype(jnp.bfloat16)

    vmem = pl.BlockSpec(memory_space=pltpu.VMEM)
    return pl.pallas_call(
        kernel,
        out_shape=jax.ShapeDtypeStruct((n, f), jnp.bfloat16),
        in_specs=[vmem] * 5,
        out_specs=vmem,
        name="projected",
    )(*heads, weight)


def shards(
    mixer_input,
    mixer_gain,
    query_weight,
    key_weight,
    value_weight,
    output_weight,
    sink_logit,
    expert_input,
    expert_gain,
    routes,
    route_logits,
    gate_weight,
    up_weight,
    down_weight,
):
    experts = lax.axis_size(EP)
    rows_here, features = expert_input.shape
    slots = 2 * rows_here * TOP_K // experts // 4
    width = features // 4
    weights = (gate_weight[0], up_weight[0], down_weight[0])
    outgoing, target, own = dispatch(
        expert_input, expert_gain, routes, weights, experts, slots, width
    )
    shares = gather_shares(own)
    received = swap(outgoing.reshape(experts, slots, width), EP)
    mixed = attention(mixer_input, mixer_gain, query_weight, key_weight, value_weight, sink_logit)
    rows = spread(received.reshape(experts * slots, width), ("Y", "X"))
    arrived = shares[3][:8] + shares[4][:8]
    inner = gated(rows, mixed, shares, arrived)
    hidden = swap(inner, ("Y", "X"))
    result, heads = lowered(hidden, shares, slots)
    returned = swap(result.reshape(4 * experts, slots, -1), (*EP, "h", "p"))
    heads = [heads] + [
        lax.ppermute(heads, ("h", "p"), [(i, i ^ k) for i in range(4)])
        for k in range(1, 4)
    ]
    mixer_output = projected(heads, output_weight)
    chances = jax.nn.softmax(route_logits.T, axis=0)
    expert_output = combine(
        returned.reshape(experts * 4 * slots, -1), target, chances
    )
    return (mixer_output, expert_output)


def solution(mesh):
    names = ("ep_0", "ep_1", "Y", "h", "X", "p")
    finer = Mesh(mesh.devices.reshape(16, 2, 2, 2, 2, 2), names)
    in_specs = (
        P(EP, None),
        P(),
        P(None, TP),
        P(None, TP),
        P(None, TP),
        P(None, TP),
        P(TP),
        P(EP, None),
        P(),
        P(EP, None),
        P(EP, None),
        P(EP, None, TP),
        P(EP, None, TP),
        P(EP, None, TP),
    )
    out_specs = (P(EP, TP), P(EP, TP))
    return jax.shard_map(
        shards, mesh=finer, in_specs=in_specs, out_specs=out_specs, check_vma=False
    )
```

```python
import itertools

import jax
import jax.numpy as jnp
from jax import lax
from jax.experimental import pallas as pl
from jax.experimental.pallas import tpu as pltpu
from jax.sharding import Mesh
from jax.sharding import PartitionSpec as P

HEAD_DIM = 64
TOP_K = 4
WINDOW = 128
GRID_W = 64
EP = ("ep_0", "ep_1")
TP = ("Y", "h", "X", "p")

EPSILON = 1e-06
LIMIT = 7.0
SLOPE = 1.702
BASE = 10000.0


def swap(pieces, axis):
    return lax.all_to_all(pieces, axis, 0, 0, tiled=True)


def spread(shard, axis):
    return swap(jnp.broadcast_to(shard[None], (lax.axis_size(axis), *shard.shape)), axis)


def activate(gate, up):
    capped = jnp.minimum(gate, LIMIT)
    bounded = jnp.clip(up, -LIMIT, LIMIT)
    return (capped * jax.nn.sigmoid(SLOPE * capped) * (bounded + 1.0)).astype(jnp.bfloat16)


def dot(a, b):
    return jnp.dot(a, b, preferred_element_type=jnp.float32)


def tall(wide):
    k, n = wide.shape
    square = jnp.concatenate([wide, jnp.zeros((n - k, n), wide.dtype)], axis=0)
    return square.T


def dispatch(rows, gain, routes, weights, experts, slots, width):
    tokens = rows.shape[0]
    pairs = experts // 2
    tall_rows, columns = weights[0].shape

    def kernel(rows_ref, gain_ref, routes_ref, *refs):
        weight_refs, refs = refs[:3], refs[3:]
        out_ref, target_ref, stacked_ref, held_ref, here_ref, sems = refs
        rows_copy = pltpu.make_async_copy(rows_ref, here_ref, sems.at[6])
        rows_copy.start()
        arriving = [
            pltpu.make_async_copy(ref, held_ref.at[i], sems.at[i])
            for i, ref in enumerate(weight_refs)
        ]
        leaving = [
            pltpu.make_async_copy(
                held_ref.at[i], stacked_ref.at[pl.ds(i * tall_rows, tall_rows)], sems.at[3 + i]
            )
            for i in range(3)
        ]
        for copy in arriving:
            copy.start()
        block = 2 * lax.axis_index("Y") + lax.axis_index("X")
        rows_copy.wait()
        for come, go in zip(arriving, leaving):
            come.wait()
            go.start()
        values = here_ref[...].astype(jnp.float32)
        scale = lax.rsqrt(jnp.mean(values * values, axis=-1, keepdims=True) + EPSILON)
        start = pl.multiple_of(block * width, width)
        own = here_ref[:, pl.ds(start, width)].astype(jnp.float32)
        normed = (own * scale * gain_ref[:, pl.ds(start, width)]).astype(jnp.bfloat16)
        first = lax.broadcasted_iota(jnp.int32, (tokens, tokens), 0)
        second = lax.broadcasted_iota(jnp.int32, (tokens, tokens), 1)
        parity = lax.axis_index("p")
        expert = lax.broadcasted_iota(jnp.int32, (pairs, tokens), 0) * 2 + parity
        named = jnp.zeros((pairs, tokens), jnp.float32)
        for k in range(TOP_K):
            named = named + (routes_ref[k : k + 1, :] == expert).astype(jnp.float32)
        earlier = dot(named.astype(jnp.bfloat16), (first < second).astype(jnp.bfloat16))
        rank = jnp.where(named > 0.0, earlier.astype(jnp.int32), -1)
        rank = rank - lax.axis_index("h") * (2 * slots)
        slot = lax.broadcasted_iota(jnp.int32, (pairs, 2 * slots, tokens), 1)
        chosen = (rank[:, None, :] == slot).astype(jnp.float32)
        chosen = chosen.reshape(experts * slots, tokens).astype(jnp.bfloat16)
        out_ref[...] = dot(chosen, normed).astype(jnp.bfloat16)
        routed = tall(routes_ref[...].astype(jnp.float32))
        column = lax.broadcasted_iota(jnp.int32, (tokens, experts), 1)
        wanted = column.astype(jnp.float32)
        marks = [(routed[:, k : k + 1] == wanted).astype(jnp.float32) for k in range(TOP_K)]
        before = dot((second < first).astype(jnp.bfloat16), sum(marks).astype(jnp.bfloat16))
        before = before.astype(jnp.int32)
        core, half, spot = (before // slots) % 2, before // (2 * slots), before % slots
        position = (((column // 2) * 2 + core) * 2 + half) * 2 + column % 2
        position = (position * slots + spot).astype(jnp.float32)
        target_ref[...] = jnp.concatenate(
            [jnp.sum(mark * position, axis=1, keepdims=True) for mark in marks], axis=1
        ).astype(jnp.int32)
        for copy in leaving:
            copy.wait()

    vmem = pl.BlockSpec(memory_space=pltpu.VMEM)
    anywhere = pl.BlockSpec(memory_space=pl.ANY)
    return pl.pallas_call(
        kernel,
        out_shape=(
            jax.ShapeDtypeStruct((experts * slots, width), jnp.bfloat16),
            jax.ShapeDtypeStruct((tokens, TOP_K), jnp.int32),
            jax.ShapeDtypeStruct((3 * tall_rows, columns), jnp.bfloat16),
        ),
        in_specs=[anywhere] + [vmem] * 2 + [anywhere] * 3,
        out_specs=(vmem, vmem, anywhere),
        scratch_shapes=[
            pltpu.VMEM((3, tall_rows, columns), jnp.bfloat16),
            pltpu.VMEM(rows.shape, rows.dtype),
            pltpu.SemaphoreType.DMA((7,)),
        ],
        name="dispatch",
    )(rows, gain[None, :], routes.T, *weights)


def device_pairs(where):
    names = list(itertools.product(range(2), repeat=5))
    number = {name: i for i, name in enumerate(names)}
    return [(number[n], number[where(*n)]) for n in names if where(*n) is not None]


def gather_shares(own):
    axes = ("ep_1", "Y", "h", "X", "p")

    def outer(c, Y, h, X, p):
        return (c, Y, 1 - h, X, p) if c == p else (1 - c, Y, h, X, 1 - p)

    def cross(c, Y, h, X, p):
        return (1 - c, Y, h, X, p) if c == p else (c, Y, 1 - h, X, 1 - p)

    def trade(c, Y, h, X, p):
        return (1 - c, Y, h, X, p)

    def give(c, Y, h, X, p):
        return (1 - c, Y, h, X, p) if c == p else None

    first = lax.ppermute(own, axes, device_pairs(outer))
    second = lax.ppermute(own, axes, device_pairs(cross))
    third = lax.ppermute(first, axes, device_pairs(trade))
    fourth = lax.ppermute(second, axes, device_pairs(give))
    return own, first, second, third, fourth


def share_order():
    c, h, p = (lax.axis_index(a) for a in ("ep_1", "h", "p"))
    native = c == p
    own, up = 2 * h + p, 2 * (1 - h) + p
    side, across = 2 * h + (1 - p), 2 * (1 - h) + (1 - p)
    return native, [own, jnp.where(native, up, side), across, jnp.where(native, side, up)]


def copy_share(native, shares, index, start, size, target, sem):
    own, first, second, third, fourth = shares
    rows = pl.ds(start, size)
    if index in (1, 3):
        source = first if index == 1 else third
        pltpu.make_async_copy(source.at[rows], target, sem).start()
        return
    here, there = (own, second) if index == 0 else (second, fourth)

    @pl.when(native)
    def _():
        pltpu.make_async_copy(here.at[rows], target, sem).start()

    @pl.when(jnp.logical_not(native))
    def _():
        pltpu.make_async_copy(there.at[rows], target, sem).start()


def gated(rows, mixed, shares, arrived):
    parts, n, k = rows.shape
    u = shares[0].shape[1]
    j = mixed.shape[1]
    whole = parts * k

    def kernel(rows_ref, mixed_ref, _, *refs):
        shares, refs = refs[:5], refs[5:]
        out_ref, here_ref, weights_ref, hidden_ref, sems, row_sems, out_sems = refs
        native, order = share_order()
        arrivals = [
            pltpu.make_async_copy(rows_ref.at[part], here_ref.at[part], row_sems.at[part])
            for part in range(parts)
        ]
        arrivals.append(
            pltpu.make_async_copy(
                mixed_ref, hidden_ref.at[:, pl.ds(4 * u, j)], row_sems.at[parts]
            )
        )
        targets = [
            (weights_ref.at[i, :, pl.ds(side * u, u)], sems.at[i, side])
            for i in range(4)
            for side in range(2)
        ]
        for copy in arrivals:
            copy.start()
        for i in range(4):
            for side in range(2):
                copy_share(native, shares, i, side * whole, whole, *targets[2 * i + side])
        for copy in arrivals:
            copy.wait()
        for target in targets:
            pltpu.make_async_copy(shares[1].at[pl.ds(0, whole)], *target).wait()
        for i in range(4):
            total = dot(here_ref[0], weights_ref[i, :k, :])
            for part in range(1, parts):
                total = total + dot(here_ref[part], weights_ref[i, part * k : (part + 1) * k, :])
            lane = pl.multiple_of(order[i] * u, u)
            hidden_ref[:, pl.ds(lane, u)] = activate(total[:, :u], total[:, u:])
        leaving = [
            pltpu.make_async_copy(hidden_ref, out_ref.at[copy], out_sems.at[copy])
            for copy in range(parts)
        ]
        for copy in leaving:
            copy.start()
        for copy in leaving:
            copy.wait()

    anywhere = pl.BlockSpec(memory_space=pl.ANY)
    return pl.pallas_call(
        kernel,
        out_shape=jax.ShapeDtypeStruct((parts, n, 4 * u + j), jnp.bfloat16),
        in_specs=[anywhere] * 8,
        out_specs=anywhere,
        scratch_shapes=[
            pltpu.VMEM((parts, n, k), jnp.bfloat16),
            pltpu.VMEM((4, whole, 2 * u), jnp.bfloat16),
            pltpu.VMEM((n, 4 * u + j), jnp.bfloat16),
            pltpu.SemaphoreType.DMA((4, 2)),
            pltpu.SemaphoreType.DMA((parts + 1,)),
            pltpu.SemaphoreType.DMA((parts,)),
        ],
        name="gated",
    )(rows, mixed, arrived, *shares)


def lowered(hidden, shares, slots):
    parts, n, wide = hidden.shape
    f = shares[0].shape[1]
    k = 4 * f
    j = wide - k
    whole = parts * k
    half = k // 2

    def kernel(hidden_ref, *refs):
        shares, refs = refs[:5], refs[5:]
        out_ref, heads_ref, here_ref, weights_ref, sems, row_sems = refs
        native, order = share_order()
        targets = [
            (weights_ref.at[i // 2, :, pl.ds((i % 2) * f, f)], sems.at[i]) for i in range(4)
        ]
        arrivals = [
            pltpu.make_async_copy(hidden_ref.at[part], here_ref.at[part], row_sems.at[part])
            for part in range(parts)
        ]
        heads = pltpu.make_async_copy(
            here_ref.at[:, :, pl.ds(k, j)], heads_ref, row_sems.at[parts]
        )
        for copy in arrivals:
            copy.start()
        for i in range(4):
            copy_share(native, shares, i, 2 * whole, whole, *targets[i])
        for copy in arrivals:
            copy.wait()
        heads.start()
        for target in targets:
            pltpu.make_async_copy(shares[1].at[pl.ds(0, whole)], *target).wait()
        for pair in range(2):
            total = jnp.zeros((n, 2 * f), jnp.float32)
            for Y, X, h in itertools.product(range(2), repeat=3):
                unit = (8 * Y + 4 * h + 2 * X) * f
                piece = here_ref[2 * Y + X, :, h * half : (h + 1) * half]
                total = total + dot(piece, weights_ref[pair, unit : unit + half, :])
            rounded = total.astype(jnp.bfloat16).reshape(n // slots, slots, 2 * f)
            out_ref[:, order[2 * pair]] = rounded[:, :, :f]
            out_ref[:, order[2 * pair + 1]] = rounded[:, :, f:]
        heads.wait()

    vmem = pl.BlockSpec(memory_space=pltpu.VMEM)
    anywhere = pl.BlockSpec(memory_space=pl.ANY)
    return pl.pallas_call(
        kernel,
        out_shape=(
            jax.ShapeDtypeStruct((n // slots, 4, slots, f), jnp.bfloat16),
            jax.ShapeDtypeStruct((parts, n, j), jnp.bfloat16),
        ),
        in_specs=[anywhere] * 6,
        out_specs=(vmem, anywhere),
        scratch_shapes=[
            pltpu.VMEM((parts, n, wide), jnp.bfloat16),
            pltpu.VMEM((2, whole, 2 * f), jnp.bfloat16),
            pltpu.SemaphoreType.DMA((4,)),
            pltpu.SemaphoreType.DMA((parts + 1,)),
        ],
        name="lowered",
    )(hidden, *shares)


def selectors(target, logits, slots):
    tokens = target.shape[0]

    def kernel(target_ref, logits_ref, out_ref):
        chances = tall(jax.nn.softmax(logits_ref[...], axis=0))
        lane = lax.broadcasted_iota(jnp.int32, (tokens, slots), 1)
        rest = jnp.zeros((tokens, slots), jnp.float32)
        for k in range(TOP_K):
            rest = jnp.where(target_ref[:, k : k + 1] == lane, chances[:, k : k + 1], rest)
        for part in range(3):
            rounded = rest.astype(jnp.bfloat16)
            out_ref[part * tokens : (part + 1) * tokens, :] = rounded
            rest = rest - rounded.astype(jnp.float32)

    vmem = pl.BlockSpec(memory_space=pltpu.VMEM)
    return pl.pallas_call(
        kernel,
        out_shape=jax.ShapeDtypeStruct((3 * tokens, slots), jnp.bfloat16),
        in_specs=[vmem] * 2,
        out_specs=vmem,
        name="selectors",
    )(target, logits)


def rotary_tables(first, rows, width):
    quarter = HEAD_DIM // 4
    lane = jnp.arange(width, dtype=jnp.int32)
    frequency = BASE ** (-(lane % quarter).astype(jnp.float32) / quarter)
    at = jnp.arange(GRID_W + rows, dtype=jnp.int32)
    place = jnp.where(at < GRID_W, at, at - GRID_W + first)
    angle = place.astype(jnp.float32)[:, None] * frequency
    sign = jnp.where(lane % (2 * quarter) < quarter, -1.0, 1.0)
    return jnp.cos(angle), jnp.sin(angle) * sign


def projections(rows, gain, query_weight, key_weight, value_weight):
    tokens, _ = rows.shape
    width = query_weight.shape[1]
    half = width // 2
    quarter = HEAD_DIM // 4
    spans = tokens // GRID_W
    cosine, sine = rotary_tables(lax.axis_index(EP) * spans, spans, width)

    def kernel(
        rows_ref, gain_ref, query_ref, key_ref, value_ref, cos_ref, sin_ref, out_ref, *pair_refs
    ):
        values = rows_ref[...].astype(jnp.float32)
        scale = lax.rsqrt(jnp.mean(values * values, axis=-1, keepdims=True) + EPSILON)
        normed = (values * scale * gain_ref[...]).astype(jnp.bfloat16)
        lane = lax.broadcasted_iota(jnp.int32, (tokens, width), 1)
        near = lane % (2 * quarter) < quarter
        by_row = lax.broadcasted_iota(jnp.int32, (GRID_W, width), 1) % HEAD_DIM < HEAD_DIM // 2

        def table(ref):
            columns = ref[:GRID_W, :]
            parts = [
                jnp.where(by_row, ref[GRID_W + i : GRID_W + i + 1, :], columns)
                for i in range(spans)
            ]
            return jnp.concatenate(parts, axis=0)

        cos, sin = table(cos_ref), table(sin_ref)

        def turned(a):
            partner = jnp.where(
                near, pltpu.roll(a, width - quarter, 1), pltpu.roll(a, quarter, 1)
            )
            return (a * cos + partner * sin).astype(jnp.bfloat16)

        def flipped(weight_ref):
            return lax.dot_general(
                normed, weight_ref[...], (((1,), (1,)), ((), ())), preferred_element_type=jnp.float32
            )

        out_ref[...] = turned(dot(normed, query_ref[...]))
        keys, mine = flipped(key_ref), flipped(value_ref)
        both = jnp.concatenate([keys, mine], axis=1)
        rounded = jnp.where(lane < half, turned(both), both.astype(jnp.bfloat16))
        for i, ref in enumerate(pair_refs):
            ref[...] = rounded[i * WINDOW : (i + 1) * WINDOW]

    vmem = pl.BlockSpec(memory_space=pltpu.VMEM)
    return pl.pallas_call(
        kernel,
        out_shape=[jax.ShapeDtypeStruct((tokens, width), jnp.bfloat16)]
        + [jax.ShapeDtypeStruct((WINDOW, width), jnp.bfloat16)] * (tokens // WINDOW),
        in_specs=[vmem] * 7,
        out_specs=[vmem] * (1 + tokens // WINDOW),
        name="projections",
    )(rows, gain[None, :], query_weight, key_weight.T, value_weight.T, cosine, sine)


def banded(query, pieces, sinks):
    tokens, width = query.shape
    blocks = tokens // WINDOW
    heads = width // HEAD_DIM

    def kernel(sink_ref, query_ref, *refs):
        piece_refs, out_ref = refs[:-1], refs[-1]
        place, last = lax.axis_index(EP), lax.axis_size(EP) - 1
        row = lax.broadcasted_iota(jnp.int32, (WINDOW, 3 * WINDOW), 0)
        column = lax.broadcasted_iota(jnp.int32, (WINDOW, 3 * WINDOW), 1)
        band = (column >= row) & (column <= row + 2 * WINDOW)
        for n in range(blocks):
            near = jnp.concatenate([piece_refs[n + i][...] for i in range(3)], axis=0)
            keys, values = near[:, :HEAD_DIM], near[:, HEAD_DIM:]
            least = jnp.where(place == 0, WINDOW, 0) if n == 0 else 0
            most = jnp.where(place == last, 2 * WINDOW, 3 * WINDOW) if n == blocks - 1 else 3 * WINDOW
            allowed = band & (column >= least) & (column < most)
            outs = []
            for r in range(heads):
                here = query_ref[n * WINDOW : (n + 1) * WINDOW, r * HEAD_DIM : (r + 1) * HEAD_DIM]
                scores = lax.dot_general(
                    here, keys, (((1,), (1,)), ((), ())), preferred_element_type=jnp.float32
                )
                scores = jnp.where(allowed, scores * HEAD_DIM ** (-0.5), -1e30)
                sink = sink_ref[r]
                top = jnp.maximum(jnp.max(scores, axis=-1, keepdims=True), sink)
                weights = jnp.exp(scores - top)
                total = jnp.sum(weights, axis=-1, keepdims=True) + jnp.exp(sink - top)
                outs.append(dot((weights / total).astype(jnp.bfloat16), values))
            mixed = jnp.concatenate(outs, axis=1).astype(jnp.bfloat16)
            out_ref[n * WINDOW : (n + 1) * WINDOW, :] = mixed

    vmem = pl.BlockSpec(memory_space=pltpu.VMEM)
    return pl.pallas_call(
        kernel,
        out_shape=jax.ShapeDtypeStruct((tokens, width), jnp.bfloat16),
        in_specs=[pl.BlockSpec(memory_space=pltpu.SMEM)] + [vmem] * (blocks + 3),
        out_specs=vmem,
        name="banded",
    )(sinks, query, *pieces)


def attention(mixer_input, mixer_gain, query_weight, key_weight, value_weight, sink_logit):
    query, *pieces = projections(mixer_input, mixer_gain, query_weight, key_weight, value_weight)
    up = [(i, i + 1) for i in range(lax.axis_size(EP) - 1)]
    before = lax.ppermute(pieces[-1], EP, up)
    after = lax.ppermute(pieces[0], EP, [(j, i) for i, j in up])
    return banded(query, [before, *pieces, after], sink_logit)


def partial_sums(heads, columns):
    parts, n, _ = heads.shape
    f = columns[0].shape[2]

    def kernel(heads_ref, *refs):
        columns_refs, out_refs = refs[:4], refs[4:]
        for columns_ref, out_ref in zip(columns_refs, out_refs):
            total = dot(heads_ref[0], columns_ref[0])
            for part in range(1, parts):
                total = total + dot(heads_ref[part], columns_ref[part])
            out_ref[...] = total

    vmem = pl.BlockSpec(memory_space=pltpu.VMEM)
    return pl.pallas_call(
        kernel,
        out_shape=[jax.ShapeDtypeStruct((n, f), jnp.float32)] * 4,
        in_specs=[vmem] * 5,
        out_specs=[vmem] * 4,
        name="partial_sums",
    )(heads, *columns)


def shards(
    mixer_input,
    mixer_gain,
    query_weight,
    key_weight,
    value_weight,
    output_weight,
    sink_logit,
    expert_input,
    expert_gain,
    routes,
    route_logits,
    gate_weight,
    up_weight,
    down_weight,
):
    experts = lax.axis_size(EP)
    rows_here, features = expert_input.shape
    slots = 2 * rows_here * TOP_K // experts // 4
    width = features // 4
    weights = (gate_weight[0], up_weight[0], down_weight[0])
    outgoing, target, own = dispatch(
        expert_input, expert_gain, routes, weights, experts, slots, width
    )
    shares = gather_shares(own)
    received = swap(outgoing.reshape(experts, slots, width), EP)
    mixed = attention(mixer_input, mixer_gain, query_weight, key_weight, value_weight, sink_logit)
    rows = spread(received.reshape(experts * slots, width), ("Y", "X"))
    arrived = shares[3][:8] + shares[4][:8]
    inner = gated(rows, mixed, shares, arrived)
    hidden = swap(inner, ("Y", "X"))
    result, heads = lowered(hidden, shares, slots)
    returned = swap(result.reshape(4 * experts, slots, -1), (*EP, "h", "p"))
    around = [[(i, i ^ k) for i in range(4)] for k in range(4)]
    size = mixed.shape[1]
    blocks = output_weight.reshape(2, 2, 2, 2, size, -1)
    columns = []
    for k in range(4):
        h, p = lax.axis_index("h") ^ (k // 2), lax.axis_index("p") ^ (k % 2)
        piece = lax.dynamic_slice_in_dim(blocks, h, 1, 1)
        piece = lax.dynamic_slice_in_dim(piece, p, 1, 3).reshape(4, size, -1)
        columns.append(lax.ppermute(piece, ("h", "p"), around[k]) if k else piece)
    own_sum, *sums = partial_sums(heads, columns)
    for k in range(1, 4):
        own_sum = own_sum + lax.ppermute(sums[k - 1], ("h", "p"), around[k])
    mixer_output = own_sum.astype(jnp.bfloat16)
    chances = selectors(target, route_logits.T, experts * 4 * slots)
    parts = dot(chances, returned.reshape(experts * 4 * slots, -1))
    parts = parts.reshape(3, rows_here, -1)
    expert_output = (parts[0] + (parts[1] + parts[2])).astype(jnp.bfloat16)
    return (mixer_output, expert_output)


def solution(mesh):
    names = ("ep_0", "ep_1", "Y", "h", "X", "p")
    finer = Mesh(mesh.devices.reshape(16, 2, 2, 2, 2, 2), names)
    in_specs = (
        P(EP, None),
        P(),
        P(None, TP),
        P(None, TP),
        P(None, TP),
        P(None, TP),
        P(TP),
        P(EP, None),
        P(),
        P(EP, None),
        P(EP, None),
        P(EP, None, TP),
        P(EP, None, TP),
        P(EP, None, TP),
    )
    out_specs = (P(EP, TP), P(EP, TP))
    return jax.shard_map(
        shards, mesh=finer, in_specs=in_specs, out_specs=out_specs, check_vma=False
    )
```

```python
import itertools

import jax
import jax.numpy as jnp
from jax import lax
from jax.experimental import pallas as pl
from jax.experimental.pallas import tpu as pltpu
from jax.sharding import Mesh
from jax.sharding import PartitionSpec as P

HEAD_DIM = 64
TOP_K = 4
WINDOW = 128
GRID_W = 64
EP = ("ep_0", "ep_1")
TP = ("Y", "h", "X", "p")

EPSILON = 1e-06
LIMIT = 7.0
SLOPE = 1.702
BASE = 10000.0


def swap(pieces, axis):
    return lax.all_to_all(pieces, axis, 0, 0, tiled=True)


def spread(shard, axis):
    return swap(jnp.broadcast_to(shard[None], (lax.axis_size(axis), *shard.shape)), axis)


def activate(gate, up):
    capped = jnp.minimum(gate, LIMIT)
    bounded = jnp.clip(up, -LIMIT, LIMIT)
    return (capped * jax.nn.sigmoid(SLOPE * capped) * (bounded + 1.0)).astype(jnp.bfloat16)


def dot(a, b):
    return jnp.dot(a, b, preferred_element_type=jnp.float32)


def tall(wide):
    k, n = wide.shape
    square = jnp.concatenate([wide, jnp.zeros((n - k, n), wide.dtype)], axis=0)
    return square.T


def dispatch(rows, gain, routes, experts, slots, width):
    tokens = rows.shape[0]
    pairs = experts // 2

    def kernel(rows_ref, gain_ref, routes_ref, out_ref, target_ref):
        block = 2 * lax.axis_index("Y") + lax.axis_index("X")
        values = rows_ref[...].astype(jnp.float32)
        scale = lax.rsqrt(jnp.mean(values * values, axis=-1, keepdims=True) + EPSILON)
        start = pl.multiple_of(block * width, width)
        own = rows_ref[:, pl.ds(start, width)].astype(jnp.float32)
        normed = (own * scale * gain_ref[:, pl.ds(start, width)]).astype(jnp.bfloat16)
        first = lax.broadcasted_iota(jnp.int32, (tokens, tokens), 0)
        second = lax.broadcasted_iota(jnp.int32, (tokens, tokens), 1)
        parity = lax.axis_index("p")
        expert = lax.broadcasted_iota(jnp.int32, (pairs, tokens), 0) * 2 + parity
        named = jnp.zeros((pairs, tokens), jnp.float32)
        for k in range(TOP_K):
            named = named + (routes_ref[k : k + 1, :] == expert).astype(jnp.float32)
        earlier = dot(named.astype(jnp.bfloat16), (first < second).astype(jnp.bfloat16))
        rank = jnp.where(named > 0.0, earlier.astype(jnp.int32), -1)
        rank = rank - lax.axis_index("h") * (2 * slots)
        slot = lax.broadcasted_iota(jnp.int32, (pairs, 2 * slots, tokens), 1)
        chosen = (rank[:, None, :] == slot).astype(jnp.float32)
        chosen = chosen.reshape(experts * slots, tokens).astype(jnp.bfloat16)
        out_ref[...] = dot(chosen, normed).astype(jnp.bfloat16)
        routed = tall(routes_ref[...].astype(jnp.float32))
        column = lax.broadcasted_iota(jnp.int32, (tokens, experts), 1)
        wanted = column.astype(jnp.float32)
        marks = [(routed[:, k : k + 1] == wanted).astype(jnp.float32) for k in range(TOP_K)]
        before = dot((second < first).astype(jnp.bfloat16), sum(marks).astype(jnp.bfloat16))
        before = before.astype(jnp.int32)
        core, half, spot = (before // slots) % 2, before // (2 * slots), before % slots
        position = (((column // 2) * 2 + core) * 2 + half) * 2 + column % 2
        position = (position * slots + spot).astype(jnp.float32)
        target_ref[...] = jnp.concatenate(
            [jnp.sum(mark * position, axis=1, keepdims=True) for mark in marks], axis=1
        ).astype(jnp.int32)

    vmem = pl.BlockSpec(memory_space=pltpu.VMEM)
    return pl.pallas_call(
        kernel,
        out_shape=(
            jax.ShapeDtypeStruct((experts * slots, width), jnp.bfloat16),
            jax.ShapeDtypeStruct((tokens, TOP_K), jnp.int32),
        ),
        in_specs=[vmem] * 3,
        out_specs=(vmem, vmem),
        name="dispatch",
    )(rows, gain[None, :], routes.T)


def device_pairs(where):
    names = list(itertools.product(range(2), repeat=5))
    number = {name: i for i, name in enumerate(names)}
    return [(number[n], number[where(*n)]) for n in names if where(*n) is not None]


def gather_shares(own):
    axes = ("ep_1", "Y", "h", "X", "p")

    def outer(c, Y, h, X, p):
        return (c, Y, 1 - h, X, p) if c == p else (1 - c, Y, h, X, 1 - p)

    def cross(c, Y, h, X, p):
        return (1 - c, Y, h, X, p) if c == p else (c, Y, 1 - h, X, 1 - p)

    def trade(c, Y, h, X, p):
        return (1 - c, Y, h, X, p)

    def give(c, Y, h, X, p):
        return (1 - c, Y, h, X, p) if c == p else None

    first = lax.ppermute(own, axes, device_pairs(outer))
    second = lax.ppermute(own, axes, device_pairs(cross))
    third = lax.ppermute(first, axes, device_pairs(trade))
    fourth = lax.ppermute(second, axes, device_pairs(give))
    return own, first, second, third, fourth


def share_order():
    c, h, p = (lax.axis_index(a) for a in ("ep_1", "h", "p"))
    native = c == p
    own, up = 2 * h + p, 2 * (1 - h) + p
    side, across = 2 * h + (1 - p), 2 * (1 - h) + (1 - p)
    return native, [own, jnp.where(native, up, side), across, jnp.where(native, side, up)]


def copy_share(native, shares, index, start, size, target, sem):
    own, first, second, third, fourth = shares
    rows = pl.ds(start, size)
    if index in (1, 3):
        source = first if index == 1 else third
        pltpu.make_async_copy(source.at[rows], target, sem).start()
        return
    here, there = (own, second) if index == 0 else (second, fourth)

    @pl.when(native)
    def _():
        pltpu.make_async_copy(here.at[rows], target, sem).start()

    @pl.when(jnp.logical_not(native))
    def _():
        pltpu.make_async_copy(there.at[rows], target, sem).start()


def gated(rows, mixed, shares, arrived):
    parts, n, k = rows.shape
    u = shares[0].shape[1]
    j = mixed.shape[1]
    whole = parts * k

    def kernel(rows_ref, mixed_ref, _, *refs):
        shares, refs = refs[:5], refs[5:]
        out_ref, here_ref, weights_ref, hidden_ref, sems, row_sems, out_sems = refs
        native, order = share_order()
        arrivals = [
            pltpu.make_async_copy(rows_ref.at[part], here_ref.at[part], row_sems.at[part])
            for part in range(parts)
        ]
        arrivals.append(
            pltpu.make_async_copy(
                mixed_ref, hidden_ref.at[:, pl.ds(4 * u, j)], row_sems.at[parts]
            )
        )
        targets = [
            (weights_ref.at[i, :, pl.ds(side * u, u)], sems.at[i, side])
            for i in range(4)
            for side in range(2)
        ]
        for copy in arrivals:
            copy.start()
        for i in range(4):
            for side in range(2):
                copy_share(native, shares, i, side * whole, whole, *targets[2 * i + side])
        for copy in arrivals:
            copy.wait()
        for target in targets:
            pltpu.make_async_copy(shares[1].at[pl.ds(0, whole)], *target).wait()
        for i in range(4):
            total = dot(here_ref[0], weights_ref[i, :k, :])
            for part in range(1, parts):
                total = total + dot(here_ref[part], weights_ref[i, part * k : (part + 1) * k, :])
            lane = pl.multiple_of(order[i] * u, u)
            hidden_ref[:, pl.ds(lane, u)] = activate(total[:, :u], total[:, u:])
        leaving = [
            pltpu.make_async_copy(hidden_ref, out_ref.at[copy], out_sems.at[copy])
            for copy in range(parts)
        ]
        for copy in leaving:
            copy.start()
        for copy in leaving:
            copy.wait()

    anywhere = pl.BlockSpec(memory_space=pl.ANY)
    return pl.pallas_call(
        kernel,
        out_shape=jax.ShapeDtypeStruct((parts, n, 4 * u + j), jnp.bfloat16),
        in_specs=[anywhere] * 8,
        out_specs=anywhere,
        scratch_shapes=[
            pltpu.VMEM((parts, n, k), jnp.bfloat16),
            pltpu.VMEM((4, whole, 2 * u), jnp.bfloat16),
            pltpu.VMEM((n, 4 * u + j), jnp.bfloat16),
            pltpu.SemaphoreType.DMA((4, 2)),
            pltpu.SemaphoreType.DMA((parts + 1,)),
            pltpu.SemaphoreType.DMA((parts,)),
        ],
        name="gated",
    )(rows, mixed, arrived, *shares)


def lowered(hidden, shares, landed, slots):
    parts, n, wide = hidden.shape
    f = shares[0].shape[1]
    k = 4 * f
    j = wide - k
    whole = parts * k
    half = k // 2

    def kernel(hidden_ref, _, *refs):
        shares, refs = refs[:5], refs[5:]
        out_ref, heads_ref, here_ref, weights_ref, sems, row_sems = refs
        native, order = share_order()
        targets = [
            (weights_ref.at[i // 2, :, pl.ds((i % 2) * f, f)], sems.at[i]) for i in range(4)
        ]
        arrivals = [
            pltpu.make_async_copy(hidden_ref.at[part], here_ref.at[part], row_sems.at[part])
            for part in range(parts)
        ]
        heads = pltpu.make_async_copy(
            here_ref.at[:, :, pl.ds(k, j)], heads_ref, row_sems.at[parts]
        )
        for copy in arrivals:
            copy.start()
        for i in range(4):
            copy_share(native, shares, i, 0, whole, *targets[i])
        for copy in arrivals:
            copy.wait()
        heads.start()
        for target in targets:
            pltpu.make_async_copy(shares[1].at[pl.ds(0, whole)], *target).wait()
        for pair in range(2):
            total = jnp.zeros((n, 2 * f), jnp.float32)
            for Y, X, h in itertools.product(range(2), repeat=3):
                unit = (8 * Y + 4 * h + 2 * X) * f
                piece = here_ref[2 * Y + X, :, h * half : (h + 1) * half]
                total = total + dot(piece, weights_ref[pair, unit : unit + half, :])
            rounded = total.astype(jnp.bfloat16).reshape(n // slots, slots, 2 * f)
            out_ref[:, order[2 * pair]] = rounded[:, :, :f]
            out_ref[:, order[2 * pair + 1]] = rounded[:, :, f:]
        heads.wait()

    vmem = pl.BlockSpec(memory_space=pltpu.VMEM)
    anywhere = pl.BlockSpec(memory_space=pl.ANY)
    return pl.pallas_call(
        kernel,
        out_shape=(
            jax.ShapeDtypeStruct((n // slots, 4, slots, f), jnp.bfloat16),
            jax.ShapeDtypeStruct((parts, n, j), jnp.bfloat16),
        ),
        in_specs=[anywhere] * 7,
        out_specs=(vmem, anywhere),
        scratch_shapes=[
            pltpu.VMEM((parts, n, wide), jnp.bfloat16),
            pltpu.VMEM((2, whole, 2 * f), jnp.bfloat16),
            pltpu.SemaphoreType.DMA((4,)),
            pltpu.SemaphoreType.DMA((parts + 1,)),
        ],
        name="lowered",
    )(hidden, landed, *shares)


def selectors(target, logits, slots):
    tokens = target.shape[0]

    def kernel(target_ref, logits_ref, out_ref):
        chances = tall(jax.nn.softmax(logits_ref[...], axis=0))
        lane = lax.broadcasted_iota(jnp.int32, (tokens, slots), 1)
        rest = jnp.zeros((tokens, slots), jnp.float32)
        for k in range(TOP_K):
            rest = jnp.where(target_ref[:, k : k + 1] == lane, chances[:, k : k + 1], rest)
        for part in range(3):
            rounded = rest.astype(jnp.bfloat16)
            out_ref[part * tokens : (part + 1) * tokens, :] = rounded
            rest = rest - rounded.astype(jnp.float32)

    vmem = pl.BlockSpec(memory_space=pltpu.VMEM)
    return pl.pallas_call(
        kernel,
        out_shape=jax.ShapeDtypeStruct((3 * tokens, slots), jnp.bfloat16),
        in_specs=[vmem] * 2,
        out_specs=vmem,
        name="selectors",
    )(target, logits)


def rotary_tables(first, rows, width):
    quarter = HEAD_DIM // 4
    lane = jnp.arange(width, dtype=jnp.int32)
    frequency = BASE ** (-(lane % quarter).astype(jnp.float32) / quarter)
    at = jnp.arange(GRID_W + rows, dtype=jnp.int32)
    place = jnp.where(at < GRID_W, at, at - GRID_W + first)
    angle = place.astype(jnp.float32)[:, None] * frequency
    sign = jnp.where(lane % (2 * quarter) < quarter, -1.0, 1.0)
    return jnp.cos(angle), jnp.sin(angle) * sign


def projections(rows, gain, query_weight, key_weight, value_weight):
    tokens, _ = rows.shape
    width = query_weight.shape[1]
    half = width // 2
    quarter = HEAD_DIM // 4
    spans = tokens // GRID_W
    cosine, sine = rotary_tables(lax.axis_index(EP) * spans, spans, width)

    def kernel(
        rows_ref, gain_ref, query_ref, key_ref, value_ref, cos_ref, sin_ref, out_ref, *pair_refs
    ):
        values = rows_ref[...].astype(jnp.float32)
        scale = lax.rsqrt(jnp.mean(values * values, axis=-1, keepdims=True) + EPSILON)
        normed = (values * scale * gain_ref[...]).astype(jnp.bfloat16)
        lane = lax.broadcasted_iota(jnp.int32, (tokens, width), 1)
        near = lane % (2 * quarter) < quarter
        by_row = lax.broadcasted_iota(jnp.int32, (GRID_W, width), 1) % HEAD_DIM < HEAD_DIM // 2

        def table(ref):
            columns = ref[:GRID_W, :]
            parts = [
                jnp.where(by_row, ref[GRID_W + i : GRID_W + i + 1, :], columns)
                for i in range(spans)
            ]
            return jnp.concatenate(parts, axis=0)

        cos, sin = table(cos_ref), table(sin_ref)

        def turned(a):
            partner = jnp.where(
                near, pltpu.roll(a, width - quarter, 1), pltpu.roll(a, quarter, 1)
            )
            return (a * cos + partner * sin).astype(jnp.bfloat16)

        def flipped(weight_ref):
            return lax.dot_general(
                normed, weight_ref[...], (((1,), (1,)), ((), ())), preferred_element_type=jnp.float32
            )

        out_ref[...] = turned(dot(normed, query_ref[...]))
        keys, mine = flipped(key_ref), flipped(value_ref)
        both = jnp.concatenate([keys, mine], axis=1)
        rounded = jnp.where(lane < half, turned(both), both.astype(jnp.bfloat16))
        for i, ref in enumerate(pair_refs):
            ref[...] = rounded[i * WINDOW : (i + 1) * WINDOW]

    vmem = pl.BlockSpec(memory_space=pltpu.VMEM)
    return pl.pallas_call(
        kernel,
        out_shape=[jax.ShapeDtypeStruct((tokens, width), jnp.bfloat16)]
        + [jax.ShapeDtypeStruct((WINDOW, width), jnp.bfloat16)] * (tokens // WINDOW),
        in_specs=[vmem] * 7,
        out_specs=[vmem] * (1 + tokens // WINDOW),
        name="projections",
    )(rows, gain[None, :], query_weight, key_weight.T, value_weight.T, cosine, sine)


def banded(query, pieces, sinks):
    tokens, width = query.shape
    blocks = tokens // WINDOW
    heads = width // HEAD_DIM

    def kernel(sink_ref, query_ref, *refs):
        piece_refs, out_ref = refs[:-1], refs[-1]
        place, last = lax.axis_index(EP), lax.axis_size(EP) - 1
        row = lax.broadcasted_iota(jnp.int32, (WINDOW, 3 * WINDOW), 0)
        column = lax.broadcasted_iota(jnp.int32, (WINDOW, 3 * WINDOW), 1)
        band = (column >= row) & (column <= row + 2 * WINDOW)
        for n in range(blocks):
            near = jnp.concatenate([piece_refs[n + i][...] for i in range(3)], axis=0)
            keys, values = near[:, :HEAD_DIM], near[:, HEAD_DIM:]
            least = jnp.where(place == 0, WINDOW, 0) if n == 0 else 0
            most = jnp.where(place == last, 2 * WINDOW, 3 * WINDOW) if n == blocks - 1 else 3 * WINDOW
            allowed = band & (column >= least) & (column < most)
            outs = []
            for r in range(heads):
                here = query_ref[n * WINDOW : (n + 1) * WINDOW, r * HEAD_DIM : (r + 1) * HEAD_DIM]
                scores = lax.dot_general(
                    here, keys, (((1,), (1,)), ((), ())), preferred_element_type=jnp.float32
                )
                scores = jnp.where(allowed, scores * HEAD_DIM ** (-0.5), -1e30)
                sink = sink_ref[r]
                top = jnp.maximum(jnp.max(scores, axis=-1, keepdims=True), sink)
                weights = jnp.exp(scores - top)
                total = jnp.sum(weights, axis=-1, keepdims=True) + jnp.exp(sink - top)
                outs.append(dot((weights / total).astype(jnp.bfloat16), values))
            mixed = jnp.concatenate(outs, axis=1).astype(jnp.bfloat16)
            out_ref[n * WINDOW : (n + 1) * WINDOW, :] = mixed

    vmem = pl.BlockSpec(memory_space=pltpu.VMEM)
    return pl.pallas_call(
        kernel,
        out_shape=jax.ShapeDtypeStruct((tokens, width), jnp.bfloat16),
        in_specs=[pl.BlockSpec(memory_space=pltpu.SMEM)] + [vmem] * (blocks + 3),
        out_specs=vmem,
        name="banded",
    )(sinks, query, *pieces)


def attention(mixer_input, mixer_gain, query_weight, key_weight, value_weight, sink_logit):
    query, *pieces = projections(mixer_input, mixer_gain, query_weight, key_weight, value_weight)
    up = [(i, i + 1) for i in range(lax.axis_size(EP) - 1)]
    before = lax.ppermute(pieces[-1], EP, up)
    after = lax.ppermute(pieces[0], EP, [(j, i) for i, j in up])
    return banded(query, [before, *pieces, after], sink_logit)


def partial_sums(heads, columns):
    parts, n, _ = heads.shape
    f = columns[0].shape[2]

    def kernel(heads_ref, *refs):
        columns_refs, out_refs = refs[:4], refs[4:]
        for columns_ref, out_ref in zip(columns_refs, out_refs):
            total = dot(heads_ref[0], columns_ref[0])
            for part in range(1, parts):
                total = total + dot(heads_ref[part], columns_ref[part])
            out_ref[...] = total

    vmem = pl.BlockSpec(memory_space=pltpu.VMEM)
    return pl.pallas_call(
        kernel,
        out_shape=[jax.ShapeDtypeStruct((n, f), jnp.float32)] * 4,
        in_specs=[vmem] * 5,
        out_specs=[vmem] * 4,
        name="partial_sums",
    )(heads, *columns)


def shards(
    mixer_input,
    mixer_gain,
    query_weight,
    key_weight,
    value_weight,
    output_weight,
    sink_logit,
    expert_input,
    expert_gain,
    routes,
    route_logits,
    gate_weight,
    up_weight,
    down_weight,
):
    experts = lax.axis_size(EP)
    rows_here, features = expert_input.shape
    slots = 2 * rows_here * TOP_K // experts // 4
    width = features // 4
    outgoing, target = dispatch(expert_input, expert_gain, routes, experts, slots, width)
    both = jnp.concatenate([gate_weight[0], up_weight[0]], axis=0)
    shares = gather_shares(both)
    down_shares = gather_shares(down_weight[0])
    received = swap(outgoing.reshape(experts, slots, width), EP)
    mixed = attention(mixer_input, mixer_gain, query_weight, key_weight, value_weight, sink_logit)
    rows = spread(received.reshape(experts * slots, width), ("Y", "X"))
    arrived = shares[3][:8] + shares[4][:8]
    inner = gated(rows, mixed, shares, arrived)
    hidden = swap(inner, ("Y", "X"))
    landed = down_shares[3][:8] + down_shares[4][:8]
    result, heads = lowered(hidden, down_shares, landed, slots)
    returned = swap(result.reshape(4 * experts, slots, -1), (*EP, "h", "p"))
    around = [[(i, i ^ k) for i in range(4)] for k in range(4)]
    size = mixed.shape[1]
    blocks = output_weight.reshape(2, 2, 2, 2, size, -1)
    columns = []
    for k in range(4):
        h, p = lax.axis_index("h") ^ (k // 2), lax.axis_index("p") ^ (k % 2)
        piece = lax.dynamic_slice_in_dim(blocks, h, 1, 1)
        piece = lax.dynamic_slice_in_dim(piece, p, 1, 3).reshape(4, size, -1)
        columns.append(lax.ppermute(piece, ("h", "p"), around[k]) if k else piece)
    own_sum, *sums = partial_sums(heads, columns)
    for k in range(1, 4):
        own_sum = own_sum + lax.ppermute(sums[k - 1], ("h", "p"), around[k])
    mixer_output = own_sum.astype(jnp.bfloat16)
    chances = selectors(target, route_logits.T, experts * 4 * slots)
    parts = dot(chances, returned.reshape(experts * 4 * slots, -1))
    parts = parts.reshape(3, rows_here, -1)
    expert_output = (parts[0] + (parts[1] + parts[2])).astype(jnp.bfloat16)
    return (mixer_output, expert_output)


def solution(mesh):
    names = ("ep_0", "ep_1", "Y", "h", "X", "p")
    finer = Mesh(mesh.devices.reshape(16, 2, 2, 2, 2, 2), names)
    in_specs = (
        P(EP, None),
        P(),
        P(None, TP),
        P(None, TP),
        P(None, TP),
        P(None, TP),
        P(TP),
        P(EP, None),
        P(),
        P(EP, None),
        P(EP, None),
        P(EP, None, TP),
        P(EP, None, TP),
        P(EP, None, TP),
    )
    out_specs = (P(EP, TP), P(EP, TP))
    return jax.shard_map(
        shards, mesh=finer, in_specs=in_specs, out_specs=out_specs, check_vma=False
    )
```

```python
import itertools

import jax
import jax.numpy as jnp
from jax import lax
from jax.experimental import pallas as pl
from jax.experimental.pallas import tpu as pltpu
from jax.sharding import Mesh
from jax.sharding import PartitionSpec as P

HEAD_DIM = 64
TOP_K = 4
WINDOW = 128
GRID_W = 64
EP = ("ep_0", "ep_1")
TP = ("h", "Y", "p", "X")

EPSILON = 1e-06
LIMIT = 7.0
SLOPE = 1.702
BASE = 10000.0


def swap(pieces, axis):
    return lax.all_to_all(pieces, axis, 0, 0, tiled=True)


def spread(shard, axis):
    return swap(jnp.broadcast_to(shard[None], (lax.axis_size(axis), *shard.shape)), axis)


def activate(gate, up):
    capped = jnp.minimum(gate, LIMIT)
    bounded = jnp.clip(up, -LIMIT, LIMIT)
    return (capped * jax.nn.sigmoid(SLOPE * capped) * (bounded + 1.0)).astype(jnp.bfloat16)


def dot(a, b):
    return jnp.dot(a, b, preferred_element_type=jnp.float32)


def tall(wide):
    k, n = wide.shape
    square = jnp.concatenate([wide, jnp.zeros((n - k, n), wide.dtype)], axis=0)
    return square.T


def dispatch(rows, gain, routes, weights, experts, slots, width):
    tokens = rows.shape[0]
    pairs = experts // 2
    tall_rows, columns = weights[0].shape

    def kernel(rows_ref, gain_ref, routes_ref, *refs):
        weight_refs, refs = refs[:3], refs[3:]
        out_ref, target_ref, stacked_ref, held_ref, here_ref, sems = refs
        rows_copy = pltpu.make_async_copy(rows_ref, here_ref, sems.at[6])
        rows_copy.start()
        arriving = [
            pltpu.make_async_copy(ref, held_ref.at[i], sems.at[i])
            for i, ref in enumerate(weight_refs)
        ]
        leaving = [
            pltpu.make_async_copy(
                held_ref.at[i], stacked_ref.at[pl.ds(i * tall_rows, tall_rows)], sems.at[3 + i]
            )
            for i in range(3)
        ]
        for copy in arriving:
            copy.start()
        block = 2 * lax.axis_index("Y") + lax.axis_index("X")
        rows_copy.wait()
        for come, go in zip(arriving, leaving):
            come.wait()
            go.start()
        values = here_ref[...].astype(jnp.float32)
        scale = lax.rsqrt(jnp.mean(values * values, axis=-1, keepdims=True) + EPSILON)
        start = pl.multiple_of(block * width, width)
        own = here_ref[:, pl.ds(start, width)].astype(jnp.float32)
        normed = (own * scale * gain_ref[:, pl.ds(start, width)]).astype(jnp.bfloat16)
        first = lax.broadcasted_iota(jnp.int32, (tokens, tokens), 0)
        second = lax.broadcasted_iota(jnp.int32, (tokens, tokens), 1)
        parity = lax.axis_index("p")
        expert = lax.broadcasted_iota(jnp.int32, (pairs, tokens), 0) * 2 + parity
        named = jnp.zeros((pairs, tokens), jnp.float32)
        for k in range(TOP_K):
            named = named + (routes_ref[k : k + 1, :] == expert).astype(jnp.float32)
        earlier = dot(named.astype(jnp.bfloat16), (first < second).astype(jnp.bfloat16))
        rank = jnp.where(named > 0.0, earlier.astype(jnp.int32), -1)
        rank = rank - lax.axis_index("h") * (2 * slots)
        slot = lax.broadcasted_iota(jnp.int32, (pairs, 2 * slots, tokens), 1)
        chosen = (rank[:, None, :] == slot).astype(jnp.float32)
        chosen = chosen.reshape(experts * slots, tokens).astype(jnp.bfloat16)
        out_ref[...] = dot(chosen, normed).astype(jnp.bfloat16)
        routed = tall(routes_ref[...].astype(jnp.float32))
        column = lax.broadcasted_iota(jnp.int32, (tokens, experts), 1)
        wanted = column.astype(jnp.float32)
        marks = [(routed[:, k : k + 1] == wanted).astype(jnp.float32) for k in range(TOP_K)]
        before = dot((second < first).astype(jnp.bfloat16), sum(marks).astype(jnp.bfloat16))
        before = before.astype(jnp.int32)
        core, half, spot = (before // slots) % 2, before // (2 * slots), before % slots
        position = (((column // 2) * 2 + core) * 2 + half) * 2 + column % 2
        position = (position * slots + spot).astype(jnp.float32)
        target_ref[...] = jnp.concatenate(
            [jnp.sum(mark * position, axis=1, keepdims=True) for mark in marks], axis=1
        ).astype(jnp.int32)
        for copy in leaving:
            copy.wait()

    vmem = pl.BlockSpec(memory_space=pltpu.VMEM)
    anywhere = pl.BlockSpec(memory_space=pl.ANY)
    return pl.pallas_call(
        kernel,
        out_shape=(
            jax.ShapeDtypeStruct((experts * slots, width), jnp.bfloat16),
            jax.ShapeDtypeStruct((tokens, TOP_K), jnp.int32),
            jax.ShapeDtypeStruct((3 * tall_rows, columns), jnp.bfloat16),
        ),
        in_specs=[anywhere] + [vmem] * 2 + [anywhere] * 3,
        out_specs=(vmem, vmem, anywhere),
        scratch_shapes=[
            pltpu.VMEM((3, tall_rows, columns), jnp.bfloat16),
            pltpu.VMEM(rows.shape, rows.dtype),
            pltpu.SemaphoreType.DMA((7,)),
        ],
        name="dispatch",
    )(rows, gain[None, :], routes.T, *weights)


def device_pairs(where):
    names = list(itertools.product(range(2), repeat=5))
    number = {name: i for i, name in enumerate(names)}
    return [(number[n], number[where(*n)]) for n in names if where(*n) is not None]


def gather_shares(own):
    axes = ("ep_1", "h", "Y", "p", "X")

    def outer(c, h, Y, p, X):
        return (c, 1 - h, Y, p, X) if c == p else (1 - c, h, Y, 1 - p, X)

    def cross(c, h, Y, p, X):
        return (1 - c, h, Y, p, X) if c == p else (c, 1 - h, Y, 1 - p, X)

    def trade(c, h, Y, p, X):
        return (1 - c, h, Y, p, X)

    def give(c, h, Y, p, X):
        return (1 - c, h, Y, p, X) if c == p else None

    first = lax.ppermute(own, axes, device_pairs(outer))
    second = lax.ppermute(own, axes, device_pairs(cross))
    third = lax.ppermute(first, axes, device_pairs(trade))
    fourth = lax.ppermute(second, axes, device_pairs(give))
    return own, first, second, third, fourth


def share_order():
    c, h, p = (lax.axis_index(a) for a in ("ep_1", "h", "p"))
    native = c == p
    own, up = 2 * h + p, 2 * (1 - h) + p
    side, across = 2 * h + (1 - p), 2 * (1 - h) + (1 - p)
    return native, [own, jnp.where(native, up, side), across, jnp.where(native, side, up)]


def copy_share(native, shares, index, start, size, target, sem):
    own, first, second, third, fourth = shares
    rows = pl.ds(start, size)
    if index in (1, 3):
        source = first if index == 1 else third
        pltpu.make_async_copy(source.at[rows], target, sem).start()
        return
    here, there = (own, second) if index == 0 else (second, fourth)

    @pl.when(native)
    def _():
        pltpu.make_async_copy(here.at[rows], target, sem).start()

    @pl.when(jnp.logical_not(native))
    def _():
        pltpu.make_async_copy(there.at[rows], target, sem).start()


def gated(rows, mixed, shares, arrived):
    parts, n, k = rows.shape
    u = shares[0].shape[1]
    j = mixed.shape[1]
    whole = parts * k

    def kernel(rows_ref, mixed_ref, _, *refs):
        shares, refs = refs[:5], refs[5:]
        out_ref, here_ref, weights_ref, hidden_ref, sems, row_sems, out_sems = refs
        native, order = share_order()
        arrivals = [
            pltpu.make_async_copy(rows_ref.at[part], here_ref.at[part], row_sems.at[part])
            for part in range(parts)
        ]
        arrivals.append(
            pltpu.make_async_copy(
                mixed_ref, hidden_ref.at[:, pl.ds(4 * u, j)], row_sems.at[parts]
            )
        )
        targets = [
            (weights_ref.at[i, :, pl.ds(side * u, u)], sems.at[i, side])
            for i in range(4)
            for side in range(2)
        ]
        for copy in arrivals:
            copy.start()
        for i in range(4):
            for side in range(2):
                copy_share(native, shares, i, side * whole, whole, *targets[2 * i + side])
        for copy in arrivals:
            copy.wait()
        for target in targets:
            pltpu.make_async_copy(shares[1].at[pl.ds(0, whole)], *target).wait()
        for i in range(4):
            total = dot(here_ref[0], weights_ref[i, :k, :])
            for part in range(1, parts):
                total = total + dot(here_ref[part], weights_ref[i, part * k : (part + 1) * k, :])
            lane = pl.multiple_of(order[i] * u, u)
            hidden_ref[:, pl.ds(lane, u)] = activate(total[:, :u], total[:, u:])
        leaving = [
            pltpu.make_async_copy(hidden_ref, out_ref.at[copy], out_sems.at[copy])
            for copy in range(parts)
        ]
        for copy in leaving:
            copy.start()
        for copy in leaving:
            copy.wait()

    anywhere = pl.BlockSpec(memory_space=pl.ANY)
    return pl.pallas_call(
        kernel,
        out_shape=jax.ShapeDtypeStruct((parts, n, 4 * u + j), jnp.bfloat16),
        in_specs=[anywhere] * 8,
        out_specs=anywhere,
        scratch_shapes=[
            pltpu.VMEM((parts, n, k), jnp.bfloat16),
            pltpu.VMEM((4, whole, 2 * u), jnp.bfloat16),
            pltpu.VMEM((n, 4 * u + j), jnp.bfloat16),
            pltpu.SemaphoreType.DMA((4, 2)),
            pltpu.SemaphoreType.DMA((parts + 1,)),
            pltpu.SemaphoreType.DMA((parts,)),
        ],
        name="gated",
    )(rows, mixed, arrived, *shares)


def lowered(hidden, shares, slots):
    parts, n, wide = hidden.shape
    f = shares[0].shape[1]
    k = 4 * f
    j = wide - k
    whole = parts * k
    half = k // 2

    def kernel(hidden_ref, *refs):
        shares, refs = refs[:5], refs[5:]
        out_ref, heads_ref, here_ref, weights_ref, sems, row_sems = refs
        native, order = share_order()
        targets = [
            (weights_ref.at[i // 2, :, pl.ds((i % 2) * f, f)], sems.at[i]) for i in range(4)
        ]
        arrivals = [
            pltpu.make_async_copy(hidden_ref.at[part], here_ref.at[part], row_sems.at[part])
            for part in range(parts)
        ]
        heads = pltpu.make_async_copy(
            here_ref.at[:, :, pl.ds(k, j)], heads_ref, row_sems.at[parts]
        )
        for copy in arrivals:
            copy.start()
        for i in range(4):
            copy_share(native, shares, i, 2 * whole, whole, *targets[i])
        for copy in arrivals:
            copy.wait()
        heads.start()
        for target in targets:
            pltpu.make_async_copy(shares[1].at[pl.ds(0, whole)], *target).wait()
        for pair in range(2):
            total = jnp.zeros((n, 2 * f), jnp.float32)
            for Y, X, h in itertools.product(range(2), repeat=3):
                units = [(8 * h + 4 * Y + 2 * p + X) * f for p in range(2)]
                below = [weights_ref[pair, unit : unit + f, :] for unit in units]
                piece = here_ref[2 * Y + X, :, h * half : (h + 1) * half]
                total = total + dot(piece, jnp.concatenate(below, axis=0))
            rounded = total.astype(jnp.bfloat16).reshape(n // slots, slots, 2 * f)
            out_ref[:, order[2 * pair]] = rounded[:, :, :f]
            out_ref[:, order[2 * pair + 1]] = rounded[:, :, f:]
        heads.wait()

    vmem = pl.BlockSpec(memory_space=pltpu.VMEM)
    anywhere = pl.BlockSpec(memory_space=pl.ANY)
    return pl.pallas_call(
        kernel,
        out_shape=(
            jax.ShapeDtypeStruct((n // slots, 4, slots, f), jnp.bfloat16),
            jax.ShapeDtypeStruct((parts, n, j), jnp.bfloat16),
        ),
        in_specs=[anywhere] * 6,
        out_specs=(vmem, anywhere),
        scratch_shapes=[
            pltpu.VMEM((parts, n, wide), jnp.bfloat16),
            pltpu.VMEM((2, whole, 2 * f), jnp.bfloat16),
            pltpu.SemaphoreType.DMA((4,)),
            pltpu.SemaphoreType.DMA((parts + 1,)),
        ],
        name="lowered",
    )(hidden, *shares)


def selectors(target, logits, slots):
    tokens = target.shape[0]

    def kernel(target_ref, logits_ref, out_ref):
        chances = tall(jax.nn.softmax(logits_ref[...], axis=0))
        lane = lax.broadcasted_iota(jnp.int32, (tokens, slots), 1)
        rest = jnp.zeros((tokens, slots), jnp.float32)
        for k in range(TOP_K):
            rest = jnp.where(target_ref[:, k : k + 1] == lane, chances[:, k : k + 1], rest)
        for part in range(3):
            rounded = rest.astype(jnp.bfloat16)
            out_ref[part * tokens : (part + 1) * tokens, :] = rounded
            rest = rest - rounded.astype(jnp.float32)

    vmem = pl.BlockSpec(memory_space=pltpu.VMEM)
    return pl.pallas_call(
        kernel,
        out_shape=jax.ShapeDtypeStruct((3 * tokens, slots), jnp.bfloat16),
        in_specs=[vmem] * 2,
        out_specs=vmem,
        name="selectors",
    )(target, logits)


def rotary_tables(first, rows, width):
    quarter = HEAD_DIM // 4
    lane = jnp.arange(width, dtype=jnp.int32)
    frequency = BASE ** (-(lane % quarter).astype(jnp.float32) / quarter)
    at = jnp.arange(GRID_W + rows, dtype=jnp.int32)
    place = jnp.where(at < GRID_W, at, at - GRID_W + first)
    angle = place.astype(jnp.float32)[:, None] * frequency
    sign = jnp.where(lane % (2 * quarter) < quarter, -1.0, 1.0)
    return jnp.cos(angle), jnp.sin(angle) * sign


def projections(rows, gain, query_weight, key_weight, value_weight):
    tokens, _ = rows.shape
    width = query_weight.shape[1]
    half = width // 2
    quarter = HEAD_DIM // 4
    spans = tokens // GRID_W
    cosine, sine = rotary_tables(lax.axis_index(EP) * spans, spans, width)

    def kernel(
        rows_ref, gain_ref, query_ref, key_ref, value_ref, cos_ref, sin_ref, out_ref, *pair_refs
    ):
        values = rows_ref[...].astype(jnp.float32)
        scale = lax.rsqrt(jnp.mean(values * values, axis=-1, keepdims=True) + EPSILON)
        normed = (values * scale * gain_ref[...]).astype(jnp.bfloat16)
        lane = lax.broadcasted_iota(jnp.int32, (tokens, width), 1)
        near = lane % (2 * quarter) < quarter
        by_row = lax.broadcasted_iota(jnp.int32, (GRID_W, width), 1) % HEAD_DIM < HEAD_DIM // 2

        def table(ref):
            columns = ref[:GRID_W, :]
            parts = [
                jnp.where(by_row, ref[GRID_W + i : GRID_W + i + 1, :], columns)
                for i in range(spans)
            ]
            return jnp.concatenate(parts, axis=0)

        cos, sin = table(cos_ref), table(sin_ref)

        def turned(a):
            partner = jnp.where(
                near, pltpu.roll(a, width - quarter, 1), pltpu.roll(a, quarter, 1)
            )
            return (a * cos + partner * sin).astype(jnp.bfloat16)

        def flipped(weight_ref):
            return lax.dot_general(
                normed, weight_ref[...], (((1,), (1,)), ((), ())), preferred_element_type=jnp.float32
            )

        out_ref[...] = turned(dot(normed, query_ref[...]))
        keys, mine = flipped(key_ref), flipped(value_ref)
        both = jnp.concatenate([keys, mine], axis=1)
        rounded = jnp.where(lane < half, turned(both), both.astype(jnp.bfloat16))
        for i, ref in enumerate(pair_refs):
            ref[...] = rounded[i * WINDOW : (i + 1) * WINDOW]

    vmem = pl.BlockSpec(memory_space=pltpu.VMEM)
    return pl.pallas_call(
        kernel,
        out_shape=[jax.ShapeDtypeStruct((tokens, width), jnp.bfloat16)]
        + [jax.ShapeDtypeStruct((WINDOW, width), jnp.bfloat16)] * (tokens // WINDOW),
        in_specs=[vmem] * 7,
        out_specs=[vmem] * (1 + tokens // WINDOW),
        name="projections",
    )(rows, gain[None, :], query_weight, key_weight.T, value_weight.T, cosine, sine)


def banded(query, pieces, sinks):
    tokens, width = query.shape
    blocks = tokens // WINDOW
    heads = width // HEAD_DIM

    def kernel(sink_ref, query_ref, *refs):
        piece_refs, out_ref = refs[:-1], refs[-1]
        place, last = lax.axis_index(EP), lax.axis_size(EP) - 1
        row = lax.broadcasted_iota(jnp.int32, (WINDOW, 3 * WINDOW), 0)
        column = lax.broadcasted_iota(jnp.int32, (WINDOW, 3 * WINDOW), 1)
        band = (column >= row) & (column <= row + 2 * WINDOW)
        for n in range(blocks):
            near = jnp.concatenate([piece_refs[n + i][...] for i in range(3)], axis=0)
            keys, values = near[:, :HEAD_DIM], near[:, HEAD_DIM:]
            least = jnp.where(place == 0, WINDOW, 0) if n == 0 else 0
            most = jnp.where(place == last, 2 * WINDOW, 3 * WINDOW) if n == blocks - 1 else 3 * WINDOW
            allowed = band & (column >= least) & (column < most)
            outs = []
            for r in range(heads):
                here = query_ref[n * WINDOW : (n + 1) * WINDOW, r * HEAD_DIM : (r + 1) * HEAD_DIM]
                scores = lax.dot_general(
                    here, keys, (((1,), (1,)), ((), ())), preferred_element_type=jnp.float32
                )
                scores = jnp.where(allowed, scores * HEAD_DIM ** (-0.5), -1e30)
                sink = sink_ref[r]
                top = jnp.maximum(jnp.max(scores, axis=-1, keepdims=True), sink)
                weights = jnp.exp(scores - top)
                total = jnp.sum(weights, axis=-1, keepdims=True) + jnp.exp(sink - top)
                outs.append(dot((weights / total).astype(jnp.bfloat16), values))
            mixed = jnp.concatenate(outs, axis=1).astype(jnp.bfloat16)
            out_ref[n * WINDOW : (n + 1) * WINDOW, :] = mixed

    vmem = pl.BlockSpec(memory_space=pltpu.VMEM)
    return pl.pallas_call(
        kernel,
        out_shape=jax.ShapeDtypeStruct((tokens, width), jnp.bfloat16),
        in_specs=[pl.BlockSpec(memory_space=pltpu.SMEM)] + [vmem] * (blocks + 3),
        out_specs=vmem,
        name="banded",
    )(sinks, query, *pieces)


def attention(mixer_input, mixer_gain, query_weight, key_weight, value_weight, sink_logit):
    query, *pieces = projections(mixer_input, mixer_gain, query_weight, key_weight, value_weight)
    up = [(i, i + 1) for i in range(lax.axis_size(EP) - 1)]
    before = lax.ppermute(pieces[-1], EP, up)
    after = lax.ppermute(pieces[0], EP, [(j, i) for i, j in up])
    return banded(query, [before, *pieces, after], sink_logit)


def partial_sums(heads, columns):
    parts, n, _ = heads.shape
    f = columns[0].shape[2]

    def kernel(heads_ref, *refs):
        columns_refs, out_refs = refs[:4], refs[4:]
        for columns_ref, out_ref in zip(columns_refs, out_refs):
            total = dot(heads_ref[0], columns_ref[0])
            for part in range(1, parts):
                total = total + dot(heads_ref[part], columns_ref[part])
            out_ref[...] = total

    vmem = pl.BlockSpec(memory_space=pltpu.VMEM)
    return pl.pallas_call(
        kernel,
        out_shape=[jax.ShapeDtypeStruct((n, f), jnp.float32)] * 4,
        in_specs=[vmem] * 5,
        out_specs=[vmem] * 4,
        name="partial_sums",
    )(heads, *columns)


def shards(
    mixer_input,
    mixer_gain,
    query_weight,
    key_weight,
    value_weight,
    output_weight,
    sink_logit,
    expert_input,
    expert_gain,
    routes,
    route_logits,
    gate_weight,
    up_weight,
    down_weight,
):
    experts = lax.axis_size(EP)
    rows_here, features = expert_input.shape
    slots = 2 * rows_here * TOP_K // experts // 4
    width = features // 4
    weights = (gate_weight[0], up_weight[0], down_weight[0])
    outgoing, target, own = dispatch(
        expert_input, expert_gain, routes, weights, experts, slots, width
    )
    shares = gather_shares(own)
    received = swap(outgoing.reshape(experts, slots, width), EP)
    mixed = attention(mixer_input, mixer_gain, query_weight, key_weight, value_weight, sink_logit)
    rows = spread(received.reshape(experts * slots, width), ("Y", "X"))
    arrived = shares[3][:8] + shares[4][:8]
    inner = gated(rows, mixed, shares, arrived)
    hidden = swap(inner, ("Y", "X"))
    result, heads = lowered(hidden, shares, slots)
    returned = swap(result.reshape(4 * experts, slots, -1), (*EP, "h", "p"))
    around = [[(i, i ^ k) for i in range(4)] for k in range(4)]
    size = mixed.shape[1]
    blocks = output_weight.reshape(2, 2, 2, 2, size, -1)
    columns = []
    for k in range(4):
        h, p = lax.axis_index("h") ^ (k // 2), lax.axis_index("p") ^ (k % 2)
        piece = lax.dynamic_slice_in_dim(blocks, h, 1, 0)
        piece = lax.dynamic_slice_in_dim(piece, p, 1, 2).reshape(4, size, -1)
        columns.append(lax.ppermute(piece, ("h", "p"), around[k]) if k else piece)
    own_sum, *sums = partial_sums(heads, columns)
    for k in range(1, 4):
        own_sum = own_sum + lax.ppermute(sums[k - 1], ("h", "p"), around[k])
    mixer_output = own_sum.astype(jnp.bfloat16)
    chances = selectors(target, route_logits.T, experts * 4 * slots)
    parts = dot(chances, returned.reshape(experts * 4 * slots, -1))
    parts = parts.reshape(3, rows_here, -1)
    expert_output = (parts[0] + (parts[1] + parts[2])).astype(jnp.bfloat16)
    return (mixer_output, expert_output)


def solution(mesh):
    names = ("ep_0", "ep_1", "h", "Y", "p", "X")
    finer = Mesh(mesh.devices.reshape(16, 2, 2, 2, 2, 2), names)
    in_specs = (
        P(EP, None),
        P(),
        P(None, TP),
        P(None, TP),
        P(None, TP),
        P(None, TP),
        P(TP),
        P(EP, None),
        P(),
        P(EP, None),
        P(EP, None),
        P(EP, None, TP),
        P(EP, None, TP),
        P(EP, None, TP),
    )
    out_specs = (P(EP, TP), P(EP, TP))
    return jax.shard_map(
        shards, mesh=finer, in_specs=in_specs, out_specs=out_specs, check_vma=False
    )
```

```python
import itertools

import jax
import jax.numpy as jnp
from jax import lax
from jax.experimental import pallas as pl
from jax.experimental.pallas import tpu as pltpu
from jax.sharding import Mesh
from jax.sharding import PartitionSpec as P

HEAD_DIM = 64
TOP_K = 4
WINDOW = 128
GRID_W = 64
EP = ("ep_0", "ep_1")
TP = ("Y", "h", "X", "p")

EPSILON = 1e-06
LIMIT = 7.0
SLOPE = 1.702
BASE = 10000.0


def swap(pieces, axis):
    return lax.all_to_all(pieces, axis, 0, 0, tiled=True)


def spread(shard, axis):
    return swap(jnp.broadcast_to(shard[None], (lax.axis_size(axis), *shard.shape)), axis)


def activate(gate, up):
    capped = jnp.minimum(gate, LIMIT)
    bounded = jnp.clip(up, -LIMIT, LIMIT)
    return (capped * jax.nn.sigmoid(SLOPE * capped) * (bounded + 1.0)).astype(jnp.bfloat16)


def dot(a, b):
    return jnp.dot(a, b, preferred_element_type=jnp.float32)


def tall(wide):
    k, n = wide.shape
    square = jnp.concatenate([wide, jnp.zeros((n - k, n), wide.dtype)], axis=0)
    return square.T


def dispatch(rows, gain, routes, weights, experts, slots, width):
    tokens = rows.shape[0]
    pairs = experts // 2
    tall_rows, columns = weights[0].shape

    def kernel(rows_ref, gain_ref, routes_ref, *refs):
        weight_refs, refs = refs[:3], refs[3:]
        out_ref, target_ref, stacked_ref, held_ref, here_ref, sems = refs
        rows_copy = pltpu.make_async_copy(rows_ref, here_ref, sems.at[6])
        rows_copy.start()
        arriving = [
            pltpu.make_async_copy(ref, held_ref.at[i], sems.at[i])
            for i, ref in enumerate(weight_refs)
        ]
        leaving = [
            pltpu.make_async_copy(
                held_ref.at[i], stacked_ref.at[pl.ds(i * tall_rows, tall_rows)], sems.at[3 + i]
            )
            for i in range(3)
        ]
        for copy in arriving:
            copy.start()
        block = 2 * lax.axis_index("Y") + lax.axis_index("X")
        rows_copy.wait()
        for come, go in zip(arriving, leaving):
            come.wait()
            go.start()
        values = here_ref[...].astype(jnp.float32)
        scale = lax.rsqrt(jnp.mean(values * values, axis=-1, keepdims=True) + EPSILON)
        start = pl.multiple_of(block * width, width)
        own = here_ref[:, pl.ds(start, width)].astype(jnp.float32)
        normed = (own * scale * gain_ref[:, pl.ds(start, width)]).astype(jnp.bfloat16)
        first = lax.broadcasted_iota(jnp.int32, (tokens, tokens), 0)
        second = lax.broadcasted_iota(jnp.int32, (tokens, tokens), 1)
        parity = lax.axis_index("p")
        expert = lax.broadcasted_iota(jnp.int32, (pairs, tokens), 0) * 2 + parity
        named = jnp.zeros((pairs, tokens), jnp.float32)
        for k in range(TOP_K):
            named = named + (routes_ref[k : k + 1, :] == expert).astype(jnp.float32)
        earlier = dot(named.astype(jnp.bfloat16), (first < second).astype(jnp.bfloat16))
        rank = jnp.where(named > 0.0, earlier.astype(jnp.int32), -1)
        rank = rank - lax.axis_index("h") * (2 * slots)
        slot = lax.broadcasted_iota(jnp.int32, (pairs, 2 * slots, tokens), 1)
        chosen = (rank[:, None, :] == slot).astype(jnp.float32)
        chosen = chosen.reshape(experts * slots, tokens).astype(jnp.bfloat16)
        out_ref[...] = dot(chosen, normed).astype(jnp.bfloat16)
        routed = tall(routes_ref[...].astype(jnp.float32))
        column = lax.broadcasted_iota(jnp.int32, (tokens, experts), 1)
        wanted = column.astype(jnp.float32)
        marks = [(routed[:, k : k + 1] == wanted).astype(jnp.float32) for k in range(TOP_K)]
        before = dot((second < first).astype(jnp.bfloat16), sum(marks).astype(jnp.bfloat16))
        before = before.astype(jnp.int32)
        core, half, spot = (before // slots) % 2, before // (2 * slots), before % slots
        position = (((column // 2) * 2 + core) * 2 + half) * 2 + column % 2
        position = (position * slots + spot).astype(jnp.float32)
        target_ref[...] = jnp.concatenate(
            [jnp.sum(mark * position, axis=1, keepdims=True) for mark in marks], axis=1
        ).astype(jnp.int32)
        for copy in leaving:
            copy.wait()

    vmem = pl.BlockSpec(memory_space=pltpu.VMEM)
    anywhere = pl.BlockSpec(memory_space=pl.ANY)
    return pl.pallas_call(
        kernel,
        out_shape=(
            jax.ShapeDtypeStruct((experts * slots, width), jnp.bfloat16),
            jax.ShapeDtypeStruct((tokens, TOP_K), jnp.int32),
            jax.ShapeDtypeStruct((3 * tall_rows, columns), jnp.bfloat16),
        ),
        in_specs=[anywhere] + [vmem] * 2 + [anywhere] * 3,
        out_specs=(vmem, vmem, anywhere),
        scratch_shapes=[
            pltpu.VMEM((3, tall_rows, columns), jnp.bfloat16),
            pltpu.VMEM(rows.shape, rows.dtype),
            pltpu.SemaphoreType.DMA((7,)),
        ],
        name="dispatch",
    )(rows, gain[None, :], routes.T, *weights)


def device_pairs(where):
    names = list(itertools.product(range(2), repeat=5))
    number = {name: i for i, name in enumerate(names)}
    return [(number[n], number[where(*n)]) for n in names if where(*n) is not None]


def gather_shares(own):
    axes = ("ep_1", "Y", "h", "X", "p")

    def outer(c, Y, h, X, p):
        return (c, Y, 1 - h, X, p) if c == p else (1 - c, Y, h, X, 1 - p)

    def cross(c, Y, h, X, p):
        return (1 - c, Y, h, X, p) if c == p else (c, Y, 1 - h, X, 1 - p)

    def trade(c, Y, h, X, p):
        return (1 - c, Y, h, X, p)

    def give(c, Y, h, X, p):
        return (1 - c, Y, h, X, p) if c == p else None

    first = lax.ppermute(own, axes, device_pairs(outer))
    second = lax.ppermute(own, axes, device_pairs(cross))
    third = lax.ppermute(first, axes, device_pairs(trade))
    fourth = lax.ppermute(second, axes, device_pairs(give))
    return own, first, second, third, fourth


def share_order():
    c, h, p = (lax.axis_index(a) for a in ("ep_1", "h", "p"))
    native = c == p
    own, up = 2 * h + p, 2 * (1 - h) + p
    side, across = 2 * h + (1 - p), 2 * (1 - h) + (1 - p)
    return native, [own, jnp.where(native, up, side), across, jnp.where(native, side, up)]


def copy_share(native, shares, index, start, size, target, sem):
    own, first, second, third, fourth = shares
    rows = pl.ds(start, size)
    if index in (1, 3):
        source = first if index == 1 else third
        pltpu.make_async_copy(source.at[rows], target, sem).start()
        return
    here, there = (own, second) if index == 0 else (second, fourth)

    @pl.when(native)
    def _():
        pltpu.make_async_copy(here.at[rows], target, sem).start()

    @pl.when(jnp.logical_not(native))
    def _():
        pltpu.make_async_copy(there.at[rows], target, sem).start()


def gated(rows, mixed, shares, arrived):
    parts, n, k = rows.shape
    u = shares[0].shape[1]
    j = mixed.shape[1]
    whole = parts * k

    def kernel(rows_ref, mixed_ref, _, *refs):
        shares, refs = refs[:5], refs[5:]
        out_ref, here_ref, weights_ref, hidden_ref, sems, row_sems, out_sems = refs
        native, order = share_order()
        arrivals = [
            pltpu.make_async_copy(rows_ref.at[part], here_ref.at[part], row_sems.at[part])
            for part in range(parts)
        ]
        arrivals.append(
            pltpu.make_async_copy(
                mixed_ref, hidden_ref.at[:, pl.ds(4 * u, j)], row_sems.at[parts]
            )
        )
        targets = [
            (weights_ref.at[i, :, pl.ds(side * u, u)], sems.at[i, side])
            for i in range(4)
            for side in range(2)
        ]
        for copy in arrivals:
            copy.start()
        for i in range(4):
            for side in range(2):
                copy_share(native, shares, i, side * whole, whole, *targets[2 * i + side])
        for copy in arrivals:
            copy.wait()
        for target in targets:
            pltpu.make_async_copy(shares[1].at[pl.ds(0, whole)], *target).wait()
        for i in range(4):
            total = dot(here_ref[0], weights_ref[i, :k, :])
            for part in range(1, parts):
                total = total + dot(here_ref[part], weights_ref[i, part * k : (part + 1) * k, :])
            lane = pl.multiple_of(order[i] * u, u)
            hidden_ref[:, pl.ds(lane, u)] = activate(total[:, :u], total[:, u:])
        leaving = [
            pltpu.make_async_copy(hidden_ref, out_ref.at[copy], out_sems.at[copy])
            for copy in range(parts)
        ]
        for copy in leaving:
            copy.start()
        for copy in leaving:
            copy.wait()

    anywhere = pl.BlockSpec(memory_space=pl.ANY)
    return pl.pallas_call(
        kernel,
        out_shape=jax.ShapeDtypeStruct((parts, n, 4 * u + j), jnp.bfloat16),
        in_specs=[anywhere] * 8,
        out_specs=anywhere,
        scratch_shapes=[
            pltpu.VMEM((parts, n, k), jnp.bfloat16),
            pltpu.VMEM((4, whole, 2 * u), jnp.bfloat16),
            pltpu.VMEM((n, 4 * u + j), jnp.bfloat16),
            pltpu.SemaphoreType.DMA((4, 2)),
            pltpu.SemaphoreType.DMA((parts + 1,)),
            pltpu.SemaphoreType.DMA((parts,)),
        ],
        name="gated",
    )(rows, mixed, arrived, *shares)


def ordered(shares, parts):
    f = shares[0].shape[1]
    k = 4 * f
    whole = parts * k
    half = k // 2
    places = list(itertools.product(range(2), repeat=3))

    def kernel(*refs):
        shares, (out_ref, sems) = refs[:5], refs[5:]
        native, order = share_order()
        for i in range(4):
            lane = pl.multiple_of(order[i] * f, f)
            for n, (Y, X, h) in enumerate(places):
                start = 2 * whole + (8 * Y + 4 * h + 2 * X) * f
                target = out_ref.at[2 * Y + X, pl.ds(h * half, half), pl.ds(lane, f)]
                copy_share(native, shares, i, start, half, target, sems.at[i, n])
        for i in range(4):
            for n in range(len(places)):
                target = out_ref.at[0, pl.ds(0, half), pl.ds(0, f)]
                source = shares[1].at[pl.ds(0, half)]
                pltpu.make_async_copy(source, target, sems.at[i, n]).wait()

    anywhere = pl.BlockSpec(memory_space=pl.ANY)
    return pl.pallas_call(
        kernel,
        out_shape=jax.ShapeDtypeStruct((parts, k, 4 * f), jnp.bfloat16),
        in_specs=[anywhere] * 5,
        out_specs=pl.BlockSpec(memory_space=pltpu.VMEM),
        scratch_shapes=[pltpu.SemaphoreType.DMA((4, len(places)))],
        name="ordered",
    )(*shares)


def selectors(target, logits, slots):
    tokens = target.shape[0]

    def kernel(target_ref, logits_ref, out_ref):
        chances = tall(jax.nn.softmax(logits_ref[...], axis=0))
        lane = lax.broadcasted_iota(jnp.int32, (tokens, slots), 1)
        rest = jnp.zeros((tokens, slots), jnp.float32)
        for k in range(TOP_K):
            rest = jnp.where(target_ref[:, k : k + 1] == lane, chances[:, k : k + 1], rest)
        for part in range(3):
            rounded = rest.astype(jnp.bfloat16)
            out_ref[part * tokens : (part + 1) * tokens, :] = rounded
            rest = rest - rounded.astype(jnp.float32)

    vmem = pl.BlockSpec(memory_space=pltpu.VMEM)
    return pl.pallas_call(
        kernel,
        out_shape=jax.ShapeDtypeStruct((3 * tokens, slots), jnp.bfloat16),
        in_specs=[vmem] * 2,
        out_specs=vmem,
        name="selectors",
    )(target, logits)


def rotary_tables(first, rows, width):
    quarter = HEAD_DIM // 4
    lane = jnp.arange(width, dtype=jnp.int32)
    frequency = BASE ** (-(lane % quarter).astype(jnp.float32) / quarter)
    at = jnp.arange(GRID_W + rows, dtype=jnp.int32)
    place = jnp.where(at < GRID_W, at, at - GRID_W + first)
    angle = place.astype(jnp.float32)[:, None] * frequency
    sign = jnp.where(lane % (2 * quarter) < quarter, -1.0, 1.0)
    return jnp.cos(angle), jnp.sin(angle) * sign


def projections(rows, gain, query_weight, key_weight, value_weight):
    tokens, _ = rows.shape
    width = query_weight.shape[1]
    half = width // 2
    quarter = HEAD_DIM // 4
    spans = tokens // GRID_W
    cosine, sine = rotary_tables(lax.axis_index(EP) * spans, spans, width)

    def kernel(
        rows_ref, gain_ref, query_ref, key_ref, value_ref, cos_ref, sin_ref, out_ref, *pair_refs
    ):
        values = rows_ref[...].astype(jnp.float32)
        scale = lax.rsqrt(jnp.mean(values * values, axis=-1, keepdims=True) + EPSILON)
        normed = (values * scale * gain_ref[...]).astype(jnp.bfloat16)
        lane = lax.broadcasted_iota(jnp.int32, (tokens, width), 1)
        near = lane % (2 * quarter) < quarter
        by_row = lax.broadcasted_iota(jnp.int32, (GRID_W, width), 1) % HEAD_DIM < HEAD_DIM // 2

        def table(ref):
            columns = ref[:GRID_W, :]
            parts = [
                jnp.where(by_row, ref[GRID_W + i : GRID_W + i + 1, :], columns)
                for i in range(spans)
            ]
            return jnp.concatenate(parts, axis=0)

        cos, sin = table(cos_ref), table(sin_ref)

        def turned(a):
            partner = jnp.where(
                near, pltpu.roll(a, width - quarter, 1), pltpu.roll(a, quarter, 1)
            )
            return (a * cos + partner * sin).astype(jnp.bfloat16)

        def flipped(weight_ref):
            return lax.dot_general(
                normed, weight_ref[...], (((1,), (1,)), ((), ())), preferred_element_type=jnp.float32
            )

        out_ref[...] = turned(dot(normed, query_ref[...]))
        keys, mine = flipped(key_ref), flipped(value_ref)
        both = jnp.concatenate([keys, mine], axis=1)
        rounded = jnp.where(lane < half, turned(both), both.astype(jnp.bfloat16))
        for i, ref in enumerate(pair_refs):
            ref[...] = rounded[i * WINDOW : (i + 1) * WINDOW]

    vmem = pl.BlockSpec(memory_space=pltpu.VMEM)
    return pl.pallas_call(
        kernel,
        out_shape=[jax.ShapeDtypeStruct((tokens, width), jnp.bfloat16)]
        + [jax.ShapeDtypeStruct((WINDOW, width), jnp.bfloat16)] * (tokens // WINDOW),
        in_specs=[vmem] * 7,
        out_specs=[vmem] * (1 + tokens // WINDOW),
        name="projections",
    )(rows, gain[None, :], query_weight, key_weight.T, value_weight.T, cosine, sine)


def banded(query, pieces, sinks):
    tokens, width = query.shape
    blocks = tokens // WINDOW
    heads = width // HEAD_DIM

    def kernel(sink_ref, query_ref, *refs):
        piece_refs, out_ref = refs[:-1], refs[-1]
        place, last = lax.axis_index(EP), lax.axis_size(EP) - 1
        row = lax.broadcasted_iota(jnp.int32, (WINDOW, 3 * WINDOW), 0)
        column = lax.broadcasted_iota(jnp.int32, (WINDOW, 3 * WINDOW), 1)
        band = (column >= row) & (column <= row + 2 * WINDOW)
        for n in range(blocks):
            near = jnp.concatenate([piece_refs[n + i][...] for i in range(3)], axis=0)
            keys, values = near[:, :HEAD_DIM], near[:, HEAD_DIM:]
            least = jnp.where(place == 0, WINDOW, 0) if n == 0 else 0
            most = jnp.where(place == last, 2 * WINDOW, 3 * WINDOW) if n == blocks - 1 else 3 * WINDOW
            allowed = band & (column >= least) & (column < most)
            outs = []
            for r in range(heads):
                here = query_ref[n * WINDOW : (n + 1) * WINDOW, r * HEAD_DIM : (r + 1) * HEAD_DIM]
                scores = lax.dot_general(
                    here, keys, (((1,), (1,)), ((), ())), preferred_element_type=jnp.float32
                )
                scores = jnp.where(allowed, scores * HEAD_DIM ** (-0.5), -1e30)
                sink = sink_ref[r]
                top = jnp.maximum(jnp.max(scores, axis=-1, keepdims=True), sink)
                weights = jnp.exp(scores - top)
                total = jnp.sum(weights, axis=-1, keepdims=True) + jnp.exp(sink - top)
                outs.append(dot((weights / total).astype(jnp.bfloat16), values))
            mixed = jnp.concatenate(outs, axis=1).astype(jnp.bfloat16)
            out_ref[n * WINDOW : (n + 1) * WINDOW, :] = mixed

    vmem = pl.BlockSpec(memory_space=pltpu.VMEM)
    return pl.pallas_call(
        kernel,
        out_shape=jax.ShapeDtypeStruct((tokens, width), jnp.bfloat16),
        in_specs=[pl.BlockSpec(memory_space=pltpu.SMEM)] + [vmem] * (blocks + 3),
        out_specs=vmem,
        name="banded",
    )(sinks, query, *pieces)


def attention(mixer_input, mixer_gain, query_weight, key_weight, value_weight, sink_logit):
    query, *pieces = projections(mixer_input, mixer_gain, query_weight, key_weight, value_weight)
    up = [(i, i + 1) for i in range(lax.axis_size(EP) - 1)]
    before = lax.ppermute(pieces[-1], EP, up)
    after = lax.ppermute(pieces[0], EP, [(j, i) for i, j in up])
    return banded(query, [before, *pieces, after], sink_logit)


def partial_sums(heads, columns):
    parts, n, _ = heads.shape
    f = columns[0].shape[2]

    def kernel(heads_ref, *refs):
        columns_refs, out_refs = refs[:4], refs[4:]
        for columns_ref, out_ref in zip(columns_refs, out_refs):
            total = dot(heads_ref[0], columns_ref[0])
            for part in range(1, parts):
                total = total + dot(heads_ref[part], columns_ref[part])
            out_ref[...] = total

    vmem = pl.BlockSpec(memory_space=pltpu.VMEM)
    return pl.pallas_call(
        kernel,
        out_shape=[jax.ShapeDtypeStruct((n, f), jnp.float32)] * 4,
        in_specs=[vmem] * 5,
        out_specs=[vmem] * 4,
        name="partial_sums",
    )(heads, *columns)


def shards(
    mixer_input,
    mixer_gain,
    query_weight,
    key_weight,
    value_weight,
    output_weight,
    sink_logit,
    expert_input,
    expert_gain,
    routes,
    route_logits,
    gate_weight,
    up_weight,
    down_weight,
):
    experts = lax.axis_size(EP)
    rows_here, features = expert_input.shape
    slots = 2 * rows_here * TOP_K // experts // 4
    width = features // 4
    weights = (gate_weight[0], up_weight[0], down_weight[0])
    outgoing, target, own = dispatch(
        expert_input, expert_gain, routes, weights, experts, slots, width
    )
    shares = gather_shares(own)
    received = swap(outgoing.reshape(experts, slots, width), EP)
    mixed = attention(mixer_input, mixer_gain, query_weight, key_weight, value_weight, sink_logit)
    rows = spread(received.reshape(experts * slots, width), ("Y", "X"))
    arrived = shares[3][:8] + shares[4][:8]
    inner = gated(rows, mixed, shares, arrived)
    hidden = swap(inner, ("Y", "X"))
    down = ordered(shares, 4)
    result = jnp.einsum(
        "qrl,qlf->rf", hidden[:, :, :width], down, preferred_element_type=jnp.float32
    ).astype(jnp.bfloat16)
    result = result.reshape(experts, slots, 4, -1).transpose(0, 2, 1, 3)
    heads = hidden[:, :, width:]
    returned = swap(result.reshape(4 * experts, slots, -1), (*EP, "h", "p"))
    around = [[(i, i ^ k) for i in range(4)] for k in range(4)]
    size = mixed.shape[1]
    blocks = output_weight.reshape(2, 2, 2, 2, size, -1)
    columns = []
    for k in range(4):
        h, p = lax.axis_index("h") ^ (k // 2), lax.axis_index("p") ^ (k % 2)
        piece = lax.dynamic_slice_in_dim(blocks, h, 1, 1)
        piece = lax.dynamic_slice_in_dim(piece, p, 1, 3).reshape(4, size, -1)
        columns.append(lax.ppermute(piece, ("h", "p"), around[k]) if k else piece)
    own_sum, *sums = partial_sums(heads, columns)
    for k in range(1, 4):
        own_sum = own_sum + lax.ppermute(sums[k - 1], ("h", "p"), around[k])
    mixer_output = own_sum.astype(jnp.bfloat16)
    chances = selectors(target, route_logits.T, experts * 4 * slots)
    parts = dot(chances, returned.reshape(experts * 4 * slots, -1))
    parts = parts.reshape(3, rows_here, -1)
    expert_output = (parts[0] + (parts[1] + parts[2])).astype(jnp.bfloat16)
    return (mixer_output, expert_output)


def solution(mesh):
    names = ("ep_0", "ep_1", "Y", "h", "X", "p")
    finer = Mesh(mesh.devices.reshape(16, 2, 2, 2, 2, 2), names)
    in_specs = (
        P(EP, None),
        P(),
        P(None, TP),
        P(None, TP),
        P(None, TP),
        P(None, TP),
        P(TP),
        P(EP, None),
        P(),
        P(EP, None),
        P(EP, None),
        P(EP, None, TP),
        P(EP, None, TP),
        P(EP, None, TP),
    )
    out_specs = (P(EP, TP), P(EP, TP))
    return jax.shard_map(
        shards, mesh=finer, in_specs=in_specs, out_specs=out_specs, check_vma=False
    )
```
